512 devices in a mesh: grp: 2 (over y), ep: 32 (over z, core), tp: 8 (over x).
Axes of the slice: x: 8, y: 2, z: 16, core: 2. Of those that a mesh axis runs over, the one named last changes fastest.
The devices are a block of a 8x8x16 slice.
Arguments:
- recurrence_query_input: bfloat16 [8192, 2048], P(('grp', 'ep'), 'tp'), parts along dimension 0, may hold values from -6 to 6
- forget_gate_input: bfloat16 [8192, 2048], P(('grp', 'ep'), 'tp'), parts along dimension 0, may hold values from -6.5 to 6.5
- recurrence_value_input: bfloat16 [8192, 2048], P(('grp', 'ep'), 'tp'), parts along dimension 0, may hold values from -6 to 6
- output_gate_input: bfloat16 [8192, 2048], P(('grp', 'ep'), 'tp'), parts along dimension 0, may hold values from -6 to 6
- forget_lower_margin: float32 [2048], P('tp'), may hold values from 0 to 0.1
- position_decay_extra: float32 [8192, 16], P(('grp', 'ep'), 'tp'), parts along dimension 0, may hold values from -2.1 to 0
- head_norm_gain: float32 [2048], P('tp'), may hold values from 0.1 to 1.9
- recurrence_out_weight: bfloat16 [2048, 2048], P('tp'), may hold values from -0.125 to 0.125
- expert_hidden_state: bfloat16 [8192, 2048], P(('grp', 'ep')), parts along dimension 0, may hold values from -6 to 6
- chosen_expert_index: int32 [8192, 4], P(('grp', 'ep')), parts along dimension 0, may hold values from 0 to 31, all different within a row; in each aligned block of 128 rows (0 to 127, 128 to 255, ...) at most 32 rows name the same one
- chosen_expert_score: float32 [8192, 4], P(('grp', 'ep')), parts along dimension 0, may hold values from 0.02 to 1
- expert_norm_gain: float32 [2048], replicated, may hold values from 0.1 to 1.9
- routed_gate_weight: bfloat16 [32, 2048, 1024], P('ep', None, 'tp'), may hold values from -0.125 to 0.125
- routed_up_weight: bfloat16 [32, 2048, 1024], P('ep', None, 'tp'), may hold values from -0.125 to 0.125
- routed_down_weight: bfloat16 [32, 1024, 2048], P('ep', None, 'tp'), may hold values from -0.1875 to 0.1875
- shared_gate_weight: bfloat16 [2048, 1024], P(None, 'tp'), may hold values from -0.125 to 0.125
- shared_up_weight: bfloat16 [2048, 1024], P(None, 'tp'), may hold values from -0.125 to 0.125
- shared_down_weight: bfloat16 [1024, 2048], P(None, 'tp'), may hold values from -0.1875 to 0.1875
Outputs:
- recurrence_output: bfloat16 [8192, 2048], P(('grp', 'ep', 'tp')), parts along dimension 0
- expert_out: bfloat16 [8192, 2048], P(('grp', 'ep'), 'tp'), parts along dimension 0
The draws below stay inside these ranges and needn't reach their ends.
There are 2 independent parts, one for each index of `grp`. The reference program is written for one: setup_inputs(seed, part) draws one part's arguments, and reference() takes and returns one part's arrays. A program takes and returns all parts, laid end to end along the dimension named above; an argument that names none is the same for every part. Nothing has to cross between parts.
Inputs may be any that keep to these rules, and one draw needn't show every extreme that they name: `chosen_expert_index`: each row names 4 different experts. In each aligned block of 128 rows (the rows of one index of ep) no expert is named by more than 32 rows, and in every draw some block names some expert exactly 32 times.
All inputs are finite; a program needn't handle non-finite values.
Results may differ from the reference program's by a relative error of at most 0.015.
Values may be sent and summed in bfloat16 or wider, within the bound.
No kernel may reach another device: no remote copies, remote signals or barrier semaphores. Data moves between devices by JAX's collectives and lax.ppermute only.
A program may use at most 64 MiB of HBM per device.

```python
import math
import jax
import jax.numpy as jnp
import numpy as np
from jax import lax

D = 2048
HEADS = 16
HEAD_CHANNELS = 128
W = 2048
BLK = 64
FF = 1024
TOP_K = 4
EXPERTS = 32
TOKA_DEV = 128
TOKB_DEV = 128
SEQ_A = 4096
TOK_B = 4096
CAP = 32
N_EP = 32
N_TP = 8


def draw_forget_gate_input(key, part):
    noise_key, shift_key = jax.random.split(jax.random.fold_in(key, 11))
    noise = jnp.clip(jax.random.normal(noise_key, (SEQ_A, W), jnp.float32), -5.0, 5.0)
    shifts = jax.random.uniform(shift_key, (SEQ_A // TOKA_DEV, 1, 1), jnp.float32, -1.5, 1.5)
    shifted = noise.reshape(SEQ_A // TOKA_DEV, TOKA_DEV, W) + shifts
    return shifted.reshape(SEQ_A, W).astype(jnp.bfloat16)


def draw_forget_lower_margin(key, part):
    pick_key, slow_key, fast_key = jax.random.split(jax.random.fold_in(key, 23), 3)
    slow_count = HEADS // 2
    slow_heads = (jax.random.permutation(pick_key, HEADS) < slow_count)[:, None]
    slow = 2.0 * jnp.exp(jax.random.uniform(slow_key, (HEADS, HEAD_CHANNELS), jnp.float32, math.log(0.1), math.log(0.6))) / SEQ_A
    fast = jnp.exp(jax.random.uniform(fast_key, (HEADS, HEAD_CHANNELS), jnp.float32, math.log(0.03), math.log(0.09)))
    return jnp.where(slow_heads, slow, fast).reshape(W).astype(jnp.float32)


def draw_position_decay_extra(key, part):
    place_key, depth_key, count_key = jax.random.split(jax.random.fold_in(key, 37), 3)
    spots = jax.random.randint(place_key, (3, HEADS), 0, SEQ_A)
    counts = jax.random.randint(count_key, (1, HEADS), 1, 4)
    active = jnp.arange(3)[:, None] < counts
    depth = jnp.log(jax.random.uniform(depth_key, (3, HEADS), jnp.float32, 0.5, 0.8))
    positions = jnp.arange(SEQ_A)[:, None, None]
    hits = (positions == spots[None]) & active[None]
    return jnp.sum(jnp.where(hits, depth[None], 0.0), axis=1).astype(jnp.float32)


def levels(rng, shape, pieces, smallest, largest):
    def one(axis_at, parts):
        heights = jax.random.uniform(jax.random.fold_in(jax.random.fold_in(rng, 6), axis_at), (parts,), jnp.float32, smallest / len(pieces), largest / len(pieces))
        return jnp.repeat(jnp.exp(heights), shape[axis_at] // parts).reshape((-1,) + (1,) * (len(shape) - axis_at - 1))

    factor_of = one(*pieces[0])
    for cut in pieces[1:]:
        factor_of = factor_of * one(*cut)
    return factor_of


def shared_out(key, own, number, rows, number_of, top, reach, skew):
    sequence = jax.random.permutation(key, number_of)
    packed, common = load_shares(number_of, rows * top, reach, skew, True), load_shares(number_of, rows * top, reach, skew, False)
    places = jnp.arange(number_of)

    def named(tallies, turn):
        used = int((tallies > 0).sum())
        fixed = max(1, used // 4)
        moved = fixed + (places - fixed + turn * (used - fixed)) % max(1, number_of - fixed)
        return jnp.zeros((number_of,), jnp.int32).at[sequence[jnp.where(places < fixed, places, moved)]].set(jnp.asarray(tallies, jnp.int32))

    tallies = jnp.where(number % 4 == 0, named(packed, number // 4), named(common, number - number // 4 - 1))
    mixed = jax.random.permutation(jax.random.fold_in(own, 3), number_of)
    giver, taker = mixed[0:number_of // 2 * 2:2], mixed[1:number_of // 2 * 2:2]
    margin = jnp.minimum(tallies[giver] - 1, reach - tallies[taker]) // 2
    margin = jnp.where((giver == sequence[0]) | (taker == sequence[0]) | (tallies[taker] == 0), 0, jnp.maximum(margin, 0))
    moved = jax.random.randint(jax.random.fold_in(own, 4), (number_of // 2,), 0, 1 << 20) % (margin + 1)
    tallies = tallies.at[giver].add(-moved).at[taker].add(moved)
    members = jnp.searchsorted(jnp.cumsum(tallies), jnp.arange(rows * top), side="right").astype(jnp.int32)
    table = members.reshape(top, rows).T
    table = table[jax.random.permutation(jax.random.fold_in(own, 1), rows)]
    turn = jax.random.randint(jax.random.fold_in(own, 2), (rows, 1), 0, top)
    return jnp.take_along_axis(table, (jnp.arange(top)[None, :] + turn) % top, axis=1)


def load_shares(count, total, limit, lean, full):
    portions = [(1 << 20) // math.isqrt(standing ** lean) + 1 for standing in range(1, count + 1)]
    largest = limit if full else min(limit, max(-(-total // count), total * portions[0] // sum(portions)))
    least = 1 if total - largest >= count - 1 else 0
    holding, spare = [largest] + [least] * (count - 1), total - largest - least * (count - 1)
    while spare > 0:
        free = [i for i in range(1, count) if holding[i] < largest] or [i for i in range(1, count) if holding[i] < limit]
        pool, remaining = sum([portions[i] for i in free]), spare
        for i in free:
            more = min(limit - holding[i], max(1, remaining * portions[i] // pool), spare)
            holding[i] = holding[i] + more
            spare = spare - more
    return np.array(holding)


def gaussian(key, extent, width, reach, cuts=(), held_as=jnp.bfloat16):
    entries = jax.random.normal(key, extent, jnp.float32) * width
    if len(cuts) > 0:
        entries = levels(key, extent, cuts, -0.22, 0.18) * entries
    return jnp.clip(entries, min=-reach, max=reach).astype(held_as)


def setup_inputs(seed: int = 0, part: int = 0) -> dict:
    keys = jax.random.split(jax.random.key(seed), 19)
    part_splits = jax.random.split(jax.random.fold_in(keys[18], part), 19)
    recurrence_query_input = gaussian(part_splits[0], (SEQ_A, W), 1.0, 6.0, ((0, 32), (1, 8)))
    forget_gate_input = draw_forget_gate_input(jax.random.fold_in(jax.random.fold_in(keys[18], part), 71), part)
    recurrence_value_input = gaussian(part_splits[2], (SEQ_A, W), 1.0, 6.0, ((0, 32), (1, 8)))
    output_gate_input = gaussian(part_splits[3], (SEQ_A, W), 1.0, 6.0, ((0, 32), (1, 8)))
    forget_lower_margin = draw_forget_lower_margin(jax.random.fold_in(keys[18], 71), part)
    position_decay_extra = draw_position_decay_extra(jax.random.fold_in(jax.random.fold_in(keys[18], part), 71), part)
    head_norm_gain = jnp.clip(1.0 + 0.18 * jax.random.normal(keys[6], (W,), jnp.float32), 0.1, 1.9)
    recurrence_out_weight = gaussian(keys[7], (W, D), W ** -0.5, 0.125, ((0, 8),))
    expert_hidden_state = gaussian(part_splits[8], (TOK_B, D), 1.0, 6.0, ((0, 32),))
    chosen_expert_index_keys = jax.random.split(jax.random.fold_in(part_splits[9], 1), TOK_B // TOKB_DEV)
    chosen_expert_index_turns = jax.random.permutation(jax.random.fold_in(part_splits[9], 3), TOK_B // TOKB_DEV)
    chosen_expert_index = jax.vmap(lambda own, number: shared_out(jax.random.fold_in(part_splits[9], 2), own, number, TOKB_DEV, EXPERTS, TOP_K, CAP, 1))(chosen_expert_index_keys, chosen_expert_index_turns).reshape((TOK_B, TOP_K))
    chosen_expert_score = jnp.clip(jnp.exp(math.log(1.0) - 3.912023 * jax.random.uniform(part_splits[10], (TOK_B, TOP_K), jnp.float32) ** levels(part_splits[10], (TOK_B, TOP_K), ((0, 32),), -0.2, 0.2)), 0.02, 1.0)
    expert_norm_gain = jnp.clip(1.0 + 0.18 * jax.random.normal(keys[11], (D,), jnp.float32), 0.1, 1.9)
    routed_gate_weight = gaussian(keys[12], (EXPERTS, D, FF), D ** -0.5, 0.125, ((0, 32), (2, 8)))
    routed_up_weight = gaussian(keys[13], (EXPERTS, D, FF), D ** -0.5, 0.125, ((0, 32), (2, 8)))
    routed_down_weight = gaussian(keys[14], (EXPERTS, FF, D), FF ** -0.5, 0.1875, ((0, 32), (2, 8)))
    shared_gate_weight = gaussian(keys[15], (D, FF), D ** -0.5, 0.125, ((1, 8),))
    shared_up_weight = gaussian(keys[16], (D, FF), D ** -0.5, 0.125, ((1, 8),))
    shared_down_weight = gaussian(keys[17], (FF, D), FF ** -0.5, 0.1875, ((1, 8),))
    return dict(recurrence_query_input=recurrence_query_input, forget_gate_input=forget_gate_input, recurrence_value_input=recurrence_value_input, output_gate_input=output_gate_input, forget_lower_margin=forget_lower_margin, position_decay_extra=position_decay_extra, head_norm_gain=head_norm_gain, recurrence_out_weight=recurrence_out_weight, expert_hidden_state=expert_hidden_state, chosen_expert_index=chosen_expert_index, chosen_expert_score=chosen_expert_score, expert_norm_gain=expert_norm_gain, routed_gate_weight=routed_gate_weight, routed_up_weight=routed_up_weight, routed_down_weight=routed_down_weight, shared_gate_weight=shared_gate_weight, shared_up_weight=shared_up_weight, shared_down_weight=shared_down_weight)


EPSILON = 1e-06
ROUTED_SCALE = 2.5
HIGHEST_PRECISION = lax.Precision.HIGHEST

def recurrence(queries, key_gate_value, decay_logarithm, value_rows):
    length = queries.shape[0]
    blocks = length // BLK

    def split_heads(tensor):
        return tensor.reshape(blocks, BLK, HEADS, HEAD_CHANNELS).transpose(2, 0, 1, 3)
    query_heads = split_heads(queries)
    key_heads = split_heads(key_gate_value)
    value_heads = split_heads(value_rows)
    cum_decay = jnp.cumsum(split_heads(decay_logarithm), axis=2)
    middle = cum_decay[:, :, BLK // 2 - 1:BLK // 2]
    block_end = cum_decay[:, :, BLK - 1:BLK]
    scores = jnp.einsum('hncd,hnsd->hncs', query_heads * jnp.exp(cum_decay - middle), key_heads * jnp.exp(middle - cum_decay), precision=HIGHEST_PRECISION)
    causal = jnp.tril(jnp.ones((BLK, BLK), dtype=bool))
    scores = jnp.where(causal, scores, 0.0)
    within = jnp.einsum('hncs,hnse->hnce', scores, value_heads, precision=HIGHEST_PRECISION)
    updates = jnp.einsum('hncd,hnce->nhde', key_heads * jnp.exp(block_end - cum_decay), value_heads, precision=HIGHEST_PRECISION)
    block_decay = jnp.exp(block_end[:, :, 0, :]).transpose(1, 0, 2)

    def advance(carry_state, inputs):
        factor, update = inputs
        return (factor[..., None] * carry_state + update, carry_state)
    initial = jnp.zeros((HEADS, HEAD_CHANNELS, HEAD_CHANNELS), jnp.float32)
    _, starts = lax.scan(advance, initial, (block_decay, updates))
    carried = jnp.einsum('hncd,nhde->hnce', query_heads * jnp.exp(cum_decay), starts, precision=HIGHEST_PRECISION)
    return (within + carried).transpose(1, 2, 0, 3).reshape(length, HEADS, HEAD_CHANNELS)

def recurrence_reference(recurrence_query_input, forget_gate_input, recurrence_value_input, output_gate_input, forget_lower_margin, position_decay_extra, head_norm_gain, recurrence_out_weight):
    length = recurrence_query_input.shape[0]
    queries = jax.nn.silu(recurrence_query_input.astype(jnp.float32))
    key_gate_value = forget_lower_margin[None, :] * jax.nn.sigmoid(-forget_gate_input.astype(jnp.float32))
    decay_logarithm = jnp.log1p(-key_gate_value) + jnp.repeat(position_decay_extra, HEAD_CHANNELS, axis=1)
    value_rows = recurrence_value_input.astype(jnp.float32)
    outputs = recurrence(queries, key_gate_value, decay_logarithm, value_rows)
    factor = lax.rsqrt(lax.optimization_barrier(jnp.mean(outputs * outputs, axis=2, keepdims=True)) + EPSILON)
    normed = (outputs * factor).reshape(length, W) * head_norm_gain[None, :]
    gated_rows = (normed * jax.nn.silu(output_gate_input.astype(jnp.float32))).astype(jnp.bfloat16)
    columns = W // N_TP
    summed = jnp.zeros((length, D), jnp.float32)
    for member in range(N_TP):
        partial_sum = jnp.dot(gated_rows[:, member * columns:(member + 1) * columns], recurrence_out_weight[member * columns:(member + 1) * columns], preferred_element_type=jnp.float32).astype(jnp.bfloat16)
        summed = summed + lax.optimization_barrier(partial_sum).astype(jnp.float32)
    return summed.astype(jnp.bfloat16)

def expert_reference(expert_hidden_state, chosen_expert_index, chosen_expert_score, expert_norm_gain, routed_gate_weight, routed_up_weight, routed_down_weight, shared_gate_weight, shared_up_weight, shared_down_weight):
    tokens = expert_hidden_state.shape[0]
    features = expert_hidden_state.astype(jnp.float32)
    normed = (features * lax.rsqrt(lax.optimization_barrier(jnp.mean(features * features, axis=1, keepdims=True)) + EPSILON) * expert_norm_gain[None, :]).astype(jnp.bfloat16)
    gates = ROUTED_SCALE * chosen_expert_score / lax.optimization_barrier(jnp.sum(chosen_expert_score, axis=1, keepdims=True))
    blocked = chosen_expert_index.reshape(N_EP, TOKB_DEV * TOP_K)
    onehot = (blocked[:, :, None] == jnp.arange(EXPERTS, dtype=jnp.int32)[None, None, :]).astype(jnp.int32)
    places = lax.optimization_barrier(jnp.sum(onehot * (jnp.cumsum(onehot, axis=1) - 1), axis=2)).reshape(-1)
    sources = jnp.arange(tokens * TOP_K, dtype=jnp.int32) // (TOKB_DEV * TOP_K)
    slots = (chosen_expert_index.reshape(-1) * N_EP + sources) * CAP + places
    owners = jnp.full((EXPERTS * N_EP * CAP,), tokens, jnp.int32).at[slots].set(jnp.arange(tokens * TOP_K, dtype=jnp.int32) // TOP_K)
    padded = jnp.concatenate([normed, jnp.zeros((1, D), jnp.bfloat16)], axis=0)
    grouped = padded[owners].reshape(EXPERTS, N_EP * CAP, D)

    def one_expert(inputs):
        slot_rows, gate_matrix, up_matrix, down_matrix = inputs
        hidden = (jax.nn.silu(jnp.dot(slot_rows, gate_matrix, preferred_element_type=jnp.float32)) * jnp.dot(slot_rows, up_matrix, preferred_element_type=jnp.float32)).astype(jnp.bfloat16)
        return jnp.dot(hidden, down_matrix, preferred_element_type=jnp.float32).astype(jnp.bfloat16)
    results = lax.map(one_expert, (grouped, routed_gate_weight, routed_up_weight, routed_down_weight))
    picked = results.reshape(EXPERTS * N_EP * CAP, D)[slots].reshape(tokens, TOP_K, D)
    shared_hidden = (jax.nn.silu(jnp.dot(normed, shared_gate_weight, preferred_element_type=jnp.float32)) * jnp.dot(normed, shared_up_weight, preferred_element_type=jnp.float32)).astype(jnp.bfloat16)
    shared_result = jnp.dot(shared_hidden, shared_down_weight, preferred_element_type=jnp.float32)
    combined = shared_result + lax.optimization_barrier(jnp.sum(gates[:, :, None] * picked.astype(jnp.float32), axis=1))
    return combined.astype(jnp.bfloat16)

def reference(recurrence_query_input, forget_gate_input, recurrence_value_input, output_gate_input, forget_lower_margin, position_decay_extra, head_norm_gain, recurrence_out_weight, expert_hidden_state, chosen_expert_index, chosen_expert_score, expert_norm_gain, routed_gate_weight, routed_up_weight, routed_down_weight, shared_gate_weight, shared_up_weight, shared_down_weight):
    recurrence_output = recurrence_reference(recurrence_query_input, forget_gate_input, recurrence_value_input, output_gate_input, forget_lower_margin, position_decay_extra, head_norm_gain, recurrence_out_weight)
    expert_out = expert_reference(expert_hidden_state, chosen_expert_index, chosen_expert_score, expert_norm_gain, routed_gate_weight, routed_up_weight, routed_down_weight, shared_gate_weight, shared_up_weight, shared_down_weight)
    return (recurrence_output, expert_out)
```

```python
import jax
import jax.numpy as jnp
from jax import lax
from jax.sharding import Mesh
from jax.sharding import PartitionSpec as P

HEAD_CHANNELS = 128
BLK = 64
EP = ("ep_0", "ep_1")
GRP_EP = ("grp", "ep_0", "ep_1")
GRP_EP_TP = ("grp", "ep_0", "ep_1", "tp")


EPSILON = 1e-06
ROUTED_SCALE = 2.5
HIGHEST_PRECISION = lax.Precision.HIGHEST


def shifted(array, axis, step):
    count = lax.axis_size(axis)
    return lax.ppermute(array, axis, [(i, (i + step) % count) for i in range(count)])


def swapped(array, axis):
    count = lax.axis_size(axis)
    return lax.ppermute(array, axis, [(i, i ^ 1) for i in range(count)])


def exchanged(array, axis):
    return lax.all_to_all(array, axis, split_axis=0, concat_axis=0, tiled=True)


def in_blocks(array, dim, count):
    before, after = (array.shape[:dim], array.shape[dim + 1 :])
    return jnp.moveaxis(array.reshape(*before, count, -1, *after), dim, 0)


def sent_and_summed(array, axis, dim):
    pieces = in_blocks(array, dim, lax.axis_size(axis))
    return exchanged(pieces, axis).astype(jnp.float32).sum(axis=0)


def joined_along(pieces, dim):
    shape = list(pieces.shape[1:])
    shape[dim] *= pieces.shape[0]
    return jnp.moveaxis(pieces, 0, dim).reshape(shape)


def copy_for_each(array, axis):
    count = lax.axis_size(axis)
    return exchanged(jnp.broadcast_to(array[None], (count, *array.shape)), axis)


def in_parts(array, count):
    parts, rest = [], array
    for _ in range(count):
        rounded = lax.reduce_precision(rest, 8, 7)
        parts.append(rounded.astype(jnp.bfloat16))
        rest = rest - rounded
    return parts


def entering_state(log_decay, state):
    devices = lax.axis_size(EP)
    channels, width = state.shape
    part = channels // devices
    logs = jnp.stack(in_parts(log_decay, 3), axis=-1).reshape(devices, part, 3)
    logs = jnp.pad(logs, ((0, 0), (0, 0), (0, HEAD_CHANNELS - 3)))
    packed = jnp.concatenate(
        [state.astype(jnp.bfloat16).reshape(devices, part, width), logs], axis=2
    )
    arrived = exchanged(packed, EP).astype(jnp.float32)
    updates = arrived[:, :, :width]
    logs = jnp.sum(arrived[:, :, width : width + 3], axis=2)
    at = jnp.arange(devices)
    between = (at[None, None, :] > at[None, :, None]) & (at[None, None, :] < at[:, None, None])
    spans = jnp.dot(
        between.reshape(devices * devices, devices).astype(jnp.float32),
        logs,
        precision=HIGHEST_PRECISION,
    ).reshape(devices, devices, part)
    earlier = at[None, :, None] < at[:, None, None]
    factors = jnp.where(earlier, jnp.exp(spans), 0.0)
    prefix = jnp.einsum("rqc,qcv->rcv", factors, updates, precision=HIGHEST_PRECISION)
    returned = exchanged(prefix.astype(jnp.bfloat16), EP)
    return returned.astype(jnp.float32).reshape(channels, width)


def mixer_half(
    recurrence_query_input,
    forget_gate_input,
    recurrence_value_input,
    output_gate_input,
    forget_lower_margin,
    position_decay_extra,
    head_norm_gain,
    recurrence_out_weight,
):
    length = recurrence_query_input.shape[0]
    head_tensor = position_decay_extra.shape[1]
    blocks = length // BLK
    queries = jax.nn.silu(recurrence_query_input.astype(jnp.float32))
    key_gate_value = forget_lower_margin[None, :] * jax.nn.sigmoid(
        -forget_gate_input.astype(jnp.float32)
    )
    decay_logarithm = jnp.log1p(-key_gate_value) + jnp.repeat(
        position_decay_extra, HEAD_CHANNELS, axis=1
    )
    value_rows = recurrence_value_input.astype(jnp.float32)

    def split_heads(tensor):
        return tensor.reshape(blocks, BLK, head_tensor, HEAD_CHANNELS).transpose(2, 0, 1, 3)

    query_heads = split_heads(queries)
    key_heads = split_heads(key_gate_value)
    value_heads = split_heads(value_rows)
    cum_decay = jnp.cumsum(split_heads(decay_logarithm), axis=2)
    middle = cum_decay[:, :, BLK // 2 - 1 : BLK // 2]
    block_end = cum_decay[:, :, BLK - 1 : BLK]
    scores = jnp.einsum(
        "hncd,hnsd->hncs",
        query_heads * jnp.exp(cum_decay - middle),
        key_heads * jnp.exp(middle - cum_decay),
        precision=HIGHEST_PRECISION,
    )
    causal = jnp.tril(jnp.ones((BLK, BLK), dtype=bool))
    scores = jnp.where(causal, scores, 0.0)
    within = jnp.einsum("hncs,hnse->hnce", scores, value_heads, precision=HIGHEST_PRECISION)
    updates = jnp.einsum(
        "hncd,hnce->nhde",
        key_heads * jnp.exp(block_end - cum_decay),
        value_heads,
        precision=HIGHEST_PRECISION,
    )
    block_log = block_end[:, :, 0, :]
    block_decay = jnp.exp(block_log).transpose(1, 0, 2)

    def advance(carry_state, inputs):
        factor, update = inputs
        return (factor[..., None] * carry_state + update, carry_state)

    initial = jnp.zeros((head_tensor, HEAD_CHANNELS, HEAD_CHANNELS), jnp.float32)
    local_final, local_starts = lax.scan(advance, initial, (block_decay, updates))
    incoming = entering_state(
        jnp.sum(block_log, axis=1).reshape(-1), local_final.reshape(-1, HEAD_CHANNELS)
    ).reshape(head_tensor, HEAD_CHANNELS, HEAD_CHANNELS)
    before = jnp.exp(jnp.cumsum(block_log, axis=1) - block_log).transpose(1, 0, 2)
    starts = local_starts + before[..., None] * incoming[None]
    carried = jnp.einsum(
        "hncd,nhde->hnce", query_heads * jnp.exp(cum_decay), starts, precision=HIGHEST_PRECISION
    )
    outputs = (within + carried).transpose(1, 2, 0, 3).reshape(length, head_tensor, HEAD_CHANNELS)
    factor = lax.rsqrt(jnp.mean(outputs * outputs, axis=2, keepdims=True) + EPSILON)
    normed = (outputs * factor).reshape(length, head_tensor * HEAD_CHANNELS) * head_norm_gain[
        None, :
    ]
    gated_rows = (normed * jax.nn.silu(output_gate_input.astype(jnp.float32))).astype(jnp.bfloat16)
    mixed = sent_and_summed(
        jnp.dot(gated_rows, recurrence_out_weight, preferred_element_type=jnp.float32).astype(
            jnp.bfloat16
        ),
        "tp",
        0,
    )
    return mixed.astype(jnp.bfloat16)


def expert_half(
    expert_hidden_state,
    chosen_expert_index,
    chosen_expert_score,
    expert_norm_gain,
    routed_gate_weight,
    routed_up_weight,
    routed_down_weight,
    shared_gate_weight,
    shared_up_weight,
    shared_down_weight,
):
    tokens, top = chosen_expert_index.shape
    local_experts = routed_gate_weight.shape[0]
    devices = lax.axis_size(EP)
    experts = local_experts * devices
    capacity = min(tokens, 2 * tokens * top // experts)
    width_out = routed_down_weight.shape[2]
    width_members = lax.axis_size("tp")
    quads = width_members // 2
    member = lax.axis_index("tp")
    parity, quad = (member % 2, member // 2)
    share = capacity // width_members
    half = capacity // 2
    width_in = routed_gate_weight.shape[1]
    units = routed_gate_weight.shape[2]

    own_in = jnp.concatenate([routed_gate_weight[0], routed_up_weight[0]], axis=1)
    partner_in = swapped(own_in, "tp")
    own_down = routed_down_weight[0]
    partner_down = swapped(own_down, "tp")

    features = expert_hidden_state.astype(jnp.float32)
    normed = (
        features
        * lax.rsqrt(jnp.mean(features * features, axis=1, keepdims=True) + EPSILON)
        * expert_norm_gain[None, :]
    ).astype(jnp.bfloat16)
    gates = ROUTED_SCALE * chosen_expert_score / jnp.sum(chosen_expert_score, axis=1, keepdims=True)
    named = chosen_expert_index[:, :, None] == jnp.arange(experts, dtype=jnp.int32)[None, None, :]
    chosen = jnp.any(named, axis=1)
    gate_of = jnp.sum(jnp.where(named, gates[:, :, None], 0.0), axis=1)
    row = jnp.arange(tokens)
    places = jnp.dot(
        (row[None, :] < row[:, None]).astype(jnp.bfloat16),
        chosen.astype(jnp.bfloat16),
        preferred_element_type=jnp.float32,
    )
    places = jnp.where(chosen, places.astype(jnp.int32), -1)
    first = parity * half + quad * share
    picks = places.T[:, None, :] == first + jnp.arange(share)[None, :, None]
    outgoing = jnp.dot(
        picks.reshape(experts * share, tokens).astype(jnp.bfloat16),
        normed,
        preferred_element_type=jnp.float32,
    ).astype(jnp.bfloat16)
    arrived = exchanged(outgoing.reshape(devices, share, width_in), EP)
    chunk = arrived.reshape(devices * share, width_in)
    rows = chunk.shape[0]

    shared_hidden = (
        jax.nn.silu(jnp.dot(normed, shared_gate_weight, preferred_element_type=jnp.float32))
        * jnp.dot(normed, shared_up_weight, preferred_element_type=jnp.float32)
    ).astype(jnp.bfloat16)
    shared_piece = joined_along(copy_for_each(shared_hidden, "tp"), 1)
    shared = jnp.dot(shared_piece, shared_down_weight, preferred_element_type=jnp.float32)

    def hidden_of(piece):
        sides = []
        for matrix in (own_in, partner_in):
            both = jnp.dot(piece, matrix, preferred_element_type=jnp.float32)
            sides.append((jax.nn.silu(both[:, :units]) * both[:, units:]).astype(jnp.bfloat16))
        return jnp.concatenate(sides, axis=1)

    from_before = shifted(chunk, "tp", 2)
    from_after = shifted(chunk, "tp", -2)
    across_first = shifted(from_before[: rows // 2], "tp", 2)
    across_second = shifted(from_after[rows // 2 :], "tp", -2)
    hidden_own = hidden_of(chunk)
    hidden_sides = hidden_of(jnp.concatenate([from_after, from_before], axis=0))
    hidden_across = hidden_of(jnp.concatenate([across_first, across_second], axis=0))
    around = [hidden_own, hidden_sides[:rows], hidden_across, hidden_sides[rows:]]
    hidden = lax.dynamic_slice_in_dim(
        jnp.concatenate(around + around, axis=0), (quads - quad) % quads * rows, quads * rows, 0
    )

    middle = quads * rows // 2
    hidden_before = shifted(hidden, "tp", 2)
    hidden_after = shifted(hidden, "tp", -2)
    hidden_far = jnp.concatenate(
        [shifted(hidden_before[:middle], "tp", 2), shifted(hidden_after[middle:], "tp", -2)], axis=0
    )

    def down_of(step):
        at = (quad + step) % quads * 2
        blocks = []
        for side in (parity, 1 - parity):
            place = (at + side) * units
            blocks.append(
                jnp.concatenate(
                    [
                        lax.dynamic_slice_in_dim(matrix, place, units, 0)
                        for matrix in (own_down, partner_down)
                    ],
                    axis=1,
                )
            )
        return jnp.concatenate(blocks, axis=0)

    def product(piece, step):
        return jnp.dot(piece, down_of(step), preferred_element_type=jnp.float32)

    routed = product(hidden, 0) + product(hidden_before, -1) + product(hidden_after, 1)
    routed = routed + product(hidden_far, 2)
    answers = routed.astype(jnp.bfloat16).reshape(quads, devices, share, 2 * width_out)
    answers = answers.transpose(1, 0, 2, 3).reshape(devices, half, 2 * width_out)
    returned = exchanged(answers, EP).reshape(experts * half, 2 * width_out)
    filled = places[:, :, None] == parity * half + jnp.arange(half)[None, None, :]
    mixing = jnp.where(filled, gate_of[:, :, None], 0.0).reshape(tokens, experts * half)
    combined = sum(
        jnp.dot(part, returned, preferred_element_type=jnp.float32) for part in in_parts(mixing, 3)
    )
    other = swapped(combined[:, width_out:].astype(jnp.bfloat16), "tp")
    combined = shared + combined[:, :width_out] + other.astype(jnp.float32)
    return combined.astype(jnp.bfloat16)


def per_device(
    recurrence_query_input,
    forget_gate_input,
    recurrence_value_input,
    output_gate_input,
    forget_lower_margin,
    position_decay_extra,
    head_norm_gain,
    recurrence_out_weight,
    expert_hidden_state,
    chosen_expert_index,
    chosen_expert_score,
    expert_norm_gain,
    routed_gate_weight,
    routed_up_weight,
    routed_down_weight,
    shared_gate_weight,
    shared_up_weight,
    shared_down_weight,
):
    recurrence_output = mixer_half(
        recurrence_query_input,
        forget_gate_input,
        recurrence_value_input,
        output_gate_input,
        forget_lower_margin,
        position_decay_extra,
        head_norm_gain,
        recurrence_out_weight,
    )
    expert_out = expert_half(
        expert_hidden_state,
        chosen_expert_index,
        chosen_expert_score,
        expert_norm_gain,
        routed_gate_weight,
        routed_up_weight,
        routed_down_weight,
        shared_gate_weight,
        shared_up_weight,
        shared_down_weight,
    )
    return (recurrence_output, expert_out)


def solution(mesh):
    split = Mesh(
        mesh.devices.reshape(mesh.shape["grp"], 16, 2, mesh.shape["tp"]),
        ("grp", "ep_0", "ep_1", "tp"),
    )
    in_specs = (
        P(GRP_EP, "tp"),
        P(GRP_EP, "tp"),
        P(GRP_EP, "tp"),
        P(GRP_EP, "tp"),
        P("tp"),
        P(GRP_EP, "tp"),
        P("tp"),
        P("tp", None),
        P(GRP_EP, None),
        P(GRP_EP, None),
        P(GRP_EP, None),
        P(),
        P(EP, None, "tp"),
        P(EP, None, "tp"),
        P(EP, None, "tp"),
        P(None, "tp"),
        P(None, "tp"),
        P(None, "tp"),
    )
    out_specs = (P(GRP_EP_TP, None), P(GRP_EP, "tp"))
    return jax.shard_map(
        per_device, mesh=split, in_specs=in_specs, out_specs=out_specs, check_vma=False
    )
```

```python
import jax
import jax.numpy as jnp
from jax import lax
from jax.sharding import Mesh
from jax.sharding import PartitionSpec as P


HEAD_CHANNELS = 128
BLK = 64
EP = ("ep_0", "ep_1")
GRP_EP = ("grp", "ep_0", "ep_1")
GRP_EP_TP = ("grp", "ep_0", "ep_1", "tp")


EPSILON = 1e-06
ROUTED_SCALE = 2.5
HIGHEST_PRECISION = lax.Precision.HIGHEST


def shifted(array, axis, step):
    count = lax.axis_size(axis)
    return lax.ppermute(array, axis, [(i, (i + step) % count) for i in range(count)])


def swapped(array, axis, bit):
    count = lax.axis_size(axis)
    return lax.ppermute(array, axis, [(i, i ^ bit) for i in range(count)])


def exchanged(array, axis):
    return lax.all_to_all(array, axis, split_axis=0, concat_axis=0, tiled=True)


def half_of(array, dim, place):
    return lax.dynamic_index_in_dim(array, place, dim, keepdims=False)


def summed_to_owners(array, axis):
    count = lax.axis_size(axis)
    bits = count.bit_length() - 1
    member = lax.axis_index(axis)
    kept = array.reshape(*[2] * bits, -1, array.shape[1])
    for bit in range(bits):
        mine = (member >> bit) & 1
        dim = bits - 1 - bit
        arrived = swapped(half_of(kept, dim, 1 - mine).astype(jnp.bfloat16), axis, 1 << bit)
        kept = half_of(kept, dim, mine) + arrived.astype(jnp.float32)
    return kept


def gathered_columns(array, axis):
    count = lax.axis_size(axis)
    member = lax.axis_index(axis)
    for bit in reversed(range(count.bit_length() - 1)):
        arrived = swapped(array, axis, 1 << bit)
        first = ((member >> bit) & 1) == 0
        array = jnp.concatenate(
            [jnp.where(first, array, arrived), jnp.where(first, arrived, array)], axis=1
        )
    return array


def rows_by_reversed_bits(matrix, count):
    bits = count.bit_length() - 1
    split = matrix.reshape(*[2] * bits, -1, matrix.shape[1])
    order = (*reversed(range(bits)), bits, bits + 1)
    return split.transpose(order).reshape(matrix.shape)


def in_parts(array, count):
    parts, rest = [], array
    for _ in range(count):
        rounded = lax.reduce_precision(rest, 8, 7)
        parts.append(rounded.astype(jnp.bfloat16))
        rest = rest - rounded
    return parts


def entering_state(log_decay, state):
    devices = lax.axis_size(EP)
    channels, width = state.shape
    part = channels // devices
    logs = jnp.stack(in_parts(log_decay, 3), axis=-1).reshape(devices, part, 3)
    logs = jnp.pad(logs, ((0, 0), (0, 0), (0, HEAD_CHANNELS - 3)))
    packed = jnp.concatenate(
        [state.astype(jnp.bfloat16).reshape(devices, part, width), logs], axis=2
    )
    arrived = exchanged(packed, EP)
    arrived = arrived.astype(jnp.float32)
    updates = arrived[:, :, :width]
    logs = jnp.sum(arrived[:, :, width : width + 3], axis=2)
    at = jnp.arange(devices)
    between = (at[None, None, :] > at[None, :, None]) & (at[None, None, :] < at[:, None, None])
    spans = jnp.dot(
        between.reshape(devices * devices, devices).astype(jnp.float32),
        logs,
        precision=HIGHEST_PRECISION,
    ).reshape(devices, devices, part)
    earlier = at[None, :, None] < at[:, None, None]
    factors = jnp.where(earlier, jnp.exp(spans), 0.0)
    prefix = jnp.einsum("rqc,qcv->rcv", factors, updates, precision=HIGHEST_PRECISION)
    returned = exchanged(prefix.astype(jnp.bfloat16), EP)
    return returned.astype(jnp.float32).reshape(channels, width)


def mixer_half(
    recurrence_query_input,
    forget_gate_input,
    recurrence_value_input,
    output_gate_input,
    forget_lower_margin,
    position_decay_extra,
    head_norm_gain,
    recurrence_out_weight,
):
    length = recurrence_query_input.shape[0]
    head_tensor = position_decay_extra.shape[1]
    blocks = length // BLK
    queries = jax.nn.silu(recurrence_query_input.astype(jnp.float32))
    key_gate_value = forget_lower_margin[None, :] * jax.nn.sigmoid(
        -forget_gate_input.astype(jnp.float32)
    )
    decay_logarithm = jnp.log1p(-key_gate_value) + jnp.repeat(
        position_decay_extra, HEAD_CHANNELS, axis=1
    )
    value_rows = recurrence_value_input.astype(jnp.float32)

    def split_heads(tensor):
        return tensor.reshape(blocks, BLK, head_tensor, HEAD_CHANNELS).transpose(2, 0, 1, 3)

    query_heads = split_heads(queries)
    key_heads = split_heads(key_gate_value)
    value_heads = split_heads(value_rows)
    cum_decay = jnp.cumsum(split_heads(decay_logarithm), axis=2)
    middle = cum_decay[:, :, BLK // 2 - 1 : BLK // 2]
    block_end = cum_decay[:, :, BLK - 1 : BLK]
    scores = jnp.einsum(
        "hncd,hnsd->hncs",
        query_heads * jnp.exp(cum_decay - middle),
        key_heads * jnp.exp(middle - cum_decay),
        precision=HIGHEST_PRECISION,
    )
    causal = jnp.tril(jnp.ones((BLK, BLK), dtype=bool))
    scores = jnp.where(causal, scores, 0.0)
    within = jnp.einsum("hncs,hnse->hnce", scores, value_heads, precision=HIGHEST_PRECISION)
    updates = jnp.einsum(
        "hncd,hnce->nhde",
        key_heads * jnp.exp(block_end - cum_decay),
        value_heads,
        precision=HIGHEST_PRECISION,
    )
    block_log = block_end[:, :, 0, :]
    block_decay = jnp.exp(block_log).transpose(1, 0, 2)

    def advance(carry_state, inputs):
        factor, update = inputs
        return (factor[..., None] * carry_state + update, carry_state)

    initial = jnp.zeros((head_tensor, HEAD_CHANNELS, HEAD_CHANNELS), jnp.float32)
    local_final, local_starts = lax.scan(advance, initial, (block_decay, updates))
    incoming = entering_state(
        jnp.sum(block_log, axis=1).reshape(-1), local_final.reshape(-1, HEAD_CHANNELS)
    ).reshape(head_tensor, HEAD_CHANNELS, HEAD_CHANNELS)
    before = jnp.exp(jnp.cumsum(block_log, axis=1) - block_log).transpose(1, 0, 2)
    starts = local_starts + before[..., None] * incoming[None]
    carried = jnp.einsum(
        "hncd,nhde->hnce", query_heads * jnp.exp(cum_decay), starts, precision=HIGHEST_PRECISION
    )
    outputs = (within + carried).transpose(1, 2, 0, 3).reshape(length, head_tensor, HEAD_CHANNELS)
    factor = lax.rsqrt(jnp.mean(outputs * outputs, axis=2, keepdims=True) + EPSILON)
    normed = (outputs * factor).reshape(length, head_tensor * HEAD_CHANNELS) * head_norm_gain[
        None, :
    ]
    gated_rows = (normed * jax.nn.silu(output_gate_input.astype(jnp.float32))).astype(jnp.bfloat16)
    partial = jnp.dot(gated_rows, recurrence_out_weight, preferred_element_type=jnp.float32)
    return summed_to_owners(partial, "tp").astype(jnp.bfloat16)


def expert_half(
    expert_hidden_state,
    chosen_expert_index,
    chosen_expert_score,
    expert_norm_gain,
    routed_gate_weight,
    routed_up_weight,
    routed_down_weight,
    shared_gate_weight,
    shared_up_weight,
    shared_down_weight,
):
    tokens, top = chosen_expert_index.shape
    local_experts = routed_gate_weight.shape[0]
    devices = lax.axis_size(EP)
    experts = local_experts * devices
    capacity = min(tokens, 2 * tokens * top // experts)
    width_out = routed_down_weight.shape[2]
    members = lax.axis_size("tp")
    quads = members // 2
    member = lax.axis_index("tp")
    parity, quad = (member & 1, member >> 1)
    half = capacity // 2
    width_in = routed_gate_weight.shape[1] // quads
    units = routed_gate_weight.shape[2]

    own_in = jnp.concatenate([routed_gate_weight[0], routed_up_weight[0]], axis=1)
    own_down = routed_down_weight[0]
    partner_in = swapped(own_in, "tp", 1)
    partner_down = swapped(own_down, "tp", 1)

    features = expert_hidden_state.astype(jnp.float32)
    normed = (
        features
        * lax.rsqrt(jnp.mean(features * features, axis=1, keepdims=True) + EPSILON)
        * expert_norm_gain[None, :]
    ).astype(jnp.bfloat16)
    gates = ROUTED_SCALE * chosen_expert_score / jnp.sum(chosen_expert_score, axis=1, keepdims=True)
    named = chosen_expert_index[:, :, None] == jnp.arange(experts, dtype=jnp.int32)[None, None, :]
    chosen = jnp.any(named, axis=1)
    gate_of = jnp.sum(jnp.where(named, gates[:, :, None], 0.0), axis=1)
    row = jnp.arange(tokens)
    places = jnp.dot(
        (row[None, :] < row[:, None]).astype(jnp.bfloat16),
        chosen.astype(jnp.bfloat16),
        preferred_element_type=jnp.float32,
    )
    places = jnp.where(chosen, places.astype(jnp.int32), -1)
    filled = places[:, :, None] == parity * half + jnp.arange(half)[None, None, :]
    filled = filled.reshape(tokens, experts * half)
    outgoing = lax.dot_general(
        filled.astype(jnp.bfloat16),
        lax.dynamic_slice_in_dim(normed, quad * width_in, width_in, 1),
        (((0,), (0,)), ((), ())),
        preferred_element_type=jnp.float32,
    ).astype(jnp.bfloat16)
    arrived = exchanged(outgoing.reshape(devices, half, width_in), EP)
    chunk = arrived.reshape(devices * half, width_in)
    middle = chunk.shape[0] // 2

    shared_hidden = (
        jax.nn.silu(jnp.dot(normed, shared_gate_weight, preferred_element_type=jnp.float32))
        * jnp.dot(normed, shared_up_weight, preferred_element_type=jnp.float32)
    ).astype(jnp.bfloat16)
    shared_piece = gathered_columns(shared_hidden, "tp")
    shared = jnp.dot(
        shared_piece,
        rows_by_reversed_bits(shared_down_weight, members),
        preferred_element_type=jnp.float32,
    )

    def all_around(piece):
        before = shifted(piece, "tp", 2)
        after = shifted(piece, "tp", -2)
        far = [shifted(before[:middle], "tp", 2), shifted(after[middle:], "tp", -2)]
        return ((piece, 0), (before, -1), (after, 1), (jnp.concatenate(far, axis=0), 2))

    def product(pieces, matrix):
        total = None
        for piece, step in pieces:
            depth = piece.shape[1]
            block = lax.dynamic_slice_in_dim(
                matrix, ((quad + step) & (quads - 1)) * depth, depth, 0
            )
            part = jnp.dot(piece, block, preferred_element_type=jnp.float32)
            total = part if total is None else total + part
        return total

    row_pieces = all_around(chunk)
    sides = []
    for matrix in (own_in, partner_in):
        both = product(row_pieces, matrix)
        sides.append((jax.nn.silu(both[:, :units]) * both[:, units:]).astype(jnp.bfloat16))
    own, other = sides
    even = parity == 0
    hidden = jnp.concatenate([jnp.where(even, own, other), jnp.where(even, other, own)], axis=1)
    hidden_pieces = all_around(hidden)
    answers = jnp.concatenate(
        [
            product(hidden_pieces, matrix).astype(jnp.bfloat16)
            for matrix in (own_down, partner_down)
        ],
        axis=1,
    )
    returned = exchanged(answers.reshape(devices, half, 2 * width_out), EP)
    returned = returned.reshape(experts * half, 2 * width_out)
    mixing = jnp.where(filled.reshape(tokens, experts, half), gate_of[:, :, None], 0.0)
    mixing = mixing.reshape(tokens, experts * half)
    combined = sum(
        jnp.dot(part, returned, preferred_element_type=jnp.float32) for part in in_parts(mixing, 3)
    )
    other = swapped(combined[:, width_out:].astype(jnp.bfloat16), "tp", 1)
    combined = shared + combined[:, :width_out] + other.astype(jnp.float32)
    return combined.astype(jnp.bfloat16)


def per_device(
    recurrence_query_input,
    forget_gate_input,
    recurrence_value_input,
    output_gate_input,
    forget_lower_margin,
    position_decay_extra,
    head_norm_gain,
    recurrence_out_weight,
    expert_hidden_state,
    chosen_expert_index,
    chosen_expert_score,
    expert_norm_gain,
    routed_gate_weight,
    routed_up_weight,
    routed_down_weight,
    shared_gate_weight,
    shared_up_weight,
    shared_down_weight,
):
    recurrence_output = mixer_half(
        recurrence_query_input,
        forget_gate_input,
        recurrence_value_input,
        output_gate_input,
        forget_lower_margin,
        position_decay_extra,
        head_norm_gain,
        recurrence_out_weight,
    )
    expert_out = expert_half(
        expert_hidden_state,
        chosen_expert_index,
        chosen_expert_score,
        expert_norm_gain,
        routed_gate_weight,
        routed_up_weight,
        routed_down_weight,
        shared_gate_weight,
        shared_up_weight,
        shared_down_weight,
    )
    return (recurrence_output, expert_out)


def solution(mesh):
    split = Mesh(
        mesh.devices.reshape(mesh.shape["grp"], 16, 2, mesh.shape["tp"]),
        ("grp", "ep_0", "ep_1", "tp"),
    )
    in_specs = (
        P(GRP_EP, "tp"),
        P(GRP_EP, "tp"),
        P(GRP_EP, "tp"),
        P(GRP_EP, "tp"),
        P("tp"),
        P(GRP_EP, "tp"),
        P("tp"),
        P("tp", None),
        P(GRP_EP, None),
        P(GRP_EP, None),
        P(GRP_EP, None),
        P(),
        P(EP, None, "tp"),
        P(EP, None, "tp"),
        P(EP, None, "tp"),
        P(None, "tp"),
        P(None, "tp"),
        P(None, "tp"),
    )
    out_specs = (P(GRP_EP_TP, None), P(GRP_EP, "tp"))

    return jax.shard_map(
        per_device, mesh=split, in_specs=in_specs, out_specs=out_specs, check_vma=False
    )
```

```python
import functools

import jax
import jax.numpy as jnp
from jax import lax
from jax.experimental import pallas as pl
from jax.experimental.pallas import tpu as pltpu
from jax.sharding import Mesh
from jax.sharding import PartitionSpec as P


HEAD_CHANNELS = 128
BLK = 64
EP = ("ep_0", "ep_1")
GRP_EP = ("grp", "ep_0", "ep_1")
GRP_EP_TP = ("grp", "ep_0", "ep_1", "tp")


EPSILON = 1e-06
ROUTED_SCALE = 2.5
HIGHEST_PRECISION = lax.Precision.HIGHEST


def shifted(array, axis, step):
    count = lax.axis_size(axis)
    return lax.ppermute(array, axis, [(i, (i + step) % count) for i in range(count)])


def swapped(array, axis, bit):
    count = lax.axis_size(axis)
    return lax.ppermute(array, axis, [(i, i ^ bit) for i in range(count)])


def exchanged(array, axis):
    return lax.all_to_all(array, axis, split_axis=0, concat_axis=0, tiled=True)


def half_of(array, dim, place):
    return lax.dynamic_index_in_dim(array, place, dim, keepdims=False)


def summed_to_owners(array, axis):
    count = lax.axis_size(axis)
    bits = count.bit_length() - 1
    member = lax.axis_index(axis)
    kept = array.reshape(*[2] * bits, -1, array.shape[1])
    for bit in range(bits):
        mine = (member >> bit) & 1
        dim = bits - 1 - bit
        arrived = swapped(half_of(kept, dim, 1 - mine).astype(jnp.bfloat16), axis, 1 << bit)
        kept = half_of(kept, dim, mine) + arrived.astype(jnp.float32)
    return kept


def gathered_columns(array, axis):
    count = lax.axis_size(axis)
    member = lax.axis_index(axis)
    for bit in reversed(range(count.bit_length() - 1)):
        arrived = swapped(array, axis, 1 << bit)
        first = ((member >> bit) & 1) == 0
        array = jnp.concatenate(
            [jnp.where(first, array, arrived), jnp.where(first, arrived, array)], axis=1
        )
    return array


def rows_by_reversed_bits(matrix, count):
    bits = count.bit_length() - 1
    split = matrix.reshape(*[2] * bits, -1, matrix.shape[1])
    order = (*reversed(range(bits)), bits, bits + 1)
    return split.transpose(order).reshape(matrix.shape)


def in_parts(array, count):
    parts, rest = [], array
    for _ in range(count):
        rounded = lax.reduce_precision(rest, 8, 7)
        parts.append(rounded.astype(jnp.bfloat16))
        rest = rest - rounded
    return parts


def entering_state(log_decay, state):
    devices = lax.axis_size(EP)
    channels, width = state.shape
    part = channels // devices
    logs = jnp.stack(in_parts(log_decay, 3), axis=-1).reshape(devices, part, 3)
    logs = jnp.pad(logs, ((0, 0), (0, 0), (0, HEAD_CHANNELS - 3)))
    packed = jnp.concatenate(
        [state.astype(jnp.bfloat16).reshape(devices, part, width), logs], axis=2
    )
    arrived = exchanged(packed, EP)
    arrived = arrived.astype(jnp.float32)
    updates = arrived[:, :, :width]
    logs = jnp.sum(arrived[:, :, width : width + 3], axis=2)
    at = jnp.arange(devices)
    between = (at[None, None, :] > at[None, :, None]) & (at[None, None, :] < at[:, None, None])
    spans = jnp.dot(
        between.reshape(devices * devices, devices).astype(jnp.float32),
        logs,
        precision=HIGHEST_PRECISION,
    ).reshape(devices, devices, part)
    earlier = at[None, :, None] < at[:, None, None]
    factors = jnp.where(earlier, jnp.exp(spans), 0.0)
    prefix = jnp.einsum("rqc,qcv->rcv", factors, updates, precision=HIGHEST_PRECISION)
    returned = exchanged(prefix.astype(jnp.bfloat16), EP)
    return returned.astype(jnp.float32).reshape(channels, width)


def mixer_half(
    recurrence_query_input,
    forget_gate_input,
    recurrence_value_input,
    output_gate_input,
    forget_lower_margin,
    position_decay_extra,
    head_norm_gain,
    recurrence_out_weight,
):
    length = recurrence_query_input.shape[0]
    head_tensor = position_decay_extra.shape[1]
    blocks = length // BLK
    queries = jax.nn.silu(recurrence_query_input.astype(jnp.float32))
    key_gate_value = forget_lower_margin[None, :] * jax.nn.sigmoid(
        -forget_gate_input.astype(jnp.float32)
    )
    decay_logarithm = jnp.log1p(-key_gate_value) + jnp.repeat(
        position_decay_extra, HEAD_CHANNELS, axis=1
    )
    value_rows = recurrence_value_input.astype(jnp.float32)

    def split_heads(tensor):
        return tensor.reshape(blocks, BLK, head_tensor, HEAD_CHANNELS).transpose(2, 0, 1, 3)

    query_heads = split_heads(queries)
    key_heads = split_heads(key_gate_value)
    value_heads = split_heads(value_rows)
    cum_decay = jnp.cumsum(split_heads(decay_logarithm), axis=2)
    middle = cum_decay[:, :, BLK // 2 - 1 : BLK // 2]
    block_end = cum_decay[:, :, BLK - 1 : BLK]
    scores = jnp.einsum(
        "hncd,hnsd->hncs",
        query_heads * jnp.exp(cum_decay - middle),
        key_heads * jnp.exp(middle - cum_decay),
        precision=HIGHEST_PRECISION,
    )
    causal = jnp.tril(jnp.ones((BLK, BLK), dtype=bool))
    scores = jnp.where(causal, scores, 0.0)
    within = jnp.einsum("hncs,hnse->hnce", scores, value_heads, precision=HIGHEST_PRECISION)
    updates = jnp.einsum(
        "hncd,hnce->nhde",
        key_heads * jnp.exp(block_end - cum_decay),
        value_heads,
        precision=HIGHEST_PRECISION,
    )
    block_log = block_end[:, :, 0, :]
    block_decay = jnp.exp(block_log).transpose(1, 0, 2)

    def advance(carry_state, inputs):
        factor, update = inputs
        return (factor[..., None] * carry_state + update, carry_state)

    initial = jnp.zeros((head_tensor, HEAD_CHANNELS, HEAD_CHANNELS), jnp.float32)
    local_final, local_starts = lax.scan(advance, initial, (block_decay, updates))
    incoming = entering_state(
        jnp.sum(block_log, axis=1).reshape(-1), local_final.reshape(-1, HEAD_CHANNELS)
    ).reshape(head_tensor, HEAD_CHANNELS, HEAD_CHANNELS)
    before = jnp.exp(jnp.cumsum(block_log, axis=1) - block_log).transpose(1, 0, 2)
    starts = local_starts + before[..., None] * incoming[None]
    carried = jnp.einsum(
        "hncd,nhde->hnce", query_heads * jnp.exp(cum_decay), starts, precision=HIGHEST_PRECISION
    )
    outputs = (within + carried).transpose(1, 2, 0, 3).reshape(length, head_tensor, HEAD_CHANNELS)
    factor = lax.rsqrt(jnp.mean(outputs * outputs, axis=2, keepdims=True) + EPSILON)
    normed = (outputs * factor).reshape(length, head_tensor * HEAD_CHANNELS) * head_norm_gain[
        None, :
    ]
    gated_rows = (normed * jax.nn.silu(output_gate_input.astype(jnp.float32))).astype(jnp.bfloat16)
    partial = jnp.dot(gated_rows, recurrence_out_weight, preferred_element_type=jnp.float32)
    return summed_to_owners(partial, "tp").astype(jnp.bfloat16)


VMEM = pl.BlockSpec(memory_space=pltpu.VMEM)
SMEM = pl.BlockSpec(memory_space=pltpu.SMEM)


def in_vmem(kernel, shapes, *operands):
    member = lax.axis_index("tp")
    place = jnp.stack([member >> 1, member & 1])
    return pl.pallas_call(
        kernel,
        out_shape=shapes,
        in_specs=[SMEM] + [VMEM] * len(operands),
        out_specs=jax.tree.map(lambda _: VMEM, shapes),
    )(place, *operands)


def select_kernel(experts, place, hidden_state, gain, index, normed, outgoing):
    tokens, top = index.shape
    slots, width = outgoing.shape
    half = slots // experts
    features = hidden_state[...].astype(jnp.float32)
    factor = lax.rsqrt(jnp.mean(features * features, axis=1, keepdims=True) + EPSILON)
    normed[...] = (features * factor * gain[...]).astype(jnp.bfloat16)
    expert = lax.broadcasted_iota(jnp.int32, (tokens, experts), 1)
    named = [index[:, j : j + 1] == expert for j in range(top)]
    chosen = named[0]
    for other in named[1:]:
        chosen = chosen | other
    earlier = lax.broadcasted_iota(jnp.int32, (tokens, tokens), 1) < lax.broadcasted_iota(
        jnp.int32, (tokens, tokens), 0
    )
    one = jnp.float32(1)
    zero = jnp.float32(0)
    places = jnp.dot(
        jnp.where(earlier, one, zero).astype(jnp.bfloat16),
        jnp.where(chosen, one, zero).astype(jnp.bfloat16),
        preferred_element_type=jnp.float32,
    )
    places = jnp.where(chosen, places, -one).astype(jnp.bfloat16)
    slot = lax.broadcasted_iota(jnp.int32, (experts, slots), 1)
    spread = jnp.where(
        slot // half == lax.broadcasted_iota(jnp.int32, (experts, slots), 0), one, zero
    ).astype(jnp.bfloat16)
    wanted = jnp.dot(places, spread, preferred_element_type=jnp.float32).astype(jnp.int32)
    own = lax.broadcasted_iota(jnp.int32, (tokens, slots), 1) % half + place[1] * half
    filled = jnp.where(wanted == own, one, zero).astype(jnp.bfloat16)
    start = pl.multiple_of(place[0] * width, width)
    outgoing[...] = lax.dot_general(
        filled,
        normed[:, pl.ds(start, width)],
        (((0,), (0,)), ((), ())),
        preferred_element_type=jnp.float32,
    ).astype(jnp.bfloat16)


def around_product(place, pieces, matrix):
    own, before, after, far_first, far_second = pieces
    depth = own.shape[1]
    count = matrix.shape[0] // depth

    def block(step):
        start = pl.multiple_of(((place[0] + step) & (count - 1)) * depth, depth)
        return matrix[pl.ds(start, depth), :]

    def dot(piece, step):
        return jnp.dot(piece, block(step), preferred_element_type=jnp.float32)

    near = dot(own[...], 0) + dot(before[...], -1) + dot(after[...], 1)
    middle = far_first.shape[0]
    return (near[:middle] + dot(far_first[...], 2), near[middle:] + dot(far_second[...], 2))


def hidden_kernel(place, own, before, after, far_first, far_second, own_in, partner_in, hidden):
    pieces = (own, before, after, far_first, far_second)
    units = own_in.shape[1] // 2
    middle = far_first.shape[0]
    sides = []
    for matrix in (own_in, partner_in):
        sides.append(
            [
                (jax.nn.silu(both[:, :units]) * both[:, units:]).astype(jnp.bfloat16)
                for both in around_product(place, pieces, matrix)
            ]
        )
    even = place[1] == 0
    for k in range(2):
        rows = pl.ds(k * middle, middle)
        hidden[rows, :units] = jnp.where(even, sides[0][k], sides[1][k])
        hidden[rows, units:] = jnp.where(even, sides[1][k], sides[0][k])


def down_kernel(place, own, before, after, far_first, far_second, own_down, partner_down, answers):
    pieces = (own, before, after, far_first, far_second)
    middle = far_first.shape[0]
    width = own_down.shape[1]
    for side, matrix in enumerate((own_down, partner_down)):
        for k, part in enumerate(around_product(place, pieces, matrix)):
            answers[pl.ds(k * middle, middle), pl.ds(side * width, width)] = part.astype(
                jnp.bfloat16
            )


def expert_half(
    expert_hidden_state,
    chosen_expert_index,
    chosen_expert_score,
    expert_norm_gain,
    routed_gate_weight,
    routed_up_weight,
    routed_down_weight,
    shared_gate_weight,
    shared_up_weight,
    shared_down_weight,
):
    tokens, top = chosen_expert_index.shape
    local_experts = routed_gate_weight.shape[0]
    devices = lax.axis_size(EP)
    experts = local_experts * devices
    capacity = min(tokens, 2 * tokens * top // experts)
    width_out = routed_down_weight.shape[2]
    members = lax.axis_size("tp")
    quads = members // 2
    member = lax.axis_index("tp")
    parity = member & 1
    half = capacity // 2
    width_in = routed_gate_weight.shape[1] // quads
    units = routed_gate_weight.shape[2]

    own_in = jnp.concatenate([routed_gate_weight[0], routed_up_weight[0]], axis=1)
    own_down = routed_down_weight[0]
    partner_in = swapped(own_in, "tp", 1)
    partner_down = swapped(own_down, "tp", 1)

    normed, outgoing = in_vmem(
        functools.partial(select_kernel, experts),
        (
            jax.ShapeDtypeStruct(expert_hidden_state.shape, jnp.bfloat16),
            jax.ShapeDtypeStruct((experts * half, width_in), jnp.bfloat16),
        ),
        expert_hidden_state,
        expert_norm_gain[None, :],
        chosen_expert_index,
    )
    arrived = exchanged(outgoing.reshape(devices, half, width_in), EP)
    chunk = arrived.reshape(devices * half, width_in)
    middle = chunk.shape[0] // 2

    gates = ROUTED_SCALE * chosen_expert_score / jnp.sum(chosen_expert_score, axis=1, keepdims=True)
    named = chosen_expert_index[:, :, None] == jnp.arange(experts, dtype=jnp.int32)[None, None, :]
    chosen = jnp.any(named, axis=1)
    gate_of = jnp.sum(jnp.where(named, gates[:, :, None], 0.0), axis=1)
    row = jnp.arange(tokens)
    places = jnp.dot(
        (row[None, :] < row[:, None]).astype(jnp.bfloat16),
        chosen.astype(jnp.bfloat16),
        preferred_element_type=jnp.float32,
    )
    places = jnp.where(chosen, places.astype(jnp.int32), -1)
    filled = places[:, :, None] == parity * half + jnp.arange(half)[None, None, :]
    filled = filled.reshape(tokens, experts * half)
    shared_hidden = (
        jax.nn.silu(jnp.dot(normed, shared_gate_weight, preferred_element_type=jnp.float32))
        * jnp.dot(normed, shared_up_weight, preferred_element_type=jnp.float32)
    ).astype(jnp.bfloat16)
    shared_piece = gathered_columns(shared_hidden, "tp")
    shared = jnp.dot(
        shared_piece,
        rows_by_reversed_bits(shared_down_weight, members),
        preferred_element_type=jnp.float32,
    )

    def all_around(piece):
        before = shifted(piece, "tp", 2)
        after = shifted(piece, "tp", -2)
        far = [shifted(before[:middle], "tp", 2), shifted(after[middle:], "tp", -2)]
        return (piece, before, after, *far)

    hidden = in_vmem(
        hidden_kernel,
        jax.ShapeDtypeStruct((chunk.shape[0], 2 * units), jnp.bfloat16),
        *all_around(chunk),
        own_in,
        partner_in,
    )
    answers = in_vmem(
        down_kernel,
        jax.ShapeDtypeStruct((chunk.shape[0], 2 * width_out), jnp.bfloat16),
        *all_around(hidden),
        own_down,
        partner_down,
    )
    returned = exchanged(answers.reshape(devices, half, 2 * width_out), EP)
    returned = returned.reshape(experts * half, 2 * width_out)
    mixing = jnp.where(filled.reshape(tokens, experts, half), gate_of[:, :, None], 0.0)
    mixing = mixing.reshape(tokens, experts * half)
    combined = sum(
        jnp.dot(part, returned, preferred_element_type=jnp.float32) for part in in_parts(mixing, 3)
    )
    other = swapped(combined[:, width_out:].astype(jnp.bfloat16), "tp", 1)
    combined = shared + combined[:, :width_out] + other.astype(jnp.float32)
    return combined.astype(jnp.bfloat16)


def per_device(
    recurrence_query_input,
    forget_gate_input,
    recurrence_value_input,
    output_gate_input,
    forget_lower_margin,
    position_decay_extra,
    head_norm_gain,
    recurrence_out_weight,
    expert_hidden_state,
    chosen_expert_index,
    chosen_expert_score,
    expert_norm_gain,
    routed_gate_weight,
    routed_up_weight,
    routed_down_weight,
    shared_gate_weight,
    shared_up_weight,
    shared_down_weight,
):
    recurrence_output = mixer_half(
        recurrence_query_input,
        forget_gate_input,
        recurrence_value_input,
        output_gate_input,
        forget_lower_margin,
        position_decay_extra,
        head_norm_gain,
        recurrence_out_weight,
    )
    expert_out = expert_half(
        expert_hidden_state,
        chosen_expert_index,
        chosen_expert_score,
        expert_norm_gain,
        routed_gate_weight,
        routed_up_weight,
        routed_down_weight,
        shared_gate_weight,
        shared_up_weight,
        shared_down_weight,
    )
    return (recurrence_output, expert_out)


def solution(mesh):
    split = Mesh(
        mesh.devices.reshape(mesh.shape["grp"], 16, 2, mesh.shape["tp"]),
        ("grp", "ep_0", "ep_1", "tp"),
    )
    in_specs = (
        P(GRP_EP, "tp"),
        P(GRP_EP, "tp"),
        P(GRP_EP, "tp"),
        P(GRP_EP, "tp"),
        P("tp"),
        P(GRP_EP, "tp"),
        P("tp"),
        P("tp", None),
        P(GRP_EP, None),
        P(GRP_EP, None),
        P(GRP_EP, None),
        P(),
        P(EP, None, "tp"),
        P(EP, None, "tp"),
        P(EP, None, "tp"),
        P(None, "tp"),
        P(None, "tp"),
        P(None, "tp"),
    )
    out_specs = (P(GRP_EP_TP, None), P(GRP_EP, "tp"))

    return jax.shard_map(
        per_device, mesh=split, in_specs=in_specs, out_specs=out_specs, check_vma=False
    )
```

```python
import functools

import jax
import jax.numpy as jnp
from jax import lax
from jax.experimental import pallas as pl
from jax.experimental.pallas import tpu as pltpu
from jax.sharding import Mesh
from jax.sharding import PartitionSpec as P


HEAD_CHANNELS = 128
BLK = 64
EP = ("ep_0", "ep_1")
GRP_EP = ("grp", "ep_0", "ep_1")
GRP_EP_TP = ("grp", "ep_0", "ep_1", "tp")


EPSILON = 1e-06
ROUTED_SCALE = 2.5
HIGHEST_PRECISION = lax.Precision.HIGHEST


def shifted(array, axis, step):
    count = lax.axis_size(axis)
    return lax.ppermute(array, axis, [(i, (i + step) % count) for i in range(count)])


def swapped(array, axis, bit):
    count = lax.axis_size(axis)
    return lax.ppermute(array, axis, [(i, i ^ bit) for i in range(count)])


def exchanged(array, axis):
    return lax.all_to_all(array, axis, split_axis=0, concat_axis=0, tiled=True)


def half_of(array, dim, place):
    return lax.dynamic_index_in_dim(array, place, dim, keepdims=False)


def summed_to_owners(array, axis):
    count = lax.axis_size(axis)
    bits = count.bit_length() - 1
    member = lax.axis_index(axis)
    kept = array.reshape(*[2] * bits, -1, array.shape[1])
    for bit in range(bits):
        mine = (member >> bit) & 1
        dim = bits - 1 - bit
        arrived = swapped(half_of(kept, dim, 1 - mine).astype(jnp.bfloat16), axis, 1 << bit)
        kept = half_of(kept, dim, mine) + arrived.astype(jnp.float32)
    return kept


def gathered_columns(array, axis):
    count = lax.axis_size(axis)
    member = lax.axis_index(axis)
    for bit in reversed(range(count.bit_length() - 1)):
        arrived = swapped(array, axis, 1 << bit)
        first = ((member >> bit) & 1) == 0
        array = jnp.concatenate(
            [jnp.where(first, array, arrived), jnp.where(first, arrived, array)], axis=1
        )
    return array


def rows_by_reversed_bits(matrix, count):
    bits = count.bit_length() - 1
    split = matrix.reshape(*[2] * bits, -1, matrix.shape[1])
    order = (*reversed(range(bits)), bits, bits + 1)
    return split.transpose(order).reshape(matrix.shape)


def in_parts(array, count):
    parts, rest = [], array
    for _ in range(count):
        rounded = lax.reduce_precision(rest, 8, 7)
        parts.append(rounded.astype(jnp.bfloat16))
        rest = rest - rounded
    return parts


def entering_state(log_decay, state):
    devices = lax.axis_size(EP)
    channels, width = state.shape
    part = channels // devices
    logs = jnp.stack(in_parts(log_decay, 3), axis=-1).reshape(devices, part, 3)
    logs = jnp.pad(logs, ((0, 0), (0, 0), (0, HEAD_CHANNELS - 3)))
    packed = jnp.concatenate(
        [state.astype(jnp.bfloat16).reshape(devices, part, width), logs], axis=2
    )
    arrived = exchanged(packed, EP)
    arrived = arrived.astype(jnp.float32)
    updates = arrived[:, :, :width]
    logs = jnp.sum(arrived[:, :, width : width + 3], axis=2)
    at = jnp.arange(devices)
    between = (at[None, None, :] > at[None, :, None]) & (at[None, None, :] < at[:, None, None])
    spans = jnp.dot(
        between.reshape(devices * devices, devices).astype(jnp.float32),
        logs,
        precision=HIGHEST_PRECISION,
    ).reshape(devices, devices, part)
    earlier = at[None, :, None] < at[:, None, None]
    factors = jnp.where(earlier, jnp.exp(spans), 0.0)
    prefix = jnp.einsum("rqc,qcv->rcv", factors, updates, precision=HIGHEST_PRECISION)
    returned = exchanged(prefix.astype(jnp.bfloat16), EP)
    return returned.astype(jnp.float32).reshape(channels, width)


def mixer_half(
    recurrence_query_input,
    forget_gate_input,
    recurrence_value_input,
    output_gate_input,
    forget_lower_margin,
    position_decay_extra,
    head_norm_gain,
    recurrence_out_weight,
):
    length = recurrence_query_input.shape[0]
    head_tensor = position_decay_extra.shape[1]
    blocks = length // BLK
    queries = jax.nn.silu(recurrence_query_input.astype(jnp.float32))
    key_gate_value = forget_lower_margin[None, :] * jax.nn.sigmoid(
        -forget_gate_input.astype(jnp.float32)
    )
    decay_logarithm = jnp.log1p(-key_gate_value) + jnp.repeat(
        position_decay_extra, HEAD_CHANNELS, axis=1
    )
    value_rows = recurrence_value_input.astype(jnp.float32)

    def split_heads(tensor):
        return tensor.reshape(blocks, BLK, head_tensor, HEAD_CHANNELS).transpose(2, 0, 1, 3)

    query_heads = split_heads(queries)
    key_heads = split_heads(key_gate_value)
    value_heads = split_heads(value_rows)
    cum_decay = jnp.cumsum(split_heads(decay_logarithm), axis=2)
    middle = cum_decay[:, :, BLK // 2 - 1 : BLK // 2]
    block_end = cum_decay[:, :, BLK - 1 : BLK]
    scores = jnp.einsum(
        "hncd,hnsd->hncs",
        query_heads * jnp.exp(cum_decay - middle),
        key_heads * jnp.exp(middle - cum_decay),
        precision=HIGHEST_PRECISION,
    )
    causal = jnp.tril(jnp.ones((BLK, BLK), dtype=bool))
    scores = jnp.where(causal, scores, 0.0)
    within = jnp.einsum("hncs,hnse->hnce", scores, value_heads, precision=HIGHEST_PRECISION)
    updates = jnp.einsum(
        "hncd,hnce->nhde",
        key_heads * jnp.exp(block_end - cum_decay),
        value_heads,
        precision=HIGHEST_PRECISION,
    )
    block_log = block_end[:, :, 0, :]
    block_decay = jnp.exp(block_log).transpose(1, 0, 2)

    def advance(carry_state, inputs):
        factor, update = inputs
        return (factor[..., None] * carry_state + update, carry_state)

    initial = jnp.zeros((head_tensor, HEAD_CHANNELS, HEAD_CHANNELS), jnp.float32)
    local_final, local_starts = lax.scan(advance, initial, (block_decay, updates))
    incoming = entering_state(
        jnp.sum(block_log, axis=1).reshape(-1), local_final.reshape(-1, HEAD_CHANNELS)
    ).reshape(head_tensor, HEAD_CHANNELS, HEAD_CHANNELS)
    before = jnp.exp(jnp.cumsum(block_log, axis=1) - block_log).transpose(1, 0, 2)
    starts = local_starts + before[..., None] * incoming[None]
    carried = jnp.einsum(
        "hncd,nhde->hnce", query_heads * jnp.exp(cum_decay), starts, precision=HIGHEST_PRECISION
    )
    outputs = (within + carried).transpose(1, 2, 0, 3).reshape(length, head_tensor, HEAD_CHANNELS)
    factor = lax.rsqrt(jnp.mean(outputs * outputs, axis=2, keepdims=True) + EPSILON)
    normed = (outputs * factor).reshape(length, head_tensor * HEAD_CHANNELS) * head_norm_gain[
        None, :
    ]
    gated_rows = (normed * jax.nn.silu(output_gate_input.astype(jnp.float32))).astype(jnp.bfloat16)
    partial = jnp.dot(gated_rows, recurrence_out_weight, preferred_element_type=jnp.float32)
    return summed_to_owners(partial, "tp").astype(jnp.bfloat16)


VMEM = pl.BlockSpec(memory_space=pltpu.VMEM)


def in_vmem(kernel, shapes, *operands):
    return pl.pallas_call(
        kernel,
        out_shape=shapes,
        in_specs=[VMEM] * len(operands),
        out_specs=jax.tree.map(lambda _: VMEM, shapes),
    )(*operands)


def select_kernel(experts, hidden_state, gain, index, normed, outgoing):
    top, tokens = index.shape
    slots, width = outgoing.shape
    half = slots // experts
    member = lax.axis_index("tp")
    features = hidden_state[...].astype(jnp.float32)
    factor = lax.rsqrt(jnp.mean(features * features, axis=1, keepdims=True) + EPSILON)
    normed[...] = (features * factor * gain[...]).astype(jnp.bfloat16)
    expert = lax.broadcasted_iota(jnp.int32, (experts, tokens), 0)
    chosen = index[0:1, :] == expert
    for j in range(1, top):
        chosen = chosen | (index[j : j + 1, :] == expert)
    earlier = lax.broadcasted_iota(jnp.int32, (tokens, tokens), 0) < lax.broadcasted_iota(
        jnp.int32, (tokens, tokens), 1
    )
    one = jnp.float32(1)
    zero = jnp.float32(0)
    places = jnp.dot(
        jnp.where(chosen, one, zero).astype(jnp.bfloat16),
        jnp.where(earlier, one, zero).astype(jnp.bfloat16),
        preferred_element_type=jnp.float32,
    )
    places = jnp.where(chosen, places, -one).astype(jnp.bfloat16)
    slot = lax.broadcasted_iota(jnp.int32, (slots, experts), 0)
    spread = jnp.where(
        slot // half == lax.broadcasted_iota(jnp.int32, (slots, experts), 1), one, zero
    ).astype(jnp.bfloat16)
    wanted = jnp.dot(spread, places, preferred_element_type=jnp.float32).astype(jnp.int32)
    own = lax.broadcasted_iota(jnp.int32, (slots, tokens), 0) % half + (member & 1) * half
    filled = jnp.where(wanted == own, one, zero).astype(jnp.bfloat16)
    start = pl.multiple_of((member >> 1) * width, width)
    outgoing[...] = jnp.dot(
        filled, normed[:, pl.ds(start, width)], preferred_element_type=jnp.float32
    ).astype(jnp.bfloat16)


def around_product(pieces, matrix):
    own, before, after, far_first, far_second = pieces
    depth = own.shape[1]
    count = matrix.shape[0] // depth
    quad = lax.axis_index("tp") >> 1

    def block(step):
        start = pl.multiple_of(((quad + step) & (count - 1)) * depth, depth)
        return matrix[pl.ds(start, depth), :]

    def dot(piece, step):
        return jnp.dot(piece, block(step), preferred_element_type=jnp.float32)

    near = dot(own[...], 0) + dot(before[...], -1) + dot(after[...], 1)
    middle = far_first.shape[0]
    return (near[:middle] + dot(far_first[...], 2), near[middle:] + dot(far_second[...], 2))


def hidden_kernel(
    own, before, after, far_first, far_second, own_in, partner_in, hidden, hidden_first, hidden_second
):
    pieces = (own, before, after, far_first, far_second)
    units = own_in.shape[1] // 2
    middle = far_first.shape[0]
    sides = []
    for matrix in (own_in, partner_in):
        sides.append(
            [
                (jax.nn.silu(both[:, :units]) * both[:, units:]).astype(jnp.bfloat16)
                for both in around_product(pieces, matrix)
            ]
        )
    even = (lax.axis_index("tp") & 1) == 0
    for k, part in enumerate((hidden_first, hidden_second)):
        part[:, :units] = jnp.where(even, sides[0][k], sides[1][k])
        part[:, units:] = jnp.where(even, sides[1][k], sides[0][k])
        hidden[pl.ds(k * middle, middle), :] = part[...]


def down_kernel(own, before, after, far_first, far_second, own_down, partner_down, answers):
    pieces = (own, before, after, far_first, far_second)
    middle = far_first.shape[0]
    width = own_down.shape[1]
    for side, matrix in enumerate((own_down, partner_down)):
        for k, part in enumerate(around_product(pieces, matrix)):
            answers[pl.ds(k * middle, middle), pl.ds(side * width, width)] = part.astype(
                jnp.bfloat16
            )


def expert_half(
    expert_hidden_state,
    chosen_expert_index,
    chosen_expert_score,
    expert_norm_gain,
    routed_gate_weight,
    routed_up_weight,
    routed_down_weight,
    shared_gate_weight,
    shared_up_weight,
    shared_down_weight,
):
    tokens, top = chosen_expert_index.shape
    local_experts = routed_gate_weight.shape[0]
    devices = lax.axis_size(EP)
    experts = local_experts * devices
    capacity = min(tokens, 2 * tokens * top // experts)
    width_out = routed_down_weight.shape[2]
    members = lax.axis_size("tp")
    quads = members // 2
    member = lax.axis_index("tp")
    parity = member & 1
    half = capacity // 2
    width_in = routed_gate_weight.shape[1] // quads
    units = routed_gate_weight.shape[2]

    own_in = jnp.concatenate([routed_gate_weight[0], routed_up_weight[0]], axis=1)
    own_down = routed_down_weight[0]
    partner_in = swapped(own_in, "tp", 1)
    partner_down = swapped(own_down, "tp", 1)

    normed, outgoing = in_vmem(
        functools.partial(select_kernel, experts),
        (
            jax.ShapeDtypeStruct(expert_hidden_state.shape, jnp.bfloat16),
            jax.ShapeDtypeStruct((experts * half, width_in), jnp.bfloat16),
        ),
        expert_hidden_state,
        expert_norm_gain[None, :],
        chosen_expert_index.T,
    )
    arrived = exchanged(outgoing.reshape(devices, half, width_in), EP)
    chunk = arrived.reshape(devices * half, width_in)
    middle = chunk.shape[0] // 2

    gates = ROUTED_SCALE * chosen_expert_score / jnp.sum(chosen_expert_score, axis=1, keepdims=True)
    named = chosen_expert_index[:, :, None] == jnp.arange(experts, dtype=jnp.int32)[None, None, :]
    chosen = jnp.any(named, axis=1)
    gate_of = jnp.sum(jnp.where(named, gates[:, :, None], 0.0), axis=1)
    row = jnp.arange(tokens)
    places = jnp.dot(
        (row[None, :] < row[:, None]).astype(jnp.bfloat16),
        chosen.astype(jnp.bfloat16),
        preferred_element_type=jnp.float32,
    )
    places = jnp.where(chosen, places.astype(jnp.int32), -1)
    filled = places[:, :, None] == parity * half + jnp.arange(half)[None, None, :]
    filled = filled.reshape(tokens, experts * half)
    shared_hidden = (
        jax.nn.silu(jnp.dot(normed, shared_gate_weight, preferred_element_type=jnp.float32))
        * jnp.dot(normed, shared_up_weight, preferred_element_type=jnp.float32)
    ).astype(jnp.bfloat16)
    shared_piece = gathered_columns(shared_hidden, "tp")
    shared = jnp.dot(
        shared_piece,
        rows_by_reversed_bits(shared_down_weight, members),
        preferred_element_type=jnp.float32,
    )

    before = shifted(chunk, "tp", 2)
    after = shifted(chunk, "tp", -2)
    far = [shifted(before[:middle], "tp", 2), shifted(after[middle:], "tp", -2)]
    part_shape = jax.ShapeDtypeStruct((middle, 2 * units), jnp.bfloat16)
    hidden, hidden_first, hidden_second = in_vmem(
        hidden_kernel,
        (jax.ShapeDtypeStruct((chunk.shape[0], 2 * units), jnp.bfloat16), part_shape, part_shape),
        chunk,
        before,
        after,
        *far,
        own_in,
        partner_in,
    )
    far = [shifted(hidden_first, "tp", 4), shifted(hidden_second, "tp", -4)]
    before = shifted(hidden, "tp", 2)
    after = shifted(hidden, "tp", -2)
    answers = in_vmem(
        down_kernel,
        jax.ShapeDtypeStruct((chunk.shape[0], 2 * width_out), jnp.bfloat16),
        hidden,
        before,
        after,
        *far,
        own_down,
        partner_down,
    )
    returned = exchanged(answers.reshape(devices, half, 2 * width_out), EP)
    returned = returned.reshape(experts * half, 2 * width_out)
    mixing = jnp.where(filled.reshape(tokens, experts, half), gate_of[:, :, None], 0.0)
    mixing = mixing.reshape(tokens, experts * half)
    combined = sum(
        jnp.dot(part, returned, preferred_element_type=jnp.float32) for part in in_parts(mixing, 3)
    )
    other = swapped(combined[:, width_out:].astype(jnp.bfloat16), "tp", 1)
    combined = shared + combined[:, :width_out] + other.astype(jnp.float32)
    return combined.astype(jnp.bfloat16)


def per_device(
    recurrence_query_input,
    forget_gate_input,
    recurrence_value_input,
    output_gate_input,
    forget_lower_margin,
    position_decay_extra,
    head_norm_gain,
    recurrence_out_weight,
    expert_hidden_state,
    chosen_expert_index,
    chosen_expert_score,
    expert_norm_gain,
    routed_gate_weight,
    routed_up_weight,
    routed_down_weight,
    shared_gate_weight,
    shared_up_weight,
    shared_down_weight,
):
    recurrence_output = mixer_half(
        recurrence_query_input,
        forget_gate_input,
        recurrence_value_input,
        output_gate_input,
        forget_lower_margin,
        position_decay_extra,
        head_norm_gain,
        recurrence_out_weight,
    )
    expert_out = expert_half(
        expert_hidden_state,
        chosen_expert_index,
        chosen_expert_score,
        expert_norm_gain,
        routed_gate_weight,
        routed_up_weight,
        routed_down_weight,
        shared_gate_weight,
        shared_up_weight,
        shared_down_weight,
    )
    return (recurrence_output, expert_out)


def solution(mesh):
    split = Mesh(
        mesh.devices.reshape(mesh.shape["grp"], 16, 2, mesh.shape["tp"]),
        ("grp", "ep_0", "ep_1", "tp"),
    )
    in_specs = (
        P(GRP_EP, "tp"),
        P(GRP_EP, "tp"),
        P(GRP_EP, "tp"),
        P(GRP_EP, "tp"),
        P("tp"),
        P(GRP_EP, "tp"),
        P("tp"),
        P("tp", None),
        P(GRP_EP, None),
        P(GRP_EP, None),
        P(GRP_EP, None),
        P(),
        P(EP, None, "tp"),
        P(EP, None, "tp"),
        P(EP, None, "tp"),
        P(None, "tp"),
        P(None, "tp"),
        P(None, "tp"),
    )
    out_specs = (P(GRP_EP_TP, None), P(GRP_EP, "tp"))

    return jax.shard_map(
        per_device, mesh=split, in_specs=in_specs, out_specs=out_specs, check_vma=False
    )
```

```python
import functools

import jax
import jax.numpy as jnp
from jax import lax
from jax.experimental import pallas as pl
from jax.experimental.pallas import tpu as pltpu
from jax.sharding import Mesh
from jax.sharding import PartitionSpec as P


HEAD_CHANNELS = 128
BLK = 64
EP = ("ep_0", "ep_1")
GRP_EP = ("grp", "ep_0", "ep_1")
GRP_EP_TP = ("grp", "ep_0", "ep_1", "tp")


EPSILON = 1e-06
ROUTED_SCALE = 2.5
HIGHEST_PRECISION = lax.Precision.HIGHEST


def shifted(array, axis, step):
    count = lax.axis_size(axis)
    return lax.ppermute(array, axis, [(i, (i + step) % count) for i in range(count)])


def swapped(array, axis, bit):
    count = lax.axis_size(axis)
    return lax.ppermute(array, axis, [(i, i ^ bit) for i in range(count)])


def exchanged(array, axis):
    return lax.all_to_all(array, axis, split_axis=0, concat_axis=0, tiled=True)


def half_of(array, dim, place):
    return lax.dynamic_index_in_dim(array, place, dim, keepdims=False)


def summed_to_owners(array, axis):
    count = lax.axis_size(axis)
    bits = count.bit_length() - 1
    member = lax.axis_index(axis)
    kept = array.reshape(*[2] * bits, -1, array.shape[1])
    for bit in range(bits):
        mine = (member >> bit) & 1
        dim = bits - 1 - bit
        arrived = swapped(half_of(kept, dim, 1 - mine).astype(jnp.bfloat16), axis, 1 << bit)
        kept = half_of(kept, dim, mine) + arrived.astype(jnp.float32)
    return kept


def gathered_columns(array, axis):
    count = lax.axis_size(axis)
    member = lax.axis_index(axis)
    for bit in reversed(range(count.bit_length() - 1)):
        arrived = swapped(array, axis, 1 << bit)
        first = ((member >> bit) & 1) == 0
        array = jnp.concatenate(
            [jnp.where(first, array, arrived), jnp.where(first, arrived, array)], axis=1
        )
    return array


def rows_by_reversed_bits(matrix, count):
    bits = count.bit_length() - 1
    split = matrix.reshape(*[2] * bits, -1, matrix.shape[1])
    order = (*reversed(range(bits)), bits, bits + 1)
    return split.transpose(order).reshape(matrix.shape)


def in_parts(array, count):
    parts, rest = [], array
    for _ in range(count):
        rounded = lax.reduce_precision(rest, 8, 7)
        parts.append(rounded.astype(jnp.bfloat16))
        rest = rest - rounded
    return parts


def entering_state(log_decay, state):
    devices = lax.axis_size(EP)
    channels, width = state.shape
    part = channels // devices
    logs = jnp.stack(in_parts(log_decay, 3), axis=-1).reshape(devices, part, 3)
    logs = jnp.pad(logs, ((0, 0), (0, 0), (0, HEAD_CHANNELS - 3)))
    packed = jnp.concatenate(
        [state.astype(jnp.bfloat16).reshape(devices, part, width), logs], axis=2
    )
    arrived = exchanged(packed, EP)
    arrived = arrived.astype(jnp.float32)
    updates = arrived[:, :, :width]
    logs = jnp.sum(arrived[:, :, width : width + 3], axis=2)
    at = jnp.arange(devices)
    between = (at[None, None, :] > at[None, :, None]) & (at[None, None, :] < at[:, None, None])
    spans = jnp.dot(
        between.reshape(devices * devices, devices).astype(jnp.float32),
        logs,
        precision=HIGHEST_PRECISION,
    ).reshape(devices, devices, part)
    earlier = at[None, :, None] < at[:, None, None]
    factors = jnp.where(earlier, jnp.exp(spans), 0.0)
    prefix = jnp.einsum("rqc,qcv->rcv", factors, updates, precision=HIGHEST_PRECISION)
    returned = exchanged(prefix.astype(jnp.bfloat16), EP)
    return returned.astype(jnp.float32).reshape(channels, width)


def mixer_half(
    recurrence_query_input,
    forget_gate_input,
    recurrence_value_input,
    output_gate_input,
    forget_lower_margin,
    position_decay_extra,
    head_norm_gain,
    recurrence_out_weight,
):
    length = recurrence_query_input.shape[0]
    head_tensor = position_decay_extra.shape[1]
    blocks = length // BLK
    queries = jax.nn.silu(recurrence_query_input.astype(jnp.float32))
    key_gate_value = forget_lower_margin[None, :] * jax.nn.sigmoid(
        -forget_gate_input.astype(jnp.float32)
    )
    decay_logarithm = jnp.log1p(-key_gate_value) + jnp.repeat(
        position_decay_extra, HEAD_CHANNELS, axis=1
    )
    value_rows = recurrence_value_input.astype(jnp.float32)

    def split_heads(tensor):
        return tensor.reshape(blocks, BLK, head_tensor, HEAD_CHANNELS).transpose(2, 0, 1, 3)

    query_heads = split_heads(queries)
    key_heads = split_heads(key_gate_value)
    value_heads = split_heads(value_rows)
    cum_decay = jnp.cumsum(split_heads(decay_logarithm), axis=2)
    middle = cum_decay[:, :, BLK // 2 - 1 : BLK // 2]
    block_end = cum_decay[:, :, BLK - 1 : BLK]
    scores = jnp.einsum(
        "hncd,hnsd->hncs",
        query_heads * jnp.exp(cum_decay - middle),
        key_heads * jnp.exp(middle - cum_decay),
        precision=HIGHEST_PRECISION,
    )
    causal = jnp.tril(jnp.ones((BLK, BLK), dtype=bool))
    scores = jnp.where(causal, scores, 0.0)
    within = jnp.einsum("hncs,hnse->hnce", scores, value_heads, precision=HIGHEST_PRECISION)
    updates = jnp.einsum(
        "hncd,hnce->nhde",
        key_heads * jnp.exp(block_end - cum_decay),
        value_heads,
        precision=HIGHEST_PRECISION,
    )
    block_log = block_end[:, :, 0, :]
    block_decay = jnp.exp(block_log).transpose(1, 0, 2)

    def advance(carry_state, inputs):
        factor, update = inputs
        return (factor[..., None] * carry_state + update, carry_state)

    initial = jnp.zeros((head_tensor, HEAD_CHANNELS, HEAD_CHANNELS), jnp.float32)
    local_final, local_starts = lax.scan(advance, initial, (block_decay, updates))
    incoming = entering_state(
        jnp.sum(block_log, axis=1).reshape(-1), local_final.reshape(-1, HEAD_CHANNELS)
    ).reshape(head_tensor, HEAD_CHANNELS, HEAD_CHANNELS)
    before = jnp.exp(jnp.cumsum(block_log, axis=1) - block_log).transpose(1, 0, 2)
    starts = local_starts + before[..., None] * incoming[None]
    carried = jnp.einsum(
        "hncd,nhde->hnce", query_heads * jnp.exp(cum_decay), starts, precision=HIGHEST_PRECISION
    )
    outputs = (within + carried).transpose(1, 2, 0, 3).reshape(length, head_tensor, HEAD_CHANNELS)
    factor = lax.rsqrt(jnp.mean(outputs * outputs, axis=2, keepdims=True) + EPSILON)
    normed = (outputs * factor).reshape(length, head_tensor * HEAD_CHANNELS) * head_norm_gain[
        None, :
    ]
    gated_rows = (normed * jax.nn.silu(output_gate_input.astype(jnp.float32))).astype(jnp.bfloat16)
    partial = jnp.dot(gated_rows, recurrence_out_weight, preferred_element_type=jnp.float32)
    return summed_to_owners(partial, "tp").astype(jnp.bfloat16)


VMEM = pl.BlockSpec(memory_space=pltpu.VMEM)
ANY = pl.BlockSpec(memory_space=pl.ANY)


def in_vmem(kernel, shapes, *operands):
    return pl.pallas_call(
        kernel,
        out_shape=shapes,
        in_specs=[VMEM] * len(operands),
        out_specs=jax.tree.map(lambda _: VMEM, shapes),
    )(*operands)


def fetching(kernel, shapes, *operands):
    count = len(operands)

    def body(*refs):
        sources, rest = refs[:count], refs[count:]
        outputs, held, arrived = rest[: -count - 1], rest[-count - 1 : -1], rest[-1]
        copies = [
            pltpu.make_async_copy(source, target, arrived.at[i])
            for i, (source, target) in enumerate(zip(sources, held))
        ]
        for copy in copies:
            copy.start()

        def fetch(i):
            def ready():
                copies[i].wait()
                return held[i]

            return ready

        kernel(*[fetch(i) for i in range(count)], *outputs)

    return pl.pallas_call(
        body,
        out_shape=shapes,
        in_specs=[ANY] * count,
        out_specs=jax.tree.map(lambda _: VMEM, shapes),
        scratch_shapes=[pltpu.VMEM(a.shape, a.dtype) for a in operands]
        + [pltpu.SemaphoreType.DMA((count,))],
    )(*operands)


def halves_kernel(before, after, first, second, arrived):
    middle = first.shape[0]
    copies = [
        pltpu.make_async_copy(before.at[pl.ds(0, middle), :], first, arrived.at[0]),
        pltpu.make_async_copy(after.at[pl.ds(middle, middle), :], second, arrived.at[1]),
    ]
    for copy in copies:
        copy.start()
    for copy in copies:
        copy.wait()


def far_halves(before, after):
    half = jax.ShapeDtypeStruct((before.shape[0] // 2, before.shape[1]), before.dtype)
    return pl.pallas_call(
        halves_kernel,
        out_shape=(half, half),
        in_specs=[ANY, ANY],
        out_specs=(ANY, ANY),
        scratch_shapes=[pltpu.SemaphoreType.DMA((2,))],
    )(before, after)


def select_kernel(experts, hidden_state, gain, index, normed, outgoing):
    top, tokens = index.shape
    slots, width = outgoing.shape
    half = slots // experts
    member = lax.axis_index("tp")
    features = hidden_state[...].astype(jnp.float32)
    factor = lax.rsqrt(jnp.mean(features * features, axis=1, keepdims=True) + EPSILON)
    normed[...] = (features * factor * gain[...]).astype(jnp.bfloat16)
    expert = lax.broadcasted_iota(jnp.int32, (experts, tokens), 0)
    chosen = index[0:1, :] == expert
    for j in range(1, top):
        chosen = chosen | (index[j : j + 1, :] == expert)
    earlier = lax.broadcasted_iota(jnp.int32, (tokens, tokens), 0) < lax.broadcasted_iota(
        jnp.int32, (tokens, tokens), 1
    )
    one = jnp.float32(1)
    zero = jnp.float32(0)
    places = jnp.dot(
        jnp.where(chosen, one, zero).astype(jnp.bfloat16),
        jnp.where(earlier, one, zero).astype(jnp.bfloat16),
        preferred_element_type=jnp.float32,
    )
    places = jnp.where(chosen, places, -one).astype(jnp.bfloat16)
    slot = lax.broadcasted_iota(jnp.int32, (slots, experts), 0)
    spread = jnp.where(
        slot // half == lax.broadcasted_iota(jnp.int32, (slots, experts), 1), one, zero
    ).astype(jnp.bfloat16)
    wanted = jnp.dot(spread, places, preferred_element_type=jnp.float32).astype(jnp.int32)
    own = lax.broadcasted_iota(jnp.int32, (slots, tokens), 0) % half + (member & 1) * half
    filled = jnp.where(wanted == own, one, zero).astype(jnp.bfloat16)
    start = pl.multiple_of((member >> 1) * width, width)
    outgoing[...] = jnp.dot(
        filled, normed[:, pl.ds(start, width)], preferred_element_type=jnp.float32
    ).astype(jnp.bfloat16)


def around_products(pieces, matrices):
    quad = lax.axis_index("tp") >> 1
    held = []

    def dot(piece, matrix, step):
        depth = piece.shape[1]
        count = matrix.shape[0] // depth
        start = pl.multiple_of(((quad + step) & (count - 1)) * depth, depth)
        return jnp.dot(
            piece[...], matrix[pl.ds(start, depth), :], preferred_element_type=jnp.float32
        )

    near = [None] * len(matrices)
    for fetch, step in zip(pieces[:3], (0, -1, 1)):
        piece = fetch()
        for k, fetch_matrix in enumerate(matrices):
            if step == 0:
                held.append(fetch_matrix())
            part = dot(piece, held[k], step)
            near[k] = part if near[k] is None else near[k] + part
    first, second = (fetch() for fetch in pieces[3:])
    middle = first.shape[0]
    return [
        (part[:middle] + dot(first, matrix, 2), part[middle:] + dot(second, matrix, 2))
        for part, matrix in zip(near, held)
    ]


def hidden_kernel(
    own, before, after, far_first, far_second, own_in, partner_in, hidden, hidden_first, hidden_second
):
    pieces = (own, before, after, far_first, far_second)
    middle, units = (hidden_first.shape[0], hidden_first.shape[1] // 2)
    sides = [
        [
            (jax.nn.silu(both[:, :units]) * both[:, units:]).astype(jnp.bfloat16)
            for both in halves
        ]
        for halves in around_products(pieces, (own_in, partner_in))
    ]
    even = (lax.axis_index("tp") & 1) == 0
    for k, part in enumerate((hidden_first, hidden_second)):
        part[:, :units] = jnp.where(even, sides[0][k], sides[1][k])
        part[:, units:] = jnp.where(even, sides[1][k], sides[0][k])
        hidden[pl.ds(k * middle, middle), :] = part[...]


def down_kernel(own, before, after, far_first, far_second, own_down, partner_down, answers):
    pieces = (own, before, after, far_first, far_second)
    middle, width = (answers.shape[0] // 2, answers.shape[1] // 2)
    for side, halves in enumerate(around_products(pieces, (own_down, partner_down))):
        for k, part in enumerate(halves):
            answers[pl.ds(k * middle, middle), pl.ds(side * width, width)] = part.astype(
                jnp.bfloat16
            )


def expert_half(
    expert_hidden_state,
    chosen_expert_index,
    chosen_expert_score,
    expert_norm_gain,
    routed_gate_weight,
    routed_up_weight,
    routed_down_weight,
    shared_gate_weight,
    shared_up_weight,
    shared_down_weight,
):
    tokens, top = chosen_expert_index.shape
    local_experts = routed_gate_weight.shape[0]
    devices = lax.axis_size(EP)
    experts = local_experts * devices
    capacity = min(tokens, 2 * tokens * top // experts)
    width_out = routed_down_weight.shape[2]
    members = lax.axis_size("tp")
    quads = members // 2
    member = lax.axis_index("tp")
    parity = member & 1
    half = capacity // 2
    width_in = routed_gate_weight.shape[1] // quads
    units = routed_gate_weight.shape[2]

    own_in = jnp.concatenate([routed_gate_weight[0], routed_up_weight[0]], axis=1)
    own_down = routed_down_weight[0]
    partner_in = swapped(own_in, "tp", 1)
    partner_down = swapped(own_down, "tp", 1)

    normed, outgoing = in_vmem(
        functools.partial(select_kernel, experts),
        (
            jax.ShapeDtypeStruct(expert_hidden_state.shape, jnp.bfloat16),
            jax.ShapeDtypeStruct((experts * half, width_in), jnp.bfloat16),
        ),
        expert_hidden_state,
        expert_norm_gain[None, :],
        chosen_expert_index.T,
    )
    arrived = exchanged(outgoing.reshape(devices, half, width_in), EP)
    chunk = arrived.reshape(devices * half, width_in)
    middle = chunk.shape[0] // 2

    gates = ROUTED_SCALE * chosen_expert_score / jnp.sum(chosen_expert_score, axis=1, keepdims=True)
    named = chosen_expert_index[:, :, None] == jnp.arange(experts, dtype=jnp.int32)[None, None, :]
    chosen = jnp.any(named, axis=1)
    gate_of = jnp.sum(jnp.where(named, gates[:, :, None], 0.0), axis=1)
    row = jnp.arange(tokens)
    places = jnp.dot(
        (row[None, :] < row[:, None]).astype(jnp.bfloat16),
        chosen.astype(jnp.bfloat16),
        preferred_element_type=jnp.float32,
    )
    places = jnp.where(chosen, places.astype(jnp.int32), -1)
    filled = places[:, :, None] == parity * half + jnp.arange(half)[None, None, :]
    filled = filled.reshape(tokens, experts * half)
    shared_hidden = (
        jax.nn.silu(jnp.dot(normed, shared_gate_weight, preferred_element_type=jnp.float32))
        * jnp.dot(normed, shared_up_weight, preferred_element_type=jnp.float32)
    ).astype(jnp.bfloat16)
    shared_piece = gathered_columns(shared_hidden, "tp")
    shared = jnp.dot(
        shared_piece,
        rows_by_reversed_bits(shared_down_weight, members),
        preferred_element_type=jnp.float32,
    )

    before = shifted(chunk, "tp", 2)
    after = shifted(chunk, "tp", -2)
    first, second = far_halves(before, after)
    far = [shifted(first, "tp", 2), shifted(second, "tp", -2)]
    part_shape = jax.ShapeDtypeStruct((middle, 2 * units), jnp.bfloat16)
    hidden, hidden_first, hidden_second = fetching(
        hidden_kernel,
        (jax.ShapeDtypeStruct((chunk.shape[0], 2 * units), jnp.bfloat16), part_shape, part_shape),
        chunk,
        before,
        after,
        *far,
        own_in,
        partner_in,
    )
    far = [shifted(hidden_first, "tp", 4), shifted(hidden_second, "tp", -4)]
    before = shifted(hidden, "tp", 2)
    after = shifted(hidden, "tp", -2)
    answers = fetching(
        down_kernel,
        jax.ShapeDtypeStruct((chunk.shape[0], 2 * width_out), jnp.bfloat16),
        hidden,
        before,
        after,
        *far,
        own_down,
        partner_down,
    )
    returned = exchanged(answers.reshape(devices, half, 2 * width_out), EP)
    returned = returned.reshape(experts * half, 2 * width_out)
    mixing = jnp.where(filled.reshape(tokens, experts, half), gate_of[:, :, None], 0.0)
    mixing = mixing.reshape(tokens, experts * half)
    combined = sum(
        jnp.dot(part, returned, preferred_element_type=jnp.float32) for part in in_parts(mixing, 3)
    )
    other = swapped(combined[:, width_out:].astype(jnp.bfloat16), "tp", 1)
    combined = shared + combined[:, :width_out] + other.astype(jnp.float32)
    return combined.astype(jnp.bfloat16)


def per_device(
    recurrence_query_input,
    forget_gate_input,
    recurrence_value_input,
    output_gate_input,
    forget_lower_margin,
    position_decay_extra,
    head_norm_gain,
    recurrence_out_weight,
    expert_hidden_state,
    chosen_expert_index,
    chosen_expert_score,
    expert_norm_gain,
    routed_gate_weight,
    routed_up_weight,
    routed_down_weight,
    shared_gate_weight,
    shared_up_weight,
    shared_down_weight,
):
    recurrence_output = mixer_half(
        recurrence_query_input,
        forget_gate_input,
        recurrence_value_input,
        output_gate_input,
        forget_lower_margin,
        position_decay_extra,
        head_norm_gain,
        recurrence_out_weight,
    )
    expert_out = expert_half(
        expert_hidden_state,
        chosen_expert_index,
        chosen_expert_score,
        expert_norm_gain,
        routed_gate_weight,
        routed_up_weight,
        routed_down_weight,
        shared_gate_weight,
        shared_up_weight,
        shared_down_weight,
    )
    return (recurrence_output, expert_out)


def solution(mesh):
    split = Mesh(
        mesh.devices.reshape(mesh.shape["grp"], 16, 2, mesh.shape["tp"]),
        ("grp", "ep_0", "ep_1", "tp"),
    )
    in_specs = (
        P(GRP_EP, "tp"),
        P(GRP_EP, "tp"),
        P(GRP_EP, "tp"),
        P(GRP_EP, "tp"),
        P("tp"),
        P(GRP_EP, "tp"),
        P("tp"),
        P("tp", None),
        P(GRP_EP, None),
        P(GRP_EP, None),
        P(GRP_EP, None),
        P(),
        P(EP, None, "tp"),
        P(EP, None, "tp"),
        P(EP, None, "tp"),
        P(None, "tp"),
        P(None, "tp"),
        P(None, "tp"),
    )
    out_specs = (P(GRP_EP_TP, None), P(GRP_EP, "tp"))

    return jax.shard_map(
        per_device, mesh=split, in_specs=in_specs, out_specs=out_specs, check_vma=False
    )
```

```python
import functools

import jax
import jax.numpy as jnp
from jax import lax
from jax.experimental import pallas as pl
from jax.experimental.pallas import tpu as pltpu
from jax.sharding import Mesh
from jax.sharding import PartitionSpec as P


HEAD_CHANNELS = 128
BLK = 64
EP = ("ep_0", "ep_1")
GRP_EP = ("grp", "ep_0", "ep_1")
GRP_EP_TP = ("grp", "ep_0", "ep_1", "tp")


EPSILON = 1e-06
ROUTED_SCALE = 2.5
HIGHEST_PRECISION = lax.Precision.HIGHEST


def shifted(array, axis, step):
    count = lax.axis_size(axis)
    return lax.ppermute(array, axis, [(i, (i + step) % count) for i in range(count)])


def swapped(array, axis, bit):
    count = lax.axis_size(axis)
    return lax.ppermute(array, axis, [(i, i ^ bit) for i in range(count)])


def exchanged(array, axis):
    return lax.all_to_all(array, axis, split_axis=0, concat_axis=0, tiled=True)


def half_of(array, dim, place):
    return lax.dynamic_index_in_dim(array, place, dim, keepdims=False)


def summed_to_owners(array, axis):
    count = lax.axis_size(axis)
    bits = count.bit_length() - 1
    member = lax.axis_index(axis)
    kept = array.reshape(*[2] * bits, -1, array.shape[1])
    for bit in range(bits):
        mine = (member >> bit) & 1
        dim = bits - 1 - bit
        arrived = swapped(half_of(kept, dim, 1 - mine).astype(jnp.bfloat16), axis, 1 << bit)
        kept = half_of(kept, dim, mine) + arrived.astype(jnp.float32)
    return kept


def gathered_columns(array, axis):
    count = lax.axis_size(axis)
    member = lax.axis_index(axis)
    for bit in reversed(range(count.bit_length() - 1)):
        arrived = swapped(array, axis, 1 << bit)
        first = ((member >> bit) & 1) == 0
        array = jnp.concatenate(
            [jnp.where(first, array, arrived), jnp.where(first, arrived, array)], axis=1
        )
    return array


def rows_by_reversed_bits(matrix, count):
    bits = count.bit_length() - 1
    split = matrix.reshape(*[2] * bits, -1, matrix.shape[1])
    order = (*reversed(range(bits)), bits, bits + 1)
    return split.transpose(order).reshape(matrix.shape)


def in_parts(array, count):
    parts, rest = [], array
    for _ in range(count):
        rounded = lax.reduce_precision(rest, 8, 7)
        parts.append(rounded.astype(jnp.bfloat16))
        rest = rest - rounded
    return parts


def entering_state(log_decay, state):
    devices = lax.axis_size(EP)
    channels, width = state.shape
    part = channels // devices
    logs = jnp.stack(in_parts(log_decay, 3), axis=-1).reshape(devices, part, 3)
    logs = jnp.pad(logs, ((0, 0), (0, 0), (0, HEAD_CHANNELS - 3)))
    packed = jnp.concatenate(
        [state.astype(jnp.bfloat16).reshape(devices, part, width), logs], axis=2
    )
    arrived = exchanged(packed, EP)
    arrived = arrived.astype(jnp.float32)
    updates = arrived[:, :, :width]
    logs = jnp.sum(arrived[:, :, width : width + 3], axis=2)
    at = jnp.arange(devices)
    between = (at[None, None, :] > at[None, :, None]) & (at[None, None, :] < at[:, None, None])
    spans = jnp.dot(
        between.reshape(devices * devices, devices).astype(jnp.float32),
        logs,
        precision=HIGHEST_PRECISION,
    ).reshape(devices, devices, part)
    earlier = at[None, :, None] < at[:, None, None]
    factors = jnp.where(earlier, jnp.exp(spans), 0.0)
    prefix = jnp.einsum("rqc,qcv->rcv", factors, updates, precision=HIGHEST_PRECISION)
    prefix = prefix.astype(jnp.bfloat16)
    returned = exchanged(prefix, EP)
    return returned.astype(jnp.float32).reshape(channels, width)


def mixer_half(
    recurrence_query_input,
    forget_gate_input,
    recurrence_value_input,
    output_gate_input,
    forget_lower_margin,
    position_decay_extra,
    head_norm_gain,
    recurrence_out_weight,
):
    length = recurrence_query_input.shape[0]
    head_tensor = position_decay_extra.shape[1]
    blocks = length // BLK
    queries = jax.nn.silu(recurrence_query_input.astype(jnp.float32))
    key_gate_value = forget_lower_margin[None, :] * jax.nn.sigmoid(
        -forget_gate_input.astype(jnp.float32)
    )
    decay_logarithm = jnp.log1p(-key_gate_value) + jnp.repeat(
        position_decay_extra, HEAD_CHANNELS, axis=1
    )
    value_rows = recurrence_value_input.astype(jnp.float32)

    def split_heads(tensor):
        return tensor.reshape(blocks, BLK, head_tensor, HEAD_CHANNELS).transpose(2, 0, 1, 3)

    query_heads = split_heads(queries)
    key_heads = split_heads(key_gate_value)
    value_heads = split_heads(value_rows)
    cum_decay = jnp.cumsum(split_heads(decay_logarithm), axis=2)
    middle = cum_decay[:, :, BLK // 2 - 1 : BLK // 2]
    block_end = cum_decay[:, :, BLK - 1 : BLK]
    scores = jnp.einsum(
        "hncd,hnsd->hncs",
        query_heads * jnp.exp(cum_decay - middle),
        key_heads * jnp.exp(middle - cum_decay),
        precision=HIGHEST_PRECISION,
    )
    causal = jnp.tril(jnp.ones((BLK, BLK), dtype=bool))
    scores = jnp.where(causal, scores, 0.0)
    within = jnp.einsum("hncs,hnse->hnce", scores, value_heads, precision=HIGHEST_PRECISION)
    updates = jnp.einsum(
        "hncd,hnce->nhde",
        key_heads * jnp.exp(block_end - cum_decay),
        value_heads,
        precision=HIGHEST_PRECISION,
    )
    block_log = block_end[:, :, 0, :]
    block_decay = jnp.exp(block_log).transpose(1, 0, 2)

    def advance(carry_state, inputs):
        factor, update = inputs
        return (factor[..., None] * carry_state + update, carry_state)

    initial = jnp.zeros((head_tensor, HEAD_CHANNELS, HEAD_CHANNELS), jnp.float32)
    local_final, local_starts = lax.scan(advance, initial, (block_decay, updates))
    incoming = entering_state(
        jnp.sum(block_log, axis=1).reshape(-1), local_final.reshape(-1, HEAD_CHANNELS)
    ).reshape(head_tensor, HEAD_CHANNELS, HEAD_CHANNELS)
    before = jnp.exp(jnp.cumsum(block_log, axis=1) - block_log).transpose(1, 0, 2)
    starts = local_starts + before[..., None] * incoming[None]
    carried = jnp.einsum(
        "hncd,nhde->hnce", query_heads * jnp.exp(cum_decay), starts, precision=HIGHEST_PRECISION
    )
    outputs = (within + carried).transpose(1, 2, 0, 3).reshape(length, head_tensor, HEAD_CHANNELS)
    factor = lax.rsqrt(jnp.mean(outputs * outputs, axis=2, keepdims=True) + EPSILON)
    normed = (outputs * factor).reshape(length, head_tensor * HEAD_CHANNELS) * head_norm_gain[
        None, :
    ]
    gated_rows = (normed * jax.nn.silu(output_gate_input.astype(jnp.float32))).astype(jnp.bfloat16)
    partial = jnp.dot(gated_rows, recurrence_out_weight, preferred_element_type=jnp.float32)
    return summed_to_owners(partial, "tp").astype(jnp.bfloat16)


VMEM = pl.BlockSpec(memory_space=pltpu.VMEM)
ANY = pl.BlockSpec(memory_space=pl.ANY)


def in_vmem(kernel, shapes, *operands):
    return pl.pallas_call(
        kernel,
        out_shape=shapes,
        in_specs=[VMEM] * len(operands),
        out_specs=jax.tree.map(lambda _: VMEM, shapes),
    )(*operands)


def fetching(kernel, shapes, *operands):
    count = len(operands)

    def body(*refs):
        sources, rest = refs[:count], refs[count:]
        outputs, held, arrived = rest[: -count - 1], rest[-count - 1 : -1], rest[-1]
        copies = [
            pltpu.make_async_copy(source, target, arrived.at[i])
            for i, (source, target) in enumerate(zip(sources, held))
        ]
        for copy in copies:
            copy.start()

        def fetch(i):
            def ready():
                copies[i].wait()
                return held[i]

            return ready

        kernel(*[fetch(i) for i in range(count)], *outputs)

    return pl.pallas_call(
        body,
        out_shape=shapes,
        in_specs=[ANY] * count,
        out_specs=jax.tree.map(lambda _: VMEM, shapes),
        scratch_shapes=[pltpu.VMEM(a.shape, a.dtype) for a in operands]
        + [pltpu.SemaphoreType.DMA((count,))],
    )(*operands)


def halves_kernel(whole, first, second):
    middle = first.shape[0]
    first[...] = whole[:middle, :]
    second[...] = whole[middle:, :]


def halves_of(array):
    half = jax.ShapeDtypeStruct((array.shape[0] // 2, array.shape[1]), array.dtype)
    return in_vmem(halves_kernel, (half, half), array)


def select_kernel(experts, hidden_state, gain, index, normed, outgoing):
    top, tokens = index.shape
    slots, width = outgoing.shape
    half = slots // experts
    member = lax.axis_index("tp")
    features = hidden_state[...].astype(jnp.float32)
    factor = lax.rsqrt(jnp.mean(features * features, axis=1, keepdims=True) + EPSILON)
    normed[...] = (features * factor * gain[...]).astype(jnp.bfloat16)
    expert = lax.broadcasted_iota(jnp.int32, (experts, tokens), 0)
    chosen = index[0:1, :] == expert
    for j in range(1, top):
        chosen = chosen | (index[j : j + 1, :] == expert)
    earlier = lax.broadcasted_iota(jnp.int32, (tokens, tokens), 0) < lax.broadcasted_iota(
        jnp.int32, (tokens, tokens), 1
    )
    one = jnp.float32(1)
    zero = jnp.float32(0)
    places = jnp.dot(
        jnp.where(chosen, one, zero).astype(jnp.bfloat16),
        jnp.where(earlier, one, zero).astype(jnp.bfloat16),
        preferred_element_type=jnp.float32,
    )
    places = jnp.where(chosen, places, -one).astype(jnp.bfloat16)
    slot = lax.broadcasted_iota(jnp.int32, (slots, experts), 0)
    spread = jnp.where(
        slot // half == lax.broadcasted_iota(jnp.int32, (slots, experts), 1), one, zero
    ).astype(jnp.bfloat16)
    wanted = jnp.dot(spread, places, preferred_element_type=jnp.float32).astype(jnp.int32)
    own = lax.broadcasted_iota(jnp.int32, (slots, tokens), 0) % half + (member & 1) * half
    filled = jnp.where(wanted == own, one, zero).astype(jnp.bfloat16)
    start = pl.multiple_of((member >> 1) * width, width)
    outgoing[...] = jnp.dot(
        filled, normed[:, pl.ds(start, width)], preferred_element_type=jnp.float32
    ).astype(jnp.bfloat16)


def around_products(pieces, matrices):
    quad = lax.axis_index("tp") >> 1
    held = []

    def dot(piece, matrix, step):
        depth = piece.shape[1]
        count = matrix.shape[0] // depth
        start = pl.multiple_of(((quad + step) & (count - 1)) * depth, depth)
        return jnp.dot(
            piece[...], matrix[pl.ds(start, depth), :], preferred_element_type=jnp.float32
        )

    near = [None] * len(matrices)
    for fetch, step in zip(pieces[:3], (0, -1, 1)):
        piece = fetch()
        for k, fetch_matrix in enumerate(matrices):
            if step == 0:
                held.append(fetch_matrix())
            part = dot(piece, held[k], step)
            near[k] = part if near[k] is None else near[k] + part
    first, second = (fetch() for fetch in pieces[3:])
    middle = first.shape[0]
    return [
        (part[:middle] + dot(first, matrix, 2), part[middle:] + dot(second, matrix, 2))
        for part, matrix in zip(near, held)
    ]


def hidden_kernel(
    own, before, after, far_first, far_second, own_in, partner_in, hidden, hidden_first, hidden_second
):
    pieces = (own, before, after, far_first, far_second)
    middle, units = (hidden_first.shape[0], hidden_first.shape[1] // 2)
    sides = [
        [
            (jax.nn.silu(both[:, :units]) * both[:, units:]).astype(jnp.bfloat16)
            for both in halves
        ]
        for halves in around_products(pieces, (own_in, partner_in))
    ]
    even = (lax.axis_index("tp") & 1) == 0
    for k, part in enumerate((hidden_first, hidden_second)):
        part[:, :units] = jnp.where(even, sides[0][k], sides[1][k])
        part[:, units:] = jnp.where(even, sides[1][k], sides[0][k])
        hidden[pl.ds(k * middle, middle), :] = part[...]


def down_kernel(own, before, after, far_first, far_second, own_down, partner_down, answers):
    pieces = (own, before, after, far_first, far_second)
    middle, width = (answers.shape[0] // 2, answers.shape[1] // 2)
    for side, halves in enumerate(around_products(pieces, (own_down, partner_down))):
        for k, part in enumerate(halves):
            answers[pl.ds(k * middle, middle), pl.ds(side * width, width)] = part.astype(
                jnp.bfloat16
            )


def expert_half(
    expert_hidden_state,
    chosen_expert_index,
    chosen_expert_score,
    expert_norm_gain,
    routed_gate_weight,
    routed_up_weight,
    routed_down_weight,
    shared_gate_weight,
    shared_up_weight,
    shared_down_weight,
):
    tokens, top = chosen_expert_index.shape
    local_experts = routed_gate_weight.shape[0]
    devices = lax.axis_size(EP)
    experts = local_experts * devices
    capacity = min(tokens, 2 * tokens * top // experts)
    width_out = routed_down_weight.shape[2]
    members = lax.axis_size("tp")
    quads = members // 2
    member = lax.axis_index("tp")
    parity = member & 1
    half = capacity // 2
    width_in = routed_gate_weight.shape[1] // quads
    units = routed_gate_weight.shape[2]

    own_in = jnp.concatenate([routed_gate_weight[0], routed_up_weight[0]], axis=1)
    own_down = routed_down_weight[0]
    partner_in = swapped(own_in, "tp", 1)
    partner_down = swapped(own_down, "tp", 1)

    normed, outgoing = in_vmem(
        functools.partial(select_kernel, experts),
        (
            jax.ShapeDtypeStruct(expert_hidden_state.shape, jnp.bfloat16),
            jax.ShapeDtypeStruct((experts * half, width_in), jnp.bfloat16),
        ),
        expert_hidden_state,
        expert_norm_gain[None, :],
        chosen_expert_index.T,
    )
    arrived = exchanged(outgoing.reshape(devices, half, width_in), EP)
    chunk = arrived.reshape(devices * half, width_in)
    middle = chunk.shape[0] // 2

    gates = ROUTED_SCALE * chosen_expert_score / jnp.sum(chosen_expert_score, axis=1, keepdims=True)
    named = chosen_expert_index[:, :, None] == jnp.arange(experts, dtype=jnp.int32)[None, None, :]
    chosen = jnp.any(named, axis=1)
    gate_of = jnp.sum(jnp.where(named, gates[:, :, None], 0.0), axis=1)
    row = jnp.arange(tokens)
    places = jnp.dot(
        (row[None, :] < row[:, None]).astype(jnp.bfloat16),
        chosen.astype(jnp.bfloat16),
        preferred_element_type=jnp.float32,
    )
    places = jnp.where(chosen, places.astype(jnp.int32), -1)
    filled = places[:, :, None] == parity * half + jnp.arange(half)[None, None, :]
    filled = filled.reshape(tokens, experts * half)
    shared_hidden = (
        jax.nn.silu(jnp.dot(normed, shared_gate_weight, preferred_element_type=jnp.float32))
        * jnp.dot(normed, shared_up_weight, preferred_element_type=jnp.float32)
    ).astype(jnp.bfloat16)
    shared_piece = gathered_columns(shared_hidden, "tp")
    shared = jnp.dot(
        shared_piece,
        rows_by_reversed_bits(shared_down_weight, members),
        preferred_element_type=jnp.float32,
    )

    before = shifted(chunk, "tp", 2)
    after = shifted(chunk, "tp", -2)
    far = [shifted(half, "tp", step) for half, step in zip(halves_of(chunk), (4, -4))]
    part_shape = jax.ShapeDtypeStruct((middle, 2 * units), jnp.bfloat16)
    hidden, hidden_first, hidden_second = fetching(
        hidden_kernel,
        (jax.ShapeDtypeStruct((chunk.shape[0], 2 * units), jnp.bfloat16), part_shape, part_shape),
        chunk,
        before,
        after,
        *far,
        own_in,
        partner_in,
    )
    before = shifted(hidden, "tp", 2)
    after = shifted(hidden, "tp", -2)
    far = [shifted(hidden_first, "tp", 4), shifted(hidden_second, "tp", -4)]
    answers = fetching(
        down_kernel,
        jax.ShapeDtypeStruct((chunk.shape[0], 2 * width_out), jnp.bfloat16),
        hidden,
        before,
        after,
        *far,
        own_down,
        partner_down,
    )
    returned = exchanged(answers.reshape(devices, half, 2 * width_out), EP)
    returned = returned.reshape(experts * half, 2 * width_out)
    mixing = jnp.where(filled.reshape(tokens, experts, half), gate_of[:, :, None], 0.0)
    mixing = mixing.reshape(tokens, experts * half)
    combined = sum(
        jnp.dot(part, returned, preferred_element_type=jnp.float32) for part in in_parts(mixing, 3)
    )
    other = swapped(combined[:, width_out:].astype(jnp.bfloat16), "tp", 1)
    combined = shared + combined[:, :width_out] + other.astype(jnp.float32)
    return combined.astype(jnp.bfloat16)


def per_device(
    recurrence_query_input,
    forget_gate_input,
    recurrence_value_input,
    output_gate_input,
    forget_lower_margin,
    position_decay_extra,
    head_norm_gain,
    recurrence_out_weight,
    expert_hidden_state,
    chosen_expert_index,
    chosen_expert_score,
    expert_norm_gain,
    routed_gate_weight,
    routed_up_weight,
    routed_down_weight,
    shared_gate_weight,
    shared_up_weight,
    shared_down_weight,
):
    recurrence_output = mixer_half(
        recurrence_query_input,
        forget_gate_input,
        recurrence_value_input,
        output_gate_input,
        forget_lower_margin,
        position_decay_extra,
        head_norm_gain,
        recurrence_out_weight,
    )
    expert_out = expert_half(
        expert_hidden_state,
        chosen_expert_index,
        chosen_expert_score,
        expert_norm_gain,
        routed_gate_weight,
        routed_up_weight,
        routed_down_weight,
        shared_gate_weight,
        shared_up_weight,
        shared_down_weight,
    )
    return (recurrence_output, expert_out)


def solution(mesh):
    split = Mesh(
        mesh.devices.reshape(mesh.shape["grp"], 16, 2, mesh.shape["tp"]),
        ("grp", "ep_0", "ep_1", "tp"),
    )
    in_specs = (
        P(GRP_EP, "tp"),
        P(GRP_EP, "tp"),
        P(GRP_EP, "tp"),
        P(GRP_EP, "tp"),
        P("tp"),
        P(GRP_EP, "tp"),
        P("tp"),
        P("tp", None),
        P(GRP_EP, None),
        P(GRP_EP, None),
        P(GRP_EP, None),
        P(),
        P(EP, None, "tp"),
        P(EP, None, "tp"),
        P(EP, None, "tp"),
        P(None, "tp"),
        P(None, "tp"),
        P(None, "tp"),
    )
    out_specs = (P(GRP_EP_TP, None), P(GRP_EP, "tp"))

    return jax.shard_map(
        per_device, mesh=split, in_specs=in_specs, out_specs=out_specs, check_vma=False
    )
```

```python
import functools

import jax
import jax.numpy as jnp
from jax import lax
from jax.experimental import pallas as pl
from jax.experimental.pallas import tpu as pltpu
from jax.sharding import Mesh
from jax.sharding import PartitionSpec as P


HEAD_CHANNELS = 128
BLK = 64
EP = ("ep_0", "ep_1")
GRP_EP = ("grp", "ep_0", "ep_1")
TP = ("tp_quad", "tp_pair")
EP_PAIR = ("ep_0", "ep_1", "tp_pair")
GRP_EP_TP = ("grp", "ep_0", "ep_1", "tp_quad", "tp_pair")


EPSILON = 1e-06
ROUTED_SCALE = 2.5
HIGHEST_PRECISION = lax.Precision.HIGHEST


def shifted(array, axis, step):
    count = lax.axis_size(axis)
    return lax.ppermute(array, axis, [(i, (i + step) % count) for i in range(count)])


def swapped(array, axis, bit):
    count = lax.axis_size(axis)
    return lax.ppermute(array, axis, [(i, i ^ bit) for i in range(count)])


def exchanged(array, axis):
    return lax.all_to_all(array, axis, split_axis=0, concat_axis=0, tiled=True)


def half_of(array, dim, place):
    return lax.dynamic_index_in_dim(array, place, dim, keepdims=False)


def summed_to_owners(array, axis):
    count = lax.axis_size(axis)
    bits = count.bit_length() - 1
    member = lax.axis_index(axis)
    kept = array.reshape(*[2] * bits, -1, array.shape[1])
    for bit in range(bits):
        mine = (member >> bit) & 1
        dim = bits - 1 - bit
        arrived = swapped(half_of(kept, dim, 1 - mine).astype(jnp.bfloat16), axis, 1 << bit)
        kept = half_of(kept, dim, mine) + arrived.astype(jnp.float32)
    return kept


def gathered_columns(array, axis):
    count = lax.axis_size(axis)
    member = lax.axis_index(axis)
    for bit in reversed(range(count.bit_length() - 1)):
        arrived = swapped(array, axis, 1 << bit)
        first = ((member >> bit) & 1) == 0
        array = jnp.concatenate(
            [jnp.where(first, array, arrived), jnp.where(first, arrived, array)], axis=1
        )
    return array


def rows_by_reversed_bits(matrix, count):
    bits = count.bit_length() - 1
    split = matrix.reshape(*[2] * bits, -1, matrix.shape[1])
    order = (*reversed(range(bits)), bits, bits + 1)
    return split.transpose(order).reshape(matrix.shape)


def in_parts(array, count):
    parts, rest = [], array
    for _ in range(count):
        rounded = lax.reduce_precision(rest, 8, 7)
        parts.append(rounded.astype(jnp.bfloat16))
        rest = rest - rounded
    return parts


def entering_state(log_decay, state):
    devices = lax.axis_size(EP)
    channels, width = state.shape
    part = channels // devices
    logs = jnp.stack(in_parts(log_decay, 3), axis=-1).reshape(devices, part, 3)
    logs = jnp.pad(logs, ((0, 0), (0, 0), (0, HEAD_CHANNELS - 3)))
    packed = jnp.concatenate(
        [state.astype(jnp.bfloat16).reshape(devices, part, width), logs], axis=2
    )
    arrived = exchanged(packed, EP)
    arrived = arrived.astype(jnp.float32)
    updates = arrived[:, :, :width]
    logs = jnp.sum(arrived[:, :, width : width + 3], axis=2)
    at = jnp.arange(devices)
    between = (at[None, None, :] > at[None, :, None]) & (at[None, None, :] < at[:, None, None])
    spans = jnp.dot(
        between.reshape(devices * devices, devices).astype(jnp.float32),
        logs,
        precision=HIGHEST_PRECISION,
    ).reshape(devices, devices, part)
    earlier = at[None, :, None] < at[:, None, None]
    factors = jnp.where(earlier, jnp.exp(spans), 0.0)
    prefix = jnp.einsum("rqc,qcv->rcv", factors, updates, precision=HIGHEST_PRECISION)
    prefix = prefix.astype(jnp.bfloat16)
    returned = exchanged(prefix, EP)
    return returned.astype(jnp.float32).reshape(channels, width)


def mixer_half(
    recurrence_query_input,
    forget_gate_input,
    recurrence_value_input,
    output_gate_input,
    forget_lower_margin,
    position_decay_extra,
    head_norm_gain,
    recurrence_out_weight,
):
    length = recurrence_query_input.shape[0]
    head_tensor = position_decay_extra.shape[1]
    blocks = length // BLK
    queries = jax.nn.silu(recurrence_query_input.astype(jnp.float32))
    key_gate_value = forget_lower_margin[None, :] * jax.nn.sigmoid(
        -forget_gate_input.astype(jnp.float32)
    )
    decay_logarithm = jnp.log1p(-key_gate_value) + jnp.repeat(
        position_decay_extra, HEAD_CHANNELS, axis=1
    )
    value_rows = recurrence_value_input.astype(jnp.float32)

    def split_heads(tensor):
        return tensor.reshape(blocks, BLK, head_tensor, HEAD_CHANNELS).transpose(2, 0, 1, 3)

    query_heads = split_heads(queries)
    key_heads = split_heads(key_gate_value)
    value_heads = split_heads(value_rows)
    cum_decay = jnp.cumsum(split_heads(decay_logarithm), axis=2)
    middle = cum_decay[:, :, BLK // 2 - 1 : BLK // 2]
    block_end = cum_decay[:, :, BLK - 1 : BLK]
    scores = jnp.einsum(
        "hncd,hnsd->hncs",
        query_heads * jnp.exp(cum_decay - middle),
        key_heads * jnp.exp(middle - cum_decay),
        precision=HIGHEST_PRECISION,
    )
    causal = jnp.tril(jnp.ones((BLK, BLK), dtype=bool))
    scores = jnp.where(causal, scores, 0.0)
    within = jnp.einsum("hncs,hnse->hnce", scores, value_heads, precision=HIGHEST_PRECISION)
    updates = jnp.einsum(
        "hncd,hnce->nhde",
        key_heads * jnp.exp(block_end - cum_decay),
        value_heads,
        precision=HIGHEST_PRECISION,
    )
    block_log = block_end[:, :, 0, :]
    block_decay = jnp.exp(block_log).transpose(1, 0, 2)

    def advance(carry_state, inputs):
        factor, update = inputs
        return (factor[..., None] * carry_state + update, carry_state)

    initial = jnp.zeros((head_tensor, HEAD_CHANNELS, HEAD_CHANNELS), jnp.float32)
    local_final, local_starts = lax.scan(advance, initial, (block_decay, updates))
    incoming = entering_state(
        jnp.sum(block_log, axis=1).reshape(-1), local_final.reshape(-1, HEAD_CHANNELS)
    ).reshape(head_tensor, HEAD_CHANNELS, HEAD_CHANNELS)
    before = jnp.exp(jnp.cumsum(block_log, axis=1) - block_log).transpose(1, 0, 2)
    starts = local_starts + before[..., None] * incoming[None]
    carried = jnp.einsum(
        "hncd,nhde->hnce", query_heads * jnp.exp(cum_decay), starts, precision=HIGHEST_PRECISION
    )
    outputs = (within + carried).transpose(1, 2, 0, 3).reshape(length, head_tensor, HEAD_CHANNELS)
    factor = lax.rsqrt(jnp.mean(outputs * outputs, axis=2, keepdims=True) + EPSILON)
    normed = (outputs * factor).reshape(length, head_tensor * HEAD_CHANNELS) * head_norm_gain[
        None, :
    ]
    gated_rows = (normed * jax.nn.silu(output_gate_input.astype(jnp.float32))).astype(jnp.bfloat16)
    partial = jnp.dot(gated_rows, recurrence_out_weight, preferred_element_type=jnp.float32)
    return summed_to_owners(partial, TP).astype(jnp.bfloat16)


VMEM = pl.BlockSpec(memory_space=pltpu.VMEM)
ANY = pl.BlockSpec(memory_space=pl.ANY)


def in_vmem(kernel, shapes, *operands):
    return pl.pallas_call(
        kernel,
        out_shape=shapes,
        in_specs=[VMEM] * len(operands),
        out_specs=jax.tree.map(lambda _: VMEM, shapes),
    )(*operands)


def fetching(kernel, shapes, *operands):
    count = len(operands)

    def body(*refs):
        sources, rest = refs[:count], refs[count:]
        outputs, held, arrived = rest[: -count - 1], rest[-count - 1 : -1], rest[-1]
        copies = [
            pltpu.make_async_copy(source, target, arrived.at[i])
            for i, (source, target) in enumerate(zip(sources, held))
        ]
        for copy in copies:
            copy.start()

        def fetch(i):
            def ready():
                copies[i].wait()
                return held[i]

            return ready

        kernel(*[fetch(i) for i in range(count)], *outputs)

    return pl.pallas_call(
        body,
        out_shape=shapes,
        in_specs=[ANY] * count,
        out_specs=jax.tree.map(lambda _: VMEM, shapes),
        scratch_shapes=[pltpu.VMEM(a.shape, a.dtype) for a in operands]
        + [pltpu.SemaphoreType.DMA((count,))],
    )(*operands)


def halves_kernel(whole, first, second):
    middle = first.shape[0]
    first[...] = whole[:middle, :]
    second[...] = whole[middle:, :]


def halves_of(array):
    half = jax.ShapeDtypeStruct((array.shape[0] // 2, array.shape[1]), array.dtype)
    return in_vmem(halves_kernel, (half, half), array)


def select_kernel(experts, hidden_state, gain, index, normed, outgoing):
    top, tokens = index.shape
    slots, width = outgoing.shape
    half = slots // experts
    features = hidden_state[...].astype(jnp.float32)
    factor = lax.rsqrt(jnp.mean(features * features, axis=1, keepdims=True) + EPSILON)
    normed[...] = (features * factor * gain[...]).astype(jnp.bfloat16)
    expert = lax.broadcasted_iota(jnp.int32, (experts, tokens), 0)
    chosen = index[0:1, :] == expert
    for j in range(1, top):
        chosen = chosen | (index[j : j + 1, :] == expert)
    earlier = lax.broadcasted_iota(jnp.int32, (tokens, tokens), 0) < lax.broadcasted_iota(
        jnp.int32, (tokens, tokens), 1
    )
    one = jnp.float32(1)
    zero = jnp.float32(0)
    places = jnp.dot(
        jnp.where(chosen, one, zero).astype(jnp.bfloat16),
        jnp.where(earlier, one, zero).astype(jnp.bfloat16),
        preferred_element_type=jnp.float32,
    )
    places = jnp.where(chosen, places, -one).astype(jnp.bfloat16)
    slot = lax.broadcasted_iota(jnp.int32, (slots, experts), 0)
    spread = jnp.where(
        slot // half == lax.broadcasted_iota(jnp.int32, (slots, experts), 1), one, zero
    ).astype(jnp.bfloat16)
    wanted = jnp.dot(spread, places, preferred_element_type=jnp.float32).astype(jnp.int32)
    own = lax.broadcasted_iota(jnp.int32, (slots, tokens), 0) % half + lax.axis_index("tp_pair") * half
    filled = jnp.where(wanted == own, one, zero).astype(jnp.bfloat16)
    start = pl.multiple_of(lax.axis_index("tp_quad") * width, width)
    outgoing[...] = jnp.dot(
        filled, normed[:, pl.ds(start, width)], preferred_element_type=jnp.float32
    ).astype(jnp.bfloat16)


def around_products(pieces, matrices):
    quad = lax.axis_index("tp_quad")
    held = []

    def dot(piece, matrix, step):
        depth = piece.shape[1]
        count = matrix.shape[0] // depth
        start = pl.multiple_of(((quad + step) & (count - 1)) * depth, depth)
        return jnp.dot(
            piece[...], matrix[pl.ds(start, depth), :], preferred_element_type=jnp.float32
        )

    near = [None] * len(matrices)
    for fetch, step in zip(pieces[:3], (0, -1, 1)):
        piece = fetch()
        for k, fetch_matrix in enumerate(matrices):
            if step == 0:
                held.append(fetch_matrix())
            part = dot(piece, held[k], step)
            near[k] = part if near[k] is None else near[k] + part
    first, second = (fetch() for fetch in pieces[3:])
    middle = first.shape[0]
    return [
        (part[:middle] + dot(first, matrix, 2), part[middle:] + dot(second, matrix, 2))
        for part, matrix in zip(near, held)
    ]


def hidden_kernel(
    own, before, after, far_first, far_second, own_in, partner_in, hidden, hidden_first, hidden_second
):
    pieces = (own, before, after, far_first, far_second)
    middle, units = (hidden_first.shape[0], hidden_first.shape[1] // 2)
    sides = [
        [
            (jax.nn.silu(both[:, :units]) * both[:, units:]).astype(jnp.bfloat16)
            for both in halves
        ]
        for halves in around_products(pieces, (own_in, partner_in))
    ]
    even = lax.axis_index("tp_pair") == 0
    for k, part in enumerate((hidden_first, hidden_second)):
        part[:, :units] = jnp.where(even, sides[0][k], sides[1][k])
        part[:, units:] = jnp.where(even, sides[1][k], sides[0][k])
        hidden[pl.ds(k * middle, middle), :] = part[...]


def down_kernel(own, before, after, far_first, far_second, own_down, partner_down, answers):
    pieces = (own, before, after, far_first, far_second)
    sources, _, slots, width = answers.shape
    count = sources // 2
    place = lax.axis_index("tp_pair")
    for side, halves in zip(
        (place, 1 - place), around_products(pieces, (own_down, partner_down))
    ):
        for k, part in enumerate(halves):
            answers[pl.ds(k * count, count), side] = part.astype(jnp.bfloat16).reshape(
                count, slots, width
            )


def expert_half(
    expert_hidden_state,
    chosen_expert_index,
    chosen_expert_score,
    expert_norm_gain,
    routed_gate_weight,
    routed_up_weight,
    routed_down_weight,
    shared_gate_weight,
    shared_up_weight,
    shared_down_weight,
):
    tokens, top = chosen_expert_index.shape
    local_experts = routed_gate_weight.shape[0]
    devices = lax.axis_size(EP)
    experts = local_experts * devices
    capacity = min(tokens, 2 * tokens * top // experts)
    width_out = routed_down_weight.shape[2]
    members = lax.axis_size(TP)
    quads = members // 2
    half = capacity // 2
    width_in = routed_gate_weight.shape[1] // quads
    units = routed_gate_weight.shape[2]

    own_in = jnp.concatenate([routed_gate_weight[0], routed_up_weight[0]], axis=1)
    own_down = routed_down_weight[0]
    partner_in = swapped(own_in, TP, 1)
    partner_down = swapped(own_down, TP, 1)

    normed, outgoing = in_vmem(
        functools.partial(select_kernel, experts),
        (
            jax.ShapeDtypeStruct(expert_hidden_state.shape, jnp.bfloat16),
            jax.ShapeDtypeStruct((experts * half, width_in), jnp.bfloat16),
        ),
        expert_hidden_state,
        expert_norm_gain[None, :],
        chosen_expert_index.T,
    )
    arrived = exchanged(outgoing.reshape(devices, half, width_in), EP)
    chunk = arrived.reshape(devices * half, width_in)
    middle = chunk.shape[0] // 2

    gates = ROUTED_SCALE * chosen_expert_score / jnp.sum(chosen_expert_score, axis=1, keepdims=True)
    named = chosen_expert_index[:, :, None] == jnp.arange(experts, dtype=jnp.int32)[None, None, :]
    chosen = jnp.any(named, axis=1)
    gate_of = jnp.sum(jnp.where(named, gates[:, :, None], 0.0), axis=1)
    row = jnp.arange(tokens)
    places = jnp.dot(
        (row[None, :] < row[:, None]).astype(jnp.bfloat16),
        chosen.astype(jnp.bfloat16),
        preferred_element_type=jnp.float32,
    )
    places = jnp.where(chosen, places.astype(jnp.int32), -1)
    shared_hidden = (
        jax.nn.silu(jnp.dot(normed, shared_gate_weight, preferred_element_type=jnp.float32))
        * jnp.dot(normed, shared_up_weight, preferred_element_type=jnp.float32)
    ).astype(jnp.bfloat16)
    shared_piece = gathered_columns(shared_hidden, TP)
    shared = jnp.dot(
        shared_piece,
        rows_by_reversed_bits(shared_down_weight, members),
        preferred_element_type=jnp.float32,
    )

    before = shifted(chunk, TP, 2)
    after = shifted(chunk, TP, -2)
    far = [shifted(half, TP, step) for half, step in zip(halves_of(chunk), (4, -4))]
    part_shape = jax.ShapeDtypeStruct((middle, 2 * units), jnp.bfloat16)
    hidden, hidden_first, hidden_second = fetching(
        hidden_kernel,
        (jax.ShapeDtypeStruct((chunk.shape[0], 2 * units), jnp.bfloat16), part_shape, part_shape),
        chunk,
        before,
        after,
        *far,
        own_in,
        partner_in,
    )
    before = shifted(hidden, TP, 2)
    after = shifted(hidden, TP, -2)
    far = [shifted(hidden_first, TP, 4), shifted(hidden_second, TP, -4)]
    answers = fetching(
        down_kernel,
        jax.ShapeDtypeStruct((devices, 2, half, width_out), jnp.bfloat16),
        hidden,
        before,
        after,
        *far,
        own_down,
        partner_down,
    )
    returned = exchanged(answers.reshape(2 * devices, half, width_out), EP_PAIR)
    returned = returned.reshape(experts * capacity, width_out)
    filled = places[:, :, None] == jnp.arange(capacity)[None, None, :]
    mixing = jnp.where(filled, gate_of[:, :, None], 0.0).reshape(tokens, experts * capacity)
    for part in in_parts(mixing, 3):
        shared = shared + jnp.dot(part, returned, preferred_element_type=jnp.float32)
    return shared.astype(jnp.bfloat16)


def per_device(
    recurrence_query_input,
    forget_gate_input,
    recurrence_value_input,
    output_gate_input,
    forget_lower_margin,
    position_decay_extra,
    head_norm_gain,
    recurrence_out_weight,
    expert_hidden_state,
    chosen_expert_index,
    chosen_expert_score,
    expert_norm_gain,
    routed_gate_weight,
    routed_up_weight,
    routed_down_weight,
    shared_gate_weight,
    shared_up_weight,
    shared_down_weight,
):
    recurrence_output = mixer_half(
        recurrence_query_input,
        forget_gate_input,
        recurrence_value_input,
        output_gate_input,
        forget_lower_margin,
        position_decay_extra,
        head_norm_gain,
        recurrence_out_weight,
    )
    expert_out = expert_half(
        expert_hidden_state,
        chosen_expert_index,
        chosen_expert_score,
        expert_norm_gain,
        routed_gate_weight,
        routed_up_weight,
        routed_down_weight,
        shared_gate_weight,
        shared_up_weight,
        shared_down_weight,
    )
    return (recurrence_output, expert_out)


def solution(mesh):
    split = Mesh(
        mesh.devices.reshape(mesh.shape["grp"], -1, 2, mesh.shape["tp"] // 2, 2),
        ("grp", "ep_0", "ep_1", "tp_quad", "tp_pair"),
    )
    in_specs = (
        P(GRP_EP, TP),
        P(GRP_EP, TP),
        P(GRP_EP, TP),
        P(GRP_EP, TP),
        P(TP),
        P(GRP_EP, TP),
        P(TP),
        P(TP, None),
        P(GRP_EP, None),
        P(GRP_EP, None),
        P(GRP_EP, None),
        P(),
        P(EP, None, TP),
        P(EP, None, TP),
        P(EP, None, TP),
        P(None, TP),
        P(None, TP),
        P(None, TP),
    )
    out_specs = (P(GRP_EP_TP, None), P(GRP_EP, TP))

    return jax.shard_map(
        per_device, mesh=split, in_specs=in_specs, out_specs=out_specs, check_vma=False
    )
```

```python
import functools

import jax
import jax.numpy as jnp
from jax import lax
from jax.experimental import pallas as pl
from jax.experimental.pallas import tpu as pltpu
from jax.sharding import Mesh
from jax.sharding import PartitionSpec as P


HEAD_CHANNELS = 128
BLK = 64
EP = ("ep_0", "ep_1")
GRP_EP = ("grp", "ep_0", "ep_1")
TP = ("tp_quad", "tp_pair")
EP_PAIR = ("ep_0", "ep_1", "tp_pair")
GRP_EP_TP = ("grp", "ep_0", "ep_1", "tp_quad", "tp_pair")


EPSILON = 1e-06
ROUTED_SCALE = 2.5
HIGHEST_PRECISION = lax.Precision.HIGHEST


def shifted(array, axis, step):
    count = lax.axis_size(axis)
    return lax.ppermute(array, axis, [(i, (i + step) % count) for i in range(count)])


def swapped(array, axis, bit):
    count = lax.axis_size(axis)
    return lax.ppermute(array, axis, [(i, i ^ bit) for i in range(count)])


def exchanged(array, axis):
    return lax.all_to_all(array, axis, split_axis=0, concat_axis=0, tiled=True)


def half_of(array, dim, place):
    return lax.dynamic_index_in_dim(array, place, dim, keepdims=False)


def summed_to_owners(array, axis):
    count = lax.axis_size(axis)
    bits = count.bit_length() - 1
    member = lax.axis_index(axis)
    kept = array.reshape(*[2] * bits, -1, array.shape[1])
    for bit in range(bits):
        mine = (member >> bit) & 1
        dim = bits - 1 - bit
        arrived = swapped(half_of(kept, dim, 1 - mine).astype(jnp.bfloat16), axis, 1 << bit)
        kept = half_of(kept, dim, mine) + arrived.astype(jnp.float32)
    return kept


def gathered_columns(array, axis):
    count = lax.axis_size(axis)
    member = lax.axis_index(axis)
    for bit in reversed(range(count.bit_length() - 1)):
        arrived = swapped(array, axis, 1 << bit)
        first = ((member >> bit) & 1) == 0
        array = jnp.concatenate(
            [jnp.where(first, array, arrived), jnp.where(first, arrived, array)], axis=1
        )
    return array


def rows_by_reversed_bits(matrix, count):
    bits = count.bit_length() - 1
    split = matrix.reshape(*[2] * bits, -1, matrix.shape[1])
    order = (*reversed(range(bits)), bits, bits + 1)
    return split.transpose(order).reshape(matrix.shape)


def in_parts(array, count):
    parts, rest = [], array
    for _ in range(count):
        rounded = lax.reduce_precision(rest, 8, 7)
        parts.append(rounded.astype(jnp.bfloat16))
        rest = rest - rounded
    return parts


def entering_state(log_decay, state):
    devices = lax.axis_size(EP)
    channels, width = state.shape
    part = channels // devices
    logs = jnp.stack(in_parts(log_decay, 3), axis=-1).reshape(devices, part, 3)
    logs = jnp.pad(logs, ((0, 0), (0, 0), (0, HEAD_CHANNELS - 3)))
    packed = jnp.concatenate(
        [state.astype(jnp.bfloat16).reshape(devices, part, width), logs], axis=2
    )
    arrived = exchanged(packed, EP)
    arrived = arrived.astype(jnp.float32)
    updates = arrived[:, :, :width]
    logs = jnp.sum(arrived[:, :, width : width + 3], axis=2)
    at = jnp.arange(devices)
    between = (at[None, None, :] > at[None, :, None]) & (at[None, None, :] < at[:, None, None])
    spans = jnp.dot(
        between.reshape(devices * devices, devices).astype(jnp.float32),
        logs,
        precision=HIGHEST_PRECISION,
    ).reshape(devices, devices, part)
    earlier = at[None, :, None] < at[:, None, None]
    factors = jnp.where(earlier, jnp.exp(spans), 0.0)
    prefix = jnp.einsum("rqc,qcv->rcv", factors, updates, precision=HIGHEST_PRECISION)
    prefix = prefix.astype(jnp.bfloat16)
    returned = exchanged(prefix, EP)
    return returned.astype(jnp.float32).reshape(channels, width)


def mixer_half(
    recurrence_query_input,
    forget_gate_input,
    recurrence_value_input,
    output_gate_input,
    forget_lower_margin,
    position_decay_extra,
    head_norm_gain,
    recurrence_out_weight,
):
    length = recurrence_query_input.shape[0]
    head_tensor = position_decay_extra.shape[1]
    blocks = length // BLK
    queries = jax.nn.silu(recurrence_query_input.astype(jnp.float32))
    key_gate_value = forget_lower_margin[None, :] * jax.nn.sigmoid(
        -forget_gate_input.astype(jnp.float32)
    )
    decay_logarithm = jnp.log1p(-key_gate_value) + jnp.repeat(
        position_decay_extra, HEAD_CHANNELS, axis=1
    )
    value_rows = recurrence_value_input.astype(jnp.float32)

    def split_heads(tensor):
        return tensor.reshape(blocks, BLK, head_tensor, HEAD_CHANNELS).transpose(2, 0, 1, 3)

    query_heads = split_heads(queries)
    key_heads = split_heads(key_gate_value)
    value_heads = split_heads(value_rows)
    cum_decay = jnp.cumsum(split_heads(decay_logarithm), axis=2)
    middle = cum_decay[:, :, BLK // 2 - 1 : BLK // 2]
    block_end = cum_decay[:, :, BLK - 1 : BLK]
    scores = jnp.einsum(
        "hncd,hnsd->hncs",
        query_heads * jnp.exp(cum_decay - middle),
        key_heads * jnp.exp(middle - cum_decay),
        precision=HIGHEST_PRECISION,
    )
    causal = jnp.tril(jnp.ones((BLK, BLK), dtype=bool))
    scores = jnp.where(causal, scores, 0.0)
    within = jnp.einsum("hncs,hnse->hnce", scores, value_heads, precision=HIGHEST_PRECISION)
    updates = jnp.einsum(
        "hncd,hnce->nhde",
        key_heads * jnp.exp(block_end - cum_decay),
        value_heads,
        precision=HIGHEST_PRECISION,
    )
    block_log = block_end[:, :, 0, :]
    block_decay = jnp.exp(block_log).transpose(1, 0, 2)

    def advance(carry_state, inputs):
        factor, update = inputs
        return (factor[..., None] * carry_state + update, carry_state)

    initial = jnp.zeros((head_tensor, HEAD_CHANNELS, HEAD_CHANNELS), jnp.float32)
    local_final, local_starts = lax.scan(advance, initial, (block_decay, updates))
    incoming = entering_state(
        jnp.sum(block_log, axis=1).reshape(-1), local_final.reshape(-1, HEAD_CHANNELS)
    ).reshape(head_tensor, HEAD_CHANNELS, HEAD_CHANNELS)
    before = jnp.exp(jnp.cumsum(block_log, axis=1) - block_log).transpose(1, 0, 2)
    starts = local_starts + before[..., None] * incoming[None]
    carried = jnp.einsum(
        "hncd,nhde->hnce", query_heads * jnp.exp(cum_decay), starts, precision=HIGHEST_PRECISION
    )
    outputs = (within + carried).transpose(1, 2, 0, 3).reshape(length, head_tensor, HEAD_CHANNELS)
    factor = lax.rsqrt(jnp.mean(outputs * outputs, axis=2, keepdims=True) + EPSILON)
    normed = (outputs * factor).reshape(length, head_tensor * HEAD_CHANNELS) * head_norm_gain[
        None, :
    ]
    gated_rows = (normed * jax.nn.silu(output_gate_input.astype(jnp.float32))).astype(jnp.bfloat16)
    partial = jnp.dot(gated_rows, recurrence_out_weight, preferred_element_type=jnp.float32)
    return summed_to_owners(partial, TP).astype(jnp.bfloat16)


VMEM = pl.BlockSpec(memory_space=pltpu.VMEM)
ANY = pl.BlockSpec(memory_space=pl.ANY)


def in_vmem(kernel, shapes, *operands):
    return pl.pallas_call(
        kernel,
        out_shape=shapes,
        in_specs=[VMEM] * len(operands),
        out_specs=jax.tree.map(lambda _: VMEM, shapes),
    )(*operands)


def fetching(kernel, shapes, *operands):
    count = len(operands)

    def body(*refs):
        sources, rest = refs[:count], refs[count:]
        outputs, held, arrived = rest[: -count - 1], rest[-count - 1 : -1], rest[-1]
        copies = [
            pltpu.make_async_copy(source, target, arrived.at[i])
            for i, (source, target) in enumerate(zip(sources, held))
        ]
        for copy in copies:
            copy.start()

        def fetch(i):
            def ready():
                copies[i].wait()
                return held[i]

            return ready

        kernel(*[fetch(i) for i in range(count)], *outputs)

    return pl.pallas_call(
        body,
        out_shape=shapes,
        in_specs=[ANY] * count,
        out_specs=jax.tree.map(lambda _: VMEM, shapes),
        scratch_shapes=[pltpu.VMEM(a.shape, a.dtype) for a in operands]
        + [pltpu.SemaphoreType.DMA((count,))],
    )(*operands)


def halves_kernel(whole, first, second):
    middle = first.shape[0]
    first[...] = whole[:middle, :]
    second[...] = whole[middle:, :]


def halves_of(array):
    half = jax.ShapeDtypeStruct((array.shape[0] // 2, array.shape[1]), array.dtype)
    return in_vmem(halves_kernel, (half, half), array)


def select_kernel(experts, hidden_state, gain, index, normed, outgoing):
    top, tokens = index.shape
    slots, width = outgoing.shape
    half = slots // experts
    features = hidden_state[...].astype(jnp.float32)
    factor = lax.rsqrt(jnp.mean(features * features, axis=1, keepdims=True) + EPSILON)
    normed[...] = (features * factor * gain[...]).astype(jnp.bfloat16)
    expert = lax.broadcasted_iota(jnp.int32, (experts, tokens), 0)
    chosen = index[0:1, :] == expert
    for j in range(1, top):
        chosen = chosen | (index[j : j + 1, :] == expert)
    earlier = lax.broadcasted_iota(jnp.int32, (tokens, tokens), 0) < lax.broadcasted_iota(
        jnp.int32, (tokens, tokens), 1
    )
    one = jnp.float32(1)
    zero = jnp.float32(0)
    places = jnp.dot(
        jnp.where(chosen, one, zero).astype(jnp.bfloat16),
        jnp.where(earlier, one, zero).astype(jnp.bfloat16),
        preferred_element_type=jnp.float32,
    )
    places = jnp.where(chosen, places, -one).astype(jnp.bfloat16)
    slot = lax.broadcasted_iota(jnp.int32, (slots, experts), 0)
    spread = jnp.where(
        slot // half == lax.broadcasted_iota(jnp.int32, (slots, experts), 1), one, zero
    ).astype(jnp.bfloat16)
    wanted = jnp.dot(spread, places, preferred_element_type=jnp.float32).astype(jnp.int32)
    own = lax.broadcasted_iota(jnp.int32, (slots, tokens), 0) % half + lax.axis_index("tp_pair") * half
    filled = jnp.where(wanted == own, one, zero).astype(jnp.bfloat16)
    start = pl.multiple_of(lax.axis_index("tp_quad") * width, width)
    outgoing[...] = jnp.dot(
        filled, normed[:, pl.ds(start, width)], preferred_element_type=jnp.float32
    ).astype(jnp.bfloat16)


def around_products(pieces, matrices):
    quad = lax.axis_index("tp_quad")
    held = []

    def dot(piece, matrix, step):
        depth = piece.shape[1]
        count = matrix.shape[0] // depth
        start = pl.multiple_of(((quad + step) & (count - 1)) * depth, depth)
        return jnp.dot(
            piece[...], matrix[pl.ds(start, depth), :], preferred_element_type=jnp.float32
        )

    near = [None] * len(matrices)
    for fetch, step in zip(pieces[:3], (0, -1, 1)):
        piece = fetch()
        for k, fetch_matrix in enumerate(matrices):
            if step == 0:
                held.append(fetch_matrix())
            part = dot(piece, held[k], step)
            near[k] = part if near[k] is None else near[k] + part
    first, second = (fetch() for fetch in pieces[3:])
    middle = first.shape[0]
    return [
        (part[:middle] + dot(first, matrix, 2), part[middle:] + dot(second, matrix, 2))
        for part, matrix in zip(near, held)
    ]


def hidden_kernel(
    own, before, after, far_first, far_second, own_in, partner_in, hidden, hidden_first, hidden_second
):
    pieces = (own, before, after, far_first, far_second)
    middle, units = (hidden_first.shape[0], hidden_first.shape[1] // 2)
    sides = [
        [
            (jax.nn.silu(both[:, :units]) * both[:, units:]).astype(jnp.bfloat16)
            for both in halves
        ]
        for halves in around_products(pieces, (own_in, partner_in))
    ]
    even = lax.axis_index("tp_pair") == 0
    for k, part in enumerate((hidden_first, hidden_second)):
        part[:, :units] = jnp.where(even, sides[0][k], sides[1][k])
        part[:, units:] = jnp.where(even, sides[1][k], sides[0][k])
        hidden[pl.ds(k * middle, middle), :] = part[...]


def down_kernel(own, before, after, far_first, far_second, own_down, partner_down, answers):
    pieces = (own, before, after, far_first, far_second)
    sources, _, slots, width = answers.shape
    count = sources // 2
    place = lax.axis_index("tp_pair")
    for side, halves in zip(
        (place, 1 - place), around_products(pieces, (own_down, partner_down))
    ):
        for k, part in enumerate(halves):
            answers[pl.ds(k * count, count), side] = part.astype(jnp.bfloat16).reshape(
                count, slots, width
            )


def expert_half(
    expert_hidden_state,
    chosen_expert_index,
    chosen_expert_score,
    expert_norm_gain,
    routed_gate_weight,
    routed_up_weight,
    routed_down_weight,
    shared_gate_weight,
    shared_up_weight,
    shared_down_weight,
):
    tokens, top = chosen_expert_index.shape
    local_experts = routed_gate_weight.shape[0]
    devices = lax.axis_size(EP)
    experts = local_experts * devices
    capacity = min(tokens, 2 * tokens * top // experts)
    width_out = routed_down_weight.shape[2]
    members = lax.axis_size(TP)
    quads = members // 2
    half = capacity // 2
    width_in = routed_gate_weight.shape[1] // quads
    units = routed_gate_weight.shape[2]

    own_in = jnp.concatenate([routed_gate_weight[0], routed_up_weight[0]], axis=1)
    own_down = routed_down_weight[0]
    partner_in = swapped(own_in, TP, 1)
    partner_down = swapped(own_down, TP, 1)

    normed, outgoing = in_vmem(
        functools.partial(select_kernel, experts),
        (
            jax.ShapeDtypeStruct(expert_hidden_state.shape, jnp.bfloat16),
            jax.ShapeDtypeStruct((experts * half, width_in), jnp.bfloat16),
        ),
        expert_hidden_state,
        expert_norm_gain[None, :],
        chosen_expert_index.T,
    )
    arrived = exchanged(outgoing.reshape(devices, half, width_in), EP)
    chunk = arrived.reshape(devices * half, width_in)
    middle = chunk.shape[0] // 2

    gates = ROUTED_SCALE * chosen_expert_score / jnp.sum(chosen_expert_score, axis=1, keepdims=True)
    named = chosen_expert_index[:, :, None] == jnp.arange(experts, dtype=jnp.int32)[None, None, :]
    chosen = jnp.any(named, axis=1)
    gate_of = jnp.sum(jnp.where(named, gates[:, :, None], 0.0), axis=1)
    row = jnp.arange(tokens)
    places = jnp.dot(
        (row[None, :] < row[:, None]).astype(jnp.bfloat16),
        chosen.astype(jnp.bfloat16),
        preferred_element_type=jnp.float32,
    )
    places = jnp.where(chosen, places.astype(jnp.int32), -1)
    shared_hidden = (
        jax.nn.silu(jnp.dot(normed, shared_gate_weight, preferred_element_type=jnp.float32))
        * jnp.dot(normed, shared_up_weight, preferred_element_type=jnp.float32)
    ).astype(jnp.bfloat16)
    shared_piece = gathered_columns(shared_hidden, TP)
    shared_down = rows_by_reversed_bits(shared_down_weight, members)
    shared = jnp.dot(shared_piece, shared_down, preferred_element_type=jnp.float32)

    before = shifted(chunk, TP, 2)
    after = shifted(chunk, TP, -2)
    far = [shifted(half, TP, step) for half, step in zip(halves_of(chunk), (4, -4))]
    part_shape = jax.ShapeDtypeStruct((middle, 2 * units), jnp.bfloat16)
    hidden, hidden_first, hidden_second = fetching(
        hidden_kernel,
        (jax.ShapeDtypeStruct((chunk.shape[0], 2 * units), jnp.bfloat16), part_shape, part_shape),
        chunk,
        before,
        after,
        *far,
        own_in,
        partner_in,
    )
    before = shifted(hidden, TP, 2)
    after = shifted(hidden, TP, -2)
    far = [shifted(hidden_first, TP, 4), shifted(hidden_second, TP, -4)]
    answers = fetching(
        down_kernel,
        jax.ShapeDtypeStruct((devices, 2, half, width_out), jnp.bfloat16),
        hidden,
        before,
        after,
        *far,
        own_down,
        partner_down,
    )
    returned = exchanged(answers.reshape(2 * devices, half, width_out), EP_PAIR)
    returned = returned.reshape(experts * capacity, width_out)
    filled = places[:, :, None] == jnp.arange(capacity)[None, None, :]
    mixing = jnp.where(filled, gate_of[:, :, None], 0.0).reshape(tokens, experts * capacity)
    for part in in_parts(mixing, 3):
        shared = shared + jnp.dot(part, returned, preferred_element_type=jnp.float32)
    return shared.astype(jnp.bfloat16)


def per_device(
    recurrence_query_input,
    forget_gate_input,
    recurrence_value_input,
    output_gate_input,
    forget_lower_margin,
    position_decay_extra,
    head_norm_gain,
    recurrence_out_weight,
    expert_hidden_state,
    chosen_expert_index,
    chosen_expert_score,
    expert_norm_gain,
    routed_gate_weight,
    routed_up_weight,
    routed_down_weight,
    shared_gate_weight,
    shared_up_weight,
    shared_down_weight,
):
    recurrence_output = mixer_half(
        recurrence_query_input,
        forget_gate_input,
        recurrence_value_input,
        output_gate_input,
        forget_lower_margin,
        position_decay_extra,
        head_norm_gain,
        recurrence_out_weight,
    )
    expert_out = expert_half(
        expert_hidden_state,
        chosen_expert_index,
        chosen_expert_score,
        expert_norm_gain,
        routed_gate_weight,
        routed_up_weight,
        routed_down_weight,
        shared_gate_weight,
        shared_up_weight,
        shared_down_weight,
    )
    return (recurrence_output, expert_out)


def solution(mesh):
    split = Mesh(
        mesh.devices.reshape(mesh.shape["grp"], -1, 2, mesh.shape["tp"] // 2, 2),
        ("grp", "ep_0", "ep_1", "tp_quad", "tp_pair"),
    )
    in_specs = (
        P(GRP_EP, TP),
        P(GRP_EP, TP),
        P(GRP_EP, TP),
        P(GRP_EP, TP),
        P(TP),
        P(GRP_EP, TP),
        P(TP),
        P(TP, None),
        P(GRP_EP, None),
        P(GRP_EP, None),
        P(GRP_EP, None),
        P(),
        P(EP, None, TP),
        P(EP, None, TP),
        P(EP, None, TP),
        P(None, TP),
        P(None, TP),
        P(None, TP),
    )
    out_specs = (P(GRP_EP_TP, None), P(GRP_EP, TP))

    return jax.shard_map(
        per_device, mesh=split, in_specs=in_specs, out_specs=out_specs, check_vma=False
    )
```

```python
import functools

import jax
import jax.numpy as jnp
from jax import lax
from jax.experimental import pallas as pl
from jax.experimental.pallas import tpu as pltpu
from jax.sharding import Mesh
from jax.sharding import PartitionSpec as P


HEAD_CHANNELS = 128
BLK = 64
EP = ("ep_0", "ep_1")
GRP_EP = ("grp", "ep_0", "ep_1")
QUAD, PAIR = ("tq", "tb")
TP = (QUAD, PAIR)
EP_PAIR = (*EP, PAIR)
GRP_EP_TP = (*GRP_EP, *TP)


EPSILON = 1e-06
ROUTED_SCALE = 2.5
HIGHEST_PRECISION = lax.Precision.HIGHEST


def shifted(array, axis, step):
    count = lax.axis_size(axis)
    return lax.ppermute(array, axis, [(i, (i + step) % count) for i in range(count)])


def swapped(array, axis, bit):
    count = lax.axis_size(axis)
    return lax.ppermute(array, axis, [(i, i ^ bit) for i in range(count)])


def exchanged(array, axis):
    return lax.all_to_all(array, axis, split_axis=0, concat_axis=0, tiled=True)


def half_of(array, dim, place):
    return lax.dynamic_index_in_dim(array, place, dim, keepdims=False)


def summed_to_owners(array, axis):
    count = lax.axis_size(axis)
    bits = count.bit_length() - 1
    member = lax.axis_index(axis)
    kept = array.reshape(*[2] * bits, -1, array.shape[1])
    for bit in range(bits):
        mine = (member >> bit) & 1
        dim = bits - 1 - bit
        arrived = swapped(half_of(kept, dim, 1 - mine).astype(jnp.bfloat16), axis, 1 << bit)
        kept = half_of(kept, dim, mine) + arrived.astype(jnp.float32)
    return kept


def gathered_columns(array, axis):
    count = lax.axis_size(axis)
    member = lax.axis_index(axis)
    for bit in reversed(range(count.bit_length() - 1)):
        arrived = swapped(array, axis, 1 << bit)
        first = ((member >> bit) & 1) == 0
        array = jnp.concatenate(
            [jnp.where(first, array, arrived), jnp.where(first, arrived, array)], axis=1
        )
    return array


def rows_by_reversed_bits(matrix, count):
    bits = count.bit_length() - 1
    split = matrix.reshape(*[2] * bits, -1, matrix.shape[1])
    order = (*reversed(range(bits)), bits, bits + 1)
    return split.transpose(order).reshape(matrix.shape)


def in_parts(array, count):
    parts, rest = [], array
    for _ in range(count):
        rounded = lax.reduce_precision(rest, 8, 7)
        parts.append(rounded.astype(jnp.bfloat16))
        rest = rest - rounded
    return parts


def entering_state(log_decay, state):
    devices = lax.axis_size(EP)
    channels, width = state.shape
    part = channels // devices
    logs = jnp.stack(in_parts(log_decay, 3), axis=-1).reshape(devices, part, 3)
    logs = jnp.pad(logs, ((0, 0), (0, 0), (0, HEAD_CHANNELS - 3)))
    packed = jnp.concatenate(
        [state.astype(jnp.bfloat16).reshape(devices, part, width), logs], axis=2
    )
    arrived = exchanged(packed, EP)
    arrived = arrived.astype(jnp.float32)
    updates = arrived[:, :, :width]
    logs = jnp.sum(arrived[:, :, width : width + 3], axis=2)
    at = jnp.arange(devices)
    between = (at[None, None, :] > at[None, :, None]) & (at[None, None, :] < at[:, None, None])
    spans = jnp.dot(
        between.reshape(devices * devices, devices).astype(jnp.float32),
        logs,
        precision=HIGHEST_PRECISION,
    ).reshape(devices, devices, part)
    earlier = at[None, :, None] < at[:, None, None]
    factors = jnp.where(earlier, jnp.exp(spans), 0.0)
    prefix = jnp.einsum("rqc,qcv->rcv", factors, updates, precision=HIGHEST_PRECISION)
    prefix = prefix.astype(jnp.bfloat16)
    returned = exchanged(prefix, EP)
    return returned.astype(jnp.float32).reshape(channels, width)


def mixer_half(
    recurrence_query_input,
    forget_gate_input,
    recurrence_value_input,
    output_gate_input,
    forget_lower_margin,
    position_decay_extra,
    head_norm_gain,
    recurrence_out_weight,
):
    length = recurrence_query_input.shape[0]
    head_tensor = position_decay_extra.shape[1]
    blocks = length // BLK
    queries = jax.nn.silu(recurrence_query_input.astype(jnp.float32))
    key_gate_value = forget_lower_margin[None, :] * jax.nn.sigmoid(
        -forget_gate_input.astype(jnp.float32)
    )
    decay_logarithm = jnp.log1p(-key_gate_value) + jnp.repeat(
        position_decay_extra, HEAD_CHANNELS, axis=1
    )
    value_rows = recurrence_value_input.astype(jnp.float32)

    def split_heads(tensor):
        return tensor.reshape(blocks, BLK, head_tensor, HEAD_CHANNELS).transpose(2, 0, 1, 3)

    query_heads = split_heads(queries)
    key_heads = split_heads(key_gate_value)
    value_heads = split_heads(value_rows)
    cum_decay = jnp.cumsum(split_heads(decay_logarithm), axis=2)
    middle = cum_decay[:, :, BLK // 2 - 1 : BLK // 2]
    block_end = cum_decay[:, :, BLK - 1 : BLK]
    scores = jnp.einsum(
        "hncd,hnsd->hncs",
        query_heads * jnp.exp(cum_decay - middle),
        key_heads * jnp.exp(middle - cum_decay),
        precision=HIGHEST_PRECISION,
    )
    causal = jnp.tril(jnp.ones((BLK, BLK), dtype=bool))
    scores = jnp.where(causal, scores, 0.0)
    within = jnp.einsum("hncs,hnse->hnce", scores, value_heads, precision=HIGHEST_PRECISION)
    updates = jnp.einsum(
        "hncd,hnce->nhde",
        key_heads * jnp.exp(block_end - cum_decay),
        value_heads,
        precision=HIGHEST_PRECISION,
    )
    block_log = block_end[:, :, 0, :]
    block_decay = jnp.exp(block_log).transpose(1, 0, 2)

    def advance(carry_state, inputs):
        factor, update = inputs
        return (factor[..., None] * carry_state + update, carry_state)

    initial = jnp.zeros((head_tensor, HEAD_CHANNELS, HEAD_CHANNELS), jnp.float32)
    local_final, local_starts = lax.scan(advance, initial, (block_decay, updates))
    incoming = entering_state(
        jnp.sum(block_log, axis=1).reshape(-1), local_final.reshape(-1, HEAD_CHANNELS)
    ).reshape(head_tensor, HEAD_CHANNELS, HEAD_CHANNELS)
    before = jnp.exp(jnp.cumsum(block_log, axis=1) - block_log).transpose(1, 0, 2)
    starts = local_starts + before[..., None] * incoming[None]
    carried = jnp.einsum(
        "hncd,nhde->hnce", query_heads * jnp.exp(cum_decay), starts, precision=HIGHEST_PRECISION
    )
    outputs = (within + carried).transpose(1, 2, 0, 3).reshape(length, head_tensor, HEAD_CHANNELS)
    factor = lax.rsqrt(jnp.mean(outputs * outputs, axis=2, keepdims=True) + EPSILON)
    normed = (outputs * factor).reshape(length, head_tensor * HEAD_CHANNELS) * head_norm_gain[
        None, :
    ]
    gated_rows = (normed * jax.nn.silu(output_gate_input.astype(jnp.float32))).astype(jnp.bfloat16)
    partial = jnp.dot(gated_rows, recurrence_out_weight, preferred_element_type=jnp.float32)
    return summed_to_owners(partial, TP).astype(jnp.bfloat16)


VMEM = pl.BlockSpec(memory_space=pltpu.VMEM)
ANY = pl.BlockSpec(memory_space=pl.ANY)


def in_vmem(kernel, shapes, *operands):
    return pl.pallas_call(
        kernel,
        out_shape=shapes,
        in_specs=[VMEM] * len(operands),
        out_specs=jax.tree.map(lambda _: VMEM, shapes),
    )(*operands)


def fetching(kernel, shapes, *operands):
    count = len(operands)

    def body(*refs):
        sources, rest = refs[:count], refs[count:]
        outputs, held, arrived = rest[: -count - 1], rest[-count - 1 : -1], rest[-1]
        copies = [
            pltpu.make_async_copy(source, target, arrived.at[i])
            for i, (source, target) in enumerate(zip(sources, held))
        ]
        for copy in copies:
            copy.start()

        def fetch(i):
            def ready():
                copies[i].wait()
                return held[i]

            return ready

        kernel(*[fetch(i) for i in range(count)], *outputs)

    return pl.pallas_call(
        body,
        out_shape=shapes,
        in_specs=[ANY] * count,
        out_specs=jax.tree.map(lambda _: VMEM, shapes),
        scratch_shapes=[pltpu.VMEM(a.shape, a.dtype) for a in operands]
        + [pltpu.SemaphoreType.DMA((count,))],
    )(*operands)


def halves_kernel(whole, first, second):
    middle = first.shape[0]
    first[...] = whole[:middle, :]
    second[...] = whole[middle:, :]


def halves_of(array):
    half = jax.ShapeDtypeStruct((array.shape[0] // 2, array.shape[1]), array.dtype)
    return in_vmem(halves_kernel, (half, half), array)


def select_kernel(experts, hidden_state, gain, index, normed, outgoing):
    top, tokens = index.shape
    slots, width = outgoing.shape
    half = slots // experts
    features = hidden_state[...].astype(jnp.float32)
    factor = lax.rsqrt(jnp.mean(features * features, axis=1, keepdims=True) + EPSILON)
    normed[...] = (features * factor * gain[...]).astype(jnp.bfloat16)
    expert = lax.broadcasted_iota(jnp.int32, (experts, tokens), 0)
    chosen = index[0:1, :] == expert
    for j in range(1, top):
        chosen = chosen | (index[j : j + 1, :] == expert)
    earlier = lax.broadcasted_iota(jnp.int32, (tokens, tokens), 0) < lax.broadcasted_iota(
        jnp.int32, (tokens, tokens), 1
    )
    one = jnp.float32(1)
    zero = jnp.float32(0)
    places = jnp.dot(
        jnp.where(chosen, one, zero).astype(jnp.bfloat16),
        jnp.where(earlier, one, zero).astype(jnp.bfloat16),
        preferred_element_type=jnp.float32,
    )
    places = jnp.where(chosen, places, -one).astype(jnp.bfloat16)
    slot = lax.broadcasted_iota(jnp.int32, (slots, experts), 0)
    spread = jnp.where(
        slot // half == lax.broadcasted_iota(jnp.int32, (slots, experts), 1), one, zero
    ).astype(jnp.bfloat16)
    wanted = jnp.dot(spread, places, preferred_element_type=jnp.float32).astype(jnp.int32)
    own = lax.broadcasted_iota(jnp.int32, (slots, tokens), 0) % half + lax.axis_index(PAIR) * half
    filled = jnp.where(wanted == own, one, zero).astype(jnp.bfloat16)
    start = pl.multiple_of(lax.axis_index(QUAD) * width, width)
    outgoing[...] = jnp.dot(
        filled, normed[:, pl.ds(start, width)], preferred_element_type=jnp.float32
    ).astype(jnp.bfloat16)


def around_products(pieces, matrices):
    quad = lax.axis_index(QUAD)
    held = []

    def dot(piece, matrix, step):
        depth = piece.shape[1]
        count = matrix.shape[0] // depth
        start = pl.multiple_of(((quad + step) & (count - 1)) * depth, depth)
        return jnp.dot(
            piece[...], matrix[pl.ds(start, depth), :], preferred_element_type=jnp.float32
        )

    near = [None] * len(matrices)
    for fetch, step in zip(pieces[:3], (0, -1, 1)):
        piece = fetch()
        for k, fetch_matrix in enumerate(matrices):
            if step == 0:
                held.append(fetch_matrix())
            part = dot(piece, held[k], step)
            near[k] = part if near[k] is None else near[k] + part
    first, second = (fetch() for fetch in pieces[3:])
    middle = first.shape[0]
    return [
        (part[:middle] + dot(first, matrix, 2), part[middle:] + dot(second, matrix, 2))
        for part, matrix in zip(near, held)
    ]


def hidden_kernel(
    own, before, after, far_first, far_second, own_in, partner_in, hidden, hidden_first, hidden_second
):
    pieces = (own, before, after, far_first, far_second)
    middle, units = (hidden_first.shape[0], hidden_first.shape[1] // 2)
    sides = [
        [
            (jax.nn.silu(both[:, :units]) * both[:, units:]).astype(jnp.bfloat16)
            for both in halves
        ]
        for halves in around_products(pieces, (own_in, partner_in))
    ]
    even = lax.axis_index(PAIR) == 0
    for k, part in enumerate((hidden_first, hidden_second)):
        part[:, :units] = jnp.where(even, sides[0][k], sides[1][k])
        part[:, units:] = jnp.where(even, sides[1][k], sides[0][k])
        hidden[pl.ds(k * middle, middle), :] = part[...]


def down_kernel(own, before, after, far_first, far_second, own_down, partner_down, answers):
    pieces = (own, before, after, far_first, far_second)
    sources, _, slots, width = answers.shape
    count = sources // 2
    place = lax.axis_index(PAIR)
    for side, halves in zip(
        (place, 1 - place), around_products(pieces, (own_down, partner_down))
    ):
        for k, part in enumerate(halves):
            answers[pl.ds(k * count, count), side] = part.astype(jnp.bfloat16).reshape(
                count, slots, width
            )


def expert_half(
    expert_hidden_state,
    chosen_expert_index,
    chosen_expert_score,
    expert_norm_gain,
    routed_gate_weight,
    routed_up_weight,
    routed_down_weight,
    shared_gate_weight,
    shared_up_weight,
    shared_down_weight,
):
    tokens, top = chosen_expert_index.shape
    local_experts = routed_gate_weight.shape[0]
    devices = lax.axis_size(EP)
    experts = local_experts * devices
    capacity = min(tokens, 2 * tokens * top // experts)
    width_out = routed_down_weight.shape[2]
    members = lax.axis_size(TP)
    quads = members // 2
    half = capacity // 2
    width_in = routed_gate_weight.shape[1] // quads
    units = routed_gate_weight.shape[2]

    own_in = jnp.concatenate([routed_gate_weight[0], routed_up_weight[0]], axis=1)
    own_down = routed_down_weight[0]
    partner_in = swapped(own_in, TP, 1)
    partner_down = swapped(own_down, TP, 1)

    normed, outgoing = in_vmem(
        functools.partial(select_kernel, experts),
        (
            jax.ShapeDtypeStruct(expert_hidden_state.shape, jnp.bfloat16),
            jax.ShapeDtypeStruct((experts * half, width_in), jnp.bfloat16),
        ),
        expert_hidden_state,
        expert_norm_gain[None, :],
        chosen_expert_index.T,
    )
    arrived = exchanged(outgoing.reshape(devices, half, width_in), EP)
    chunk = arrived.reshape(devices * half, width_in)
    middle = chunk.shape[0] // 2

    gates = ROUTED_SCALE * chosen_expert_score / jnp.sum(chosen_expert_score, axis=1, keepdims=True)
    named = chosen_expert_index[:, :, None] == jnp.arange(experts, dtype=jnp.int32)[None, None, :]
    chosen = jnp.any(named, axis=1)
    gate_of = jnp.sum(jnp.where(named, gates[:, :, None], 0.0), axis=1)
    row = jnp.arange(tokens)
    places = jnp.dot(
        (row[None, :] < row[:, None]).astype(jnp.bfloat16),
        chosen.astype(jnp.bfloat16),
        preferred_element_type=jnp.float32,
    )
    places = jnp.where(chosen, places.astype(jnp.int32), -1)
    shared_hidden = (
        jax.nn.silu(jnp.dot(normed, shared_gate_weight, preferred_element_type=jnp.float32))
        * jnp.dot(normed, shared_up_weight, preferred_element_type=jnp.float32)
    ).astype(jnp.bfloat16)
    shared_piece = gathered_columns(shared_hidden, TP)
    shared_down = rows_by_reversed_bits(shared_down_weight, members)
    shared = jnp.dot(shared_piece, shared_down, preferred_element_type=jnp.float32)

    before = shifted(chunk, TP, 2)
    after = shifted(chunk, TP, -2)
    far = [shifted(half, TP, step) for half, step in zip(halves_of(chunk), (4, -4))]
    part_shape = jax.ShapeDtypeStruct((middle, 2 * units), jnp.bfloat16)
    hidden, hidden_first, hidden_second = fetching(
        hidden_kernel,
        (jax.ShapeDtypeStruct((chunk.shape[0], 2 * units), jnp.bfloat16), part_shape, part_shape),
        chunk,
        before,
        after,
        *far,
        own_in,
        partner_in,
    )
    before = shifted(hidden, TP, 2)
    after = shifted(hidden, TP, -2)
    far = [shifted(hidden_first, TP, 4), shifted(hidden_second, TP, -4)]
    answers = fetching(
        down_kernel,
        jax.ShapeDtypeStruct((devices, 2, half, width_out), jnp.bfloat16),
        hidden,
        before,
        after,
        *far,
        own_down,
        partner_down,
    )
    returned = exchanged(answers.reshape(2 * devices, half, width_out), EP_PAIR)
    returned = returned.reshape(experts * capacity, width_out)
    filled = places[:, :, None] == jnp.arange(capacity)[None, None, :]
    mixing = jnp.where(filled, gate_of[:, :, None], 0.0).reshape(tokens, experts * capacity)
    for part in in_parts(mixing, 3):
        shared = shared + jnp.dot(part, returned, preferred_element_type=jnp.float32)
    return shared.astype(jnp.bfloat16)


def per_device(
    recurrence_query_input,
    forget_gate_input,
    recurrence_value_input,
    output_gate_input,
    forget_lower_margin,
    position_decay_extra,
    head_norm_gain,
    recurrence_out_weight,
    expert_hidden_state,
    chosen_expert_index,
    chosen_expert_score,
    expert_norm_gain,
    routed_gate_weight,
    routed_up_weight,
    routed_down_weight,
    shared_gate_weight,
    shared_up_weight,
    shared_down_weight,
):
    recurrence_output = mixer_half(
        recurrence_query_input,
        forget_gate_input,
        recurrence_value_input,
        output_gate_input,
        forget_lower_margin,
        position_decay_extra,
        head_norm_gain,
        recurrence_out_weight,
    )
    expert_out = expert_half(
        expert_hidden_state,
        chosen_expert_index,
        chosen_expert_score,
        expert_norm_gain,
        routed_gate_weight,
        routed_up_weight,
        routed_down_weight,
        shared_gate_weight,
        shared_up_weight,
        shared_down_weight,
    )
    return (recurrence_output, expert_out)


def solution(mesh):
    split = Mesh(
        mesh.devices.reshape(mesh.shape["grp"], -1, 2, mesh.shape["tp"] // 2, 2),
        GRP_EP_TP,
    )
    in_specs = (
        P(GRP_EP, TP),
        P(GRP_EP, TP),
        P(GRP_EP, TP),
        P(GRP_EP, TP),
        P(TP),
        P(GRP_EP, TP),
        P(TP),
        P(TP, None),
        P(GRP_EP, None),
        P(GRP_EP, None),
        P(GRP_EP, None),
        P(),
        P(EP, None, TP),
        P(EP, None, TP),
        P(EP, None, TP),
        P(None, TP),
        P(None, TP),
        P(None, TP),
    )
    out_specs = (P(GRP_EP_TP, None), P(GRP_EP, TP))

    return jax.shard_map(
        per_device, mesh=split, in_specs=in_specs, out_specs=out_specs, check_vma=False
    )
```

```python
import functools

import jax
import jax.numpy as jnp
from jax import lax
from jax.experimental import pallas as pl
from jax.experimental.pallas import tpu as pltpu
from jax.sharding import Mesh
from jax.sharding import PartitionSpec as P


HEAD_CHANNELS = 128
BLK = 64
EP = ("ep_0", "ep_1")
GRP_EP = ("grp", "ep_0", "ep_1")
QUAD, PAIR = ("tq", "tb")
TP = (QUAD, PAIR)
EP_PAIR = (*EP, PAIR)
GRP_EP_TP = (*GRP_EP, *TP)


EPSILON = 1e-06
ROUTED_SCALE = 2.5
HIGHEST_PRECISION = lax.Precision.HIGHEST


def shifted(array, axis, step):
    count = lax.axis_size(axis)
    return lax.ppermute(array, axis, [(i, (i + step) % count) for i in range(count)])


def swapped(array, axis, bit):
    count = lax.axis_size(axis)
    return lax.ppermute(array, axis, [(i, i ^ bit) for i in range(count)])


def exchanged(array, axis):
    return lax.all_to_all(array, axis, split_axis=0, concat_axis=0, tiled=True)


def half_of(array, dim, place):
    return lax.dynamic_index_in_dim(array, place, dim, keepdims=False)


def summed_to_owners(array, axis):
    count = lax.axis_size(axis)
    bits = count.bit_length() - 1
    member = lax.axis_index(axis)
    kept = array.reshape(*[2] * bits, -1, array.shape[1])
    for bit in range(bits):
        mine = (member >> bit) & 1
        dim = bits - 1 - bit
        arrived = swapped(half_of(kept, dim, 1 - mine).astype(jnp.bfloat16), axis, 1 << bit)
        kept = half_of(kept, dim, mine) + arrived.astype(jnp.float32)
    return kept


def gathered_columns(array, axis):
    count = lax.axis_size(axis)
    member = lax.axis_index(axis)
    for bit in reversed(range(count.bit_length() - 1)):
        arrived = swapped(array, axis, 1 << bit)
        first = ((member >> bit) & 1) == 0
        array = jnp.concatenate(
            [jnp.where(first, array, arrived), jnp.where(first, arrived, array)], axis=1
        )
    return array


def rows_by_reversed_bits(matrix, count):
    bits = count.bit_length() - 1
    split = matrix.reshape(*[2] * bits, -1, matrix.shape[1])
    order = (*reversed(range(bits)), bits, bits + 1)
    return split.transpose(order).reshape(matrix.shape)


def in_parts(array, count):
    parts, rest = [], array
    for _ in range(count):
        rounded = lax.reduce_precision(rest, 8, 7)
        parts.append(rounded.astype(jnp.bfloat16))
        rest = rest - rounded
    return parts


def entering_state(log_decay, state):
    devices = lax.axis_size(EP)
    channels, width = state.shape
    part = channels // devices
    logs = jnp.stack(in_parts(log_decay, 3), axis=-1).reshape(devices, part, 3)
    logs = jnp.pad(logs, ((0, 0), (0, 0), (0, HEAD_CHANNELS - 3)))
    packed = jnp.concatenate(
        [state.astype(jnp.bfloat16).reshape(devices, part, width), logs], axis=2
    )
    arrived = exchanged(packed, EP)
    arrived = arrived.astype(jnp.float32)
    updates = arrived[:, :, :width]
    logs = jnp.sum(arrived[:, :, width : width + 3], axis=2)
    at = jnp.arange(devices)
    between = (at[None, None, :] > at[None, :, None]) & (at[None, None, :] < at[:, None, None])
    spans = jnp.dot(
        between.reshape(devices * devices, devices).astype(jnp.float32),
        logs,
        precision=HIGHEST_PRECISION,
    ).reshape(devices, devices, part)
    earlier = at[None, :, None] < at[:, None, None]
    factors = jnp.where(earlier, jnp.exp(spans), 0.0)
    prefix = jnp.einsum("rqc,qcv->rcv", factors, updates, precision=HIGHEST_PRECISION)
    prefix = prefix.astype(jnp.bfloat16)
    returned = exchanged(prefix, EP)
    return returned.astype(jnp.float32).reshape(channels, width)


def mixer_half(
    recurrence_query_input,
    forget_gate_input,
    recurrence_value_input,
    output_gate_input,
    forget_lower_margin,
    position_decay_extra,
    head_norm_gain,
    recurrence_out_weight,
):
    length = recurrence_query_input.shape[0]
    head_tensor = position_decay_extra.shape[1]
    blocks = length // BLK
    queries = jax.nn.silu(recurrence_query_input.astype(jnp.float32))
    key_gate_value = forget_lower_margin[None, :] * jax.nn.sigmoid(
        -forget_gate_input.astype(jnp.float32)
    )
    decay_logarithm = jnp.log1p(-key_gate_value) + jnp.repeat(
        position_decay_extra, HEAD_CHANNELS, axis=1
    )
    value_rows = recurrence_value_input.astype(jnp.float32)

    def split_heads(tensor):
        return tensor.reshape(blocks, BLK, head_tensor, HEAD_CHANNELS).transpose(2, 0, 1, 3)

    query_heads = split_heads(queries)
    key_heads = split_heads(key_gate_value)
    value_heads = split_heads(value_rows)
    cum_decay = jnp.cumsum(split_heads(decay_logarithm), axis=2)
    middle = cum_decay[:, :, BLK // 2 - 1 : BLK // 2]
    block_end = cum_decay[:, :, BLK - 1 : BLK]
    scores = jnp.einsum(
        "hncd,hnsd->hncs",
        query_heads * jnp.exp(cum_decay - middle),
        key_heads * jnp.exp(middle - cum_decay),
        precision=HIGHEST_PRECISION,
    )
    causal = jnp.tril(jnp.ones((BLK, BLK), dtype=bool))
    scores = jnp.where(causal, scores, 0.0)
    within = jnp.einsum("hncs,hnse->hnce", scores, value_heads, precision=HIGHEST_PRECISION)
    updates = jnp.einsum(
        "hncd,hnce->nhde",
        key_heads * jnp.exp(block_end - cum_decay),
        value_heads,
        precision=HIGHEST_PRECISION,
    )
    block_log = block_end[:, :, 0, :]
    block_decay = jnp.exp(block_log).transpose(1, 0, 2)

    def advance(carry_state, inputs):
        factor, update = inputs
        return (factor[..., None] * carry_state + update, carry_state)

    initial = jnp.zeros((head_tensor, HEAD_CHANNELS, HEAD_CHANNELS), jnp.float32)
    local_final, local_starts = lax.scan(advance, initial, (block_decay, updates))
    incoming = entering_state(
        jnp.sum(block_log, axis=1).reshape(-1), local_final.reshape(-1, HEAD_CHANNELS)
    ).reshape(head_tensor, HEAD_CHANNELS, HEAD_CHANNELS)
    before = jnp.exp(jnp.cumsum(block_log, axis=1) - block_log).transpose(1, 0, 2)
    starts = local_starts + before[..., None] * incoming[None]
    carried = jnp.einsum(
        "hncd,nhde->hnce", query_heads * jnp.exp(cum_decay), starts, precision=HIGHEST_PRECISION
    )
    outputs = (within + carried).transpose(1, 2, 0, 3).reshape(length, head_tensor, HEAD_CHANNELS)
    factor = lax.rsqrt(jnp.mean(outputs * outputs, axis=2, keepdims=True) + EPSILON)
    normed = (outputs * factor).reshape(length, head_tensor * HEAD_CHANNELS) * head_norm_gain[
        None, :
    ]
    gated_rows = (normed * jax.nn.silu(output_gate_input.astype(jnp.float32))).astype(jnp.bfloat16)
    partial = jnp.dot(gated_rows, recurrence_out_weight, preferred_element_type=jnp.float32)
    return summed_to_owners(partial, TP).astype(jnp.bfloat16)


VMEM = pl.BlockSpec(memory_space=pltpu.VMEM)
ANY = pl.BlockSpec(memory_space=pl.ANY)


def in_vmem(kernel, shapes, *operands):
    return pl.pallas_call(
        kernel,
        out_shape=shapes,
        in_specs=[VMEM] * len(operands),
        out_specs=jax.tree.map(lambda _: VMEM, shapes),
    )(*operands)


def fetching(kernel, shapes, *operands):
    count = len(operands)

    def body(*refs):
        sources, rest = refs[:count], refs[count:]
        outputs, held, arrived = rest[: -count - 1], rest[-count - 1 : -1], rest[-1]
        copies = [
            pltpu.make_async_copy(source, target, arrived.at[i])
            for i, (source, target) in enumerate(zip(sources, held))
        ]
        for copy in copies:
            copy.start()

        def fetch(i):
            def ready():
                copies[i].wait()
                return held[i]

            return ready

        kernel(*[fetch(i) for i in range(count)], *outputs)

    return pl.pallas_call(
        body,
        out_shape=shapes,
        in_specs=[ANY] * count,
        out_specs=jax.tree.map(lambda _: VMEM, shapes),
        scratch_shapes=[pltpu.VMEM(a.shape, a.dtype) for a in operands]
        + [pltpu.SemaphoreType.DMA((count,))],
    )(*operands)


def halves_kernel(whole, first, second):
    middle = first.shape[0]
    first[...] = whole[:middle, :]
    second[...] = whole[middle:, :]


def halves_of(array):
    half = jax.ShapeDtypeStruct((array.shape[0] // 2, array.shape[1]), array.dtype)
    return in_vmem(halves_kernel, (half, half), array)


def select_kernel(experts, hidden_state, gain, index, normed, outgoing):
    top, tokens = index.shape
    slots, width = outgoing.shape
    half = slots // experts
    features = hidden_state[...].astype(jnp.float32)
    factor = lax.rsqrt(jnp.mean(features * features, axis=1, keepdims=True) + EPSILON)
    normed[...] = (features * factor * gain[...]).astype(jnp.bfloat16)
    expert = lax.broadcasted_iota(jnp.int32, (experts, tokens), 0)
    chosen = index[0:1, :] == expert
    for j in range(1, top):
        chosen = chosen | (index[j : j + 1, :] == expert)
    earlier = lax.broadcasted_iota(jnp.int32, (tokens, tokens), 0) < lax.broadcasted_iota(
        jnp.int32, (tokens, tokens), 1
    )
    one = jnp.float32(1)
    zero = jnp.float32(0)
    places = jnp.dot(
        jnp.where(chosen, one, zero).astype(jnp.bfloat16),
        jnp.where(earlier, one, zero).astype(jnp.bfloat16),
        preferred_element_type=jnp.float32,
    )
    places = jnp.where(chosen, places, -one).astype(jnp.bfloat16)
    slot = lax.broadcasted_iota(jnp.int32, (slots, experts), 0)
    spread = jnp.where(
        slot // half == lax.broadcasted_iota(jnp.int32, (slots, experts), 1), one, zero
    ).astype(jnp.bfloat16)
    wanted = jnp.dot(spread, places, preferred_element_type=jnp.float32).astype(jnp.int32)
    own = lax.broadcasted_iota(jnp.int32, (slots, tokens), 0) % half + lax.axis_index(PAIR) * half
    filled = jnp.where(wanted == own, one, zero).astype(jnp.bfloat16)
    start = pl.multiple_of(lax.axis_index(QUAD) * width, width)
    outgoing[...] = jnp.dot(
        filled, normed[:, pl.ds(start, width)], preferred_element_type=jnp.float32
    ).astype(jnp.bfloat16)


def around_products(pieces, matrices):
    quad = lax.axis_index(QUAD)
    held = []

    def dot(piece, matrix, step):
        depth = piece.shape[1]
        count = matrix.shape[0] // depth
        start = pl.multiple_of(((quad + step) & (count - 1)) * depth, depth)
        return jnp.dot(
            piece[...], matrix[pl.ds(start, depth), :], preferred_element_type=jnp.float32
        )

    near = [None] * len(matrices)
    for fetch, step in zip(pieces[:3], (0, -1, 1)):
        piece = fetch()
        for k, fetch_matrix in enumerate(matrices):
            if step == 0:
                held.append(fetch_matrix())
            part = dot(piece, held[k], step)
            near[k] = part if near[k] is None else near[k] + part
    first, second = (fetch() for fetch in pieces[3:])
    middle = first.shape[0]
    return [
        (part[:middle] + dot(first, matrix, 2), part[middle:] + dot(second, matrix, 2))
        for part, matrix in zip(near, held)
    ]


def hidden_kernel(
    own, before, after, far_first, far_second, own_in, partner_in, hidden, hidden_first, hidden_second
):
    pieces = (own, before, after, far_first, far_second)
    middle, units = (hidden_first.shape[0], hidden_first.shape[1] // 2)
    sides = [
        [
            (jax.nn.silu(both[:, :units]) * both[:, units:]).astype(jnp.bfloat16)
            for both in halves
        ]
        for halves in around_products(pieces, (own_in, partner_in))
    ]
    even = lax.axis_index(PAIR) == 0
    for k, part in enumerate((hidden_first, hidden_second)):
        part[:, :units] = jnp.where(even, sides[0][k], sides[1][k])
        part[:, units:] = jnp.where(even, sides[1][k], sides[0][k])
        hidden[pl.ds(k * middle, middle), :] = part[...]


def down_kernel(own, before, after, far_first, far_second, own_down, partner_down, answers):
    pieces = (own, before, after, far_first, far_second)
    sources, _, slots, width = answers.shape
    count = sources // 2
    place = lax.axis_index(PAIR)
    for side, halves in zip(
        (place, 1 - place), around_products(pieces, (own_down, partner_down))
    ):
        for k, part in enumerate(halves):
            answers[pl.ds(k * count, count), side] = part.astype(jnp.bfloat16).reshape(
                count, slots, width
            )


def expert_half(
    expert_hidden_state,
    chosen_expert_index,
    chosen_expert_score,
    expert_norm_gain,
    routed_gate_weight,
    routed_up_weight,
    routed_down_weight,
    shared_gate_weight,
    shared_up_weight,
    shared_down_weight,
):
    tokens, top = chosen_expert_index.shape
    local_experts = routed_gate_weight.shape[0]
    devices = lax.axis_size(EP)
    experts = local_experts * devices
    capacity = min(tokens, 2 * tokens * top // experts)
    width_out = routed_down_weight.shape[2]
    members = lax.axis_size(TP)
    quads = members // 2
    half = capacity // 2
    width_in = routed_gate_weight.shape[1] // quads
    units = routed_gate_weight.shape[2]

    own_in = jnp.concatenate([routed_gate_weight[0], routed_up_weight[0]], axis=1)
    own_down = routed_down_weight[0]
    partner_in = swapped(own_in, TP, 1)
    partner_down = swapped(own_down, TP, 1)

    normed, outgoing = in_vmem(
        functools.partial(select_kernel, experts),
        (
            jax.ShapeDtypeStruct(expert_hidden_state.shape, jnp.bfloat16),
            jax.ShapeDtypeStruct((experts * half, width_in), jnp.bfloat16),
        ),
        expert_hidden_state,
        expert_norm_gain[None, :],
        chosen_expert_index.T,
    )
    arrived = exchanged(outgoing.reshape(devices, half, width_in), EP)
    chunk = arrived.reshape(devices * half, width_in)
    middle = chunk.shape[0] // 2

    gates = ROUTED_SCALE * chosen_expert_score / jnp.sum(chosen_expert_score, axis=1, keepdims=True)
    named = chosen_expert_index[:, :, None] == jnp.arange(experts, dtype=jnp.int32)[None, None, :]
    chosen = jnp.any(named, axis=1)
    gate_of = jnp.sum(jnp.where(named, gates[:, :, None], 0.0), axis=1)
    row = jnp.arange(tokens)
    places = jnp.dot(
        (row[None, :] < row[:, None]).astype(jnp.bfloat16),
        chosen.astype(jnp.bfloat16),
        preferred_element_type=jnp.float32,
    )
    places = jnp.where(chosen, places.astype(jnp.int32), -1)
    shared_hidden = (
        jax.nn.silu(jnp.dot(normed, shared_gate_weight, preferred_element_type=jnp.float32))
        * jnp.dot(normed, shared_up_weight, preferred_element_type=jnp.float32)
    ).astype(jnp.bfloat16)
    shared_piece = gathered_columns(shared_hidden, TP)
    shared_down = rows_by_reversed_bits(shared_down_weight, members)
    shared = jnp.dot(shared_piece, shared_down, preferred_element_type=jnp.float32)

    before = shifted(chunk, TP, 2)
    after = shifted(chunk, TP, -2)
    far = [shifted(half, TP, step) for half, step in zip(halves_of(chunk), (4, -4))]
    part_shape = jax.ShapeDtypeStruct((middle, 2 * units), jnp.bfloat16)
    hidden, hidden_first, hidden_second = fetching(
        hidden_kernel,
        (jax.ShapeDtypeStruct((chunk.shape[0], 2 * units), jnp.bfloat16), part_shape, part_shape),
        chunk,
        before,
        after,
        *far,
        own_in,
        partner_in,
    )
    before = shifted(hidden, TP, 2)
    after = shifted(hidden, TP, -2)
    far = [shifted(hidden_first, TP, 4), shifted(hidden_second, TP, -4)]
    answers = fetching(
        down_kernel,
        jax.ShapeDtypeStruct((devices, 2, half, width_out), jnp.bfloat16),
        hidden,
        before,
        after,
        *far,
        own_down,
        partner_down,
    )
    returned = exchanged(answers.reshape(2 * devices, half, width_out), EP_PAIR)
    returned = returned.reshape(experts * capacity, width_out)
    filled = places[:, :, None] == jnp.arange(capacity)[None, None, :]
    mixing = jnp.where(filled, gate_of[:, :, None], 0.0)
    mixing_parts = in_parts(mixing.reshape(tokens, experts * capacity), 3)
    for part in mixing_parts:
        shared = shared + jnp.dot(part, returned, preferred_element_type=jnp.float32)
    return shared.astype(jnp.bfloat16)


def per_device(
    recurrence_query_input,
    forget_gate_input,
    recurrence_value_input,
    output_gate_input,
    forget_lower_margin,
    position_decay_extra,
    head_norm_gain,
    recurrence_out_weight,
    expert_hidden_state,
    chosen_expert_index,
    chosen_expert_score,
    expert_norm_gain,
    routed_gate_weight,
    routed_up_weight,
    routed_down_weight,
    shared_gate_weight,
    shared_up_weight,
    shared_down_weight,
):
    recurrence_output = mixer_half(
        recurrence_query_input,
        forget_gate_input,
        recurrence_value_input,
        output_gate_input,
        forget_lower_margin,
        position_decay_extra,
        head_norm_gain,
        recurrence_out_weight,
    )
    expert_out = expert_half(
        expert_hidden_state,
        chosen_expert_index,
        chosen_expert_score,
        expert_norm_gain,
        routed_gate_weight,
        routed_up_weight,
        routed_down_weight,
        shared_gate_weight,
        shared_up_weight,
        shared_down_weight,
    )
    return (recurrence_output, expert_out)


def solution(mesh):
    split = Mesh(
        mesh.devices.reshape(mesh.shape["grp"], -1, 2, mesh.shape["tp"] // 2, 2),
        GRP_EP_TP,
    )
    in_specs = (
        P(GRP_EP, TP),
        P(GRP_EP, TP),
        P(GRP_EP, TP),
        P(GRP_EP, TP),
        P(TP),
        P(GRP_EP, TP),
        P(TP),
        P(TP, None),
        P(GRP_EP, None),
        P(GRP_EP, None),
        P(GRP_EP, None),
        P(),
        P(EP, None, TP),
        P(EP, None, TP),
        P(EP, None, TP),
        P(None, TP),
        P(None, TP),
        P(None, TP),
    )
    out_specs = (P(GRP_EP_TP, None), P(GRP_EP, TP))

    return jax.shard_map(
        per_device, mesh=split, in_specs=in_specs, out_specs=out_specs, check_vma=False
    )
```
